128 devices in a mesh: sp: 16 (over z, y), dp: 8 (over x, core).
Axes of the slice: x: 4, y: 4, z: 4, core: 2. Of those that a mesh axis runs over, the one named last changes fastest.
Arguments:
- inputs: bfloat16 [8, 3072, 2048], P('dp', 'sp'), may hold values from -6 to 6
- in_gain: float32 [2048], replicated, may hold values from 0.1 to 1.9
- w_query: bfloat16 [2048, 1024], P('dp', 'sp'), may hold values from -0.125 to 0.125
- w_key: bfloat16 [2048, 256], P('dp', 'sp'), may hold values from -0.375 to 0.375
- w_value: bfloat16 [2048, 256], P('dp', 'sp'), may hold values from -0.125 to 0.125
- key_bias: float32 [8, 3072, 16], P('dp', None, 'sp'), may hold values from -20 to 0
- out_gain: float32 [1024], replicated, may hold values from 0.1 to 1.9
- w_out: bfloat16 [1024, 2048], P('sp', 'dp'), may hold values from -0.1875 to 0.1875
Outputs:
- mixed: bfloat16 [8, 3072, 2048], P('dp', 'sp')
The draws below stay inside these ranges and needn't reach their ends.
All inputs are finite; a program needn't handle non-finite values.
Results may differ from the reference program's by a relative error of at most 0.012.
The reference program's roundings to bfloat16 on the way (of `normed`, `queries`, `keys`, `values`, `sticks` and `head_out`) count: a program that leaves them out, or rounds other values in their place, can miss the bound.
Values may be sent and summed in bfloat16 or wider, within the bound.
A program may use at most 128 MiB of HBM per device.

```python
import math
import jax
import jax.numpy as jnp
from jax import lax

D = 2048
QUERY_HEADS = 16
KV_HEADS = 4
HEAD_DIM = 64
TOK_DEV = 192
SEQUENCE_LENGTH = 3072
BATCH_COUNT = 8


logit_shift = 4.5


def draw_key_bias(key, part):
    parallel_flows = jax.random.split(jax.random.fold_in(key, 17), 6)
    fast_share = 0.5
    coins = jax.random.uniform(parallel_flows[0], (BATCH_COUNT, 1, QUERY_HEADS), jnp.float32)
    fast = coins < fast_share
    fast_rate = jnp.exp(jax.random.uniform(parallel_flows[1], (BATCH_COUNT, 1, QUERY_HEADS), jnp.float32, math.log(1.0 / 100.0), math.log(1.0 / 30.0)))
    slow_rate = jnp.exp(jax.random.uniform(parallel_flows[2], (BATCH_COUNT, 1, QUERY_HEADS), jnp.float32, math.log(1.0 / (8.0 * SEQUENCE_LENGTH)), math.log(1.0 / (2.0 * SEQUENCE_LENGTH))))
    rate = jnp.where(fast, fast_rate, slow_rate)
    factor = jnp.exp(jax.random.uniform(parallel_flows[3], (BATCH_COUNT, SEQUENCE_LENGTH // TOK_DEV, QUERY_HEADS), jnp.float32, math.log(0.5), math.log(2.0)))
    factor = jnp.repeat(factor, TOK_DEV, axis=1)
    start_offsets = jnp.log(rate * factor) - logit_shift
    transfer_group_at = jax.random.randint(parallel_flows[4], (BATCH_COUNT, 4), 0, SEQUENCE_LENGTH)
    transfer_group = jnp.any(jnp.arange(SEQUENCE_LENGTH)[None, :, None] == transfer_group_at[:, None, :], axis=2)
    transfer_group_value = jax.random.uniform(parallel_flows[5], (BATCH_COUNT, SEQUENCE_LENGTH, QUERY_HEADS), jnp.float32, -4.0, -2.0)
    start_offsets = jnp.where(transfer_group[:, :, None], transfer_group_value, start_offsets)
    return start_offsets.astype(jnp.float32)


def block_scale(stream_key, extent, cuts, smallest, largest):
    def one(dim, parts):
        draws = jax.random.uniform(jax.random.fold_in(jax.random.fold_in(stream_key, 6), dim), (parts,), jnp.float32, smallest / len(cuts), largest / len(cuts))
        return jnp.repeat(jnp.exp(draws), extent[dim] // parts).reshape((-1,) + (1,) * (len(extent) - dim - 1))

    loudness = one(*cuts[0])
    for cut in cuts[1:]:
        loudness = loudness * one(*cut)
    return loudness


def gaussian(rng, shape, width, reach, cuts=(), kind=jnp.bfloat16):
    drawn = jax.random.normal(rng, shape, jnp.float32) * width
    if len(cuts) > 0:
        drawn = block_scale(rng, shape, cuts, -0.22, 0.18) * drawn
    return jnp.clip(drawn, min=-reach, max=reach).astype(kind)


def setup_inputs(seed: int = 0) -> dict:
    splits = jax.random.split(jax.random.key(seed), 9)
    inputs = gaussian(splits[0], (BATCH_COUNT, SEQUENCE_LENGTH, D), 1.0, 6.0, ((0, 8), (1, 16)))
    in_gain = jnp.clip(1.0 + 0.18 * jax.random.normal(splits[1], (D,), jnp.float32), 0.1, 1.9)
    w_query = gaussian(splits[2], (D, QUERY_HEADS * HEAD_DIM), D ** -0.5, 0.125, ((0, 8), (1, 16)))
    w_key = gaussian(splits[3], (D, KV_HEADS * HEAD_DIM), (D // 9) ** -0.5, 0.375, ((0, 8), (1, 16)))
    w_value = gaussian(splits[4], (D, KV_HEADS * HEAD_DIM), D ** -0.5, 0.125, ((0, 8), (1, 16)))
    key_bias = draw_key_bias(jax.random.fold_in(splits[8], 71), 0)
    out_gain = jnp.clip(1.0 + 0.18 * jax.random.normal(splits[6], (QUERY_HEADS * HEAD_DIM,), jnp.float32), 0.1, 1.9)
    w_out = gaussian(splits[7], (QUERY_HEADS * HEAD_DIM, D), (QUERY_HEADS * HEAD_DIM) ** -0.5, 0.1875, ((0, 16), (1, 8)))
    return dict(inputs=inputs, in_gain=in_gain, w_query=w_query, w_key=w_key, w_value=w_value, key_bias=key_bias, out_gain=out_gain, w_out=w_out)


norm_eps = 1e-06

def breaking_rows(query_rows, key_rows, value_rows, bias_row, start):
    logits = jnp.dot(query_rows, key_rows.T, preferred_element_type=jnp.float32) * HEAD_DIM ** (-0.5) + bias_row[None, :]
    rows = start + jnp.arange(query_rows.shape[0], dtype=jnp.int32)[:, None]
    columns = jnp.arange(key_rows.shape[0], dtype=jnp.int32)[None, :]
    strict = columns < rows
    log_keep = jnp.where(strict, jax.nn.log_sigmoid(-logits), jnp.float32(0.0))
    log_rest = lax.cumsum(log_keep, axis=1, reverse=True) - log_keep
    sticks = jnp.where(strict, jnp.exp(jax.nn.log_sigmoid(logits) + log_rest), jnp.float32(0.0)).astype(jnp.bfloat16)
    return jnp.dot(sticks, value_rows, preferred_element_type=jnp.float32)

def one_head(packed):
    query_all, key_all, value_all, bias_all = packed
    block = min(512, SEQUENCE_LENGTH)
    pieces = []
    for index in range(SEQUENCE_LENGTH // block):
        start = index * block
        end = start + block
        pieces.append(breaking_rows(query_all[start:end], key_all[:end], value_all[:end], bias_all[:end], start))
    return jnp.concatenate(pieces, axis=0)

def reference(inputs, in_gain, w_query, w_key, w_value, key_bias, out_gain, w_out):
    wide = inputs.astype(jnp.float32)
    normed = (wide * lax.rsqrt(lax.optimization_barrier(jnp.mean(wide * wide, axis=-1, keepdims=True)) + norm_eps) * in_gain).astype(jnp.bfloat16)
    flat = normed.reshape(BATCH_COUNT * SEQUENCE_LENGTH, D)
    queries = jnp.dot(flat, w_query, preferred_element_type=jnp.float32).astype(jnp.bfloat16)
    keys = jnp.dot(flat, w_key, preferred_element_type=jnp.float32).astype(jnp.bfloat16)
    values = jnp.dot(flat, w_value, preferred_element_type=jnp.float32).astype(jnp.bfloat16)
    group = QUERY_HEADS // KV_HEADS
    queries = queries.reshape(BATCH_COUNT, SEQUENCE_LENGTH, QUERY_HEADS, HEAD_DIM).transpose(0, 2, 1, 3).reshape(BATCH_COUNT * QUERY_HEADS, SEQUENCE_LENGTH, HEAD_DIM)
    keys = jnp.repeat(keys.reshape(BATCH_COUNT, SEQUENCE_LENGTH, KV_HEADS, HEAD_DIM), group, axis=2)
    keys = keys.transpose(0, 2, 1, 3).reshape(BATCH_COUNT * QUERY_HEADS, SEQUENCE_LENGTH, HEAD_DIM)
    values = jnp.repeat(values.reshape(BATCH_COUNT, SEQUENCE_LENGTH, KV_HEADS, HEAD_DIM), group, axis=2)
    values = values.transpose(0, 2, 1, 3).reshape(BATCH_COUNT * QUERY_HEADS, SEQUENCE_LENGTH, HEAD_DIM)
    biases = key_bias.transpose(0, 2, 1).reshape(BATCH_COUNT * QUERY_HEADS, SEQUENCE_LENGTH)
    attended = lax.map(one_head, (queries, keys, values, biases))
    attended = attended.reshape(BATCH_COUNT, QUERY_HEADS, SEQUENCE_LENGTH, HEAD_DIM).transpose(0, 2, 1, 3)
    scaled = attended * lax.rsqrt(lax.optimization_barrier(jnp.mean(attended * attended, axis=-1, keepdims=True)) + norm_eps)
    head_out = (scaled * out_gain.reshape(QUERY_HEADS, HEAD_DIM)).astype(jnp.bfloat16).reshape(BATCH_COUNT * SEQUENCE_LENGTH, QUERY_HEADS * HEAD_DIM)
    mixed = jnp.dot(head_out, w_out, preferred_element_type=jnp.float32).astype(jnp.bfloat16)
    return mixed.reshape(BATCH_COUNT, SEQUENCE_LENGTH, D)
```

```python
import functools

import jax
import jax.numpy as jnp
from jax import lax
from jax.experimental import pallas as pl
from jax.experimental.pallas import tpu as pltpu
from jax.sharding import PartitionSpec as P

HEAD_DIM = 64
RING = 4
EPS = 1e-06
LOG2E = 1.4426950408889634
F32 = jnp.float32
BF16 = jnp.bfloat16
MESH = pl.DeviceIdType.MESH


def rcopy(src, dst, send, recv, device):
    return pltpu.make_async_remote_copy(
        src_ref=src, dst_ref=dst, send_sem=send, recv_sem=recv, device_id=device, device_id_type=MESH
    )


def places():
    sp, dp = lax.axis_index("sp"), lax.axis_index("dp")
    z, y = lax.div(sp, RING), lax.rem(sp, RING)
    x, c = lax.div(dp, 2), lax.rem(dp, 2)

    def at(dz=0, dy=0, dx=0, dc=0):
        nz, ny = lax.rem(z + dz, RING), lax.rem(y + dy, RING)
        nx, nc = lax.rem(x + dx, RING), lax.rem(c + dc, 2)
        return {"sp": nz * RING + ny, "dp": nx * 2 + nc}

    return z, y, x, c, at


def project_kernel(
    x_ref, gain_ref, wq_ref, wk_ref, wv_ref,
    qv_ref, kk_ref,
    packs, w_all, xg, stage_qv, stage_k,
    wy_s, wy_r, wx_s, wx_r, wf_s, wf_r, wc_s, wc_r, xd_s, xd_r, xf_s, xf_r, a_s, a_r, b_s, b_r,
):
    z, y, x, c, at = places()
    rows = x_ref.shape[0]
    half = rows // 2
    depth = wq_ref.shape[0]
    packs[c, x, y] = jnp.concatenate(
        [wq_ref[...], wk_ref[...], wv_ref[...], jnp.zeros((depth, 32), BF16)], axis=1
    )
    friends = [at(dz=1), at(dz=3), at(dy=1), at(dy=2), at(dy=3), at(dx=1), at(dx=3), at(dc=1)]
    barrier = pltpu.get_barrier_semaphore()
    for f in friends:
        pl.semaphore_signal(barrier, inc=1, device_id=f, device_id_type=MESH)
    pl.semaphore_wait(barrier, len(friends))

    sent = []

    def go(copy):
        copy.start()
        sent.append(copy)

    lo, hi = pl.ds(0, half), pl.ds(half, half)
    x_right = [rcopy(x_ref.at[p], xg.at[0, p], xd_s.at[0, i], xd_r.at[0, i], at(dz=1)) for i, p in enumerate((lo, hi))]
    x_left = [rcopy(x_ref.at[p], xg.at[1, p], xd_s.at[1, i], xd_r.at[1, i], at(dz=3)) for i, p in enumerate((hi, lo))]
    go(x_right[0])
    go(x_left[0])

    def piece(o):
        return lax.rem(y + RING - o, RING)

    wy = [None] + [
        rcopy(packs.at[c, x, y], packs.at[c, x, y], wy_s.at[o], wy_r.at[o], at(dy=o)) for o in (1, 2, 3)
    ]

    def from_y(o):
        p = packs.at[c, x, piece(o)]
        return rcopy(p, p, wy_s.at[o], wy_r.at[o], at(dy=o))

    def along_x(o, d):
        p = packs.at[c, x, piece(o)]
        return rcopy(p, p, wx_s.at[d, o], wx_r.at[d, o], at(dx=1 if d == 0 else 3))

    def arrived_x(o, d):
        nx = lax.rem(x + (3 if d == 0 else 1), RING)
        p = packs.at[c, nx, piece(o)]
        return rcopy(p, p, wx_s.at[d, o], wx_r.at[d, o], at(dx=1 if d == 0 else 3))

    def far_x(o, d, source_dx):
        nx = lax.rem(x + source_dx, RING)
        part = packs.at[c, nx, piece(o), pl.ds(0 if d == 0 else depth // 2, depth // 2)]
        return rcopy(part, part, wf_s.at[d, o], wf_r.at[d, o], at(dx=1 if d == 0 else 3))

    def across(dx):
        nx = lax.rem(x + dx, RING)
        slab = packs.at[c, nx]
        return rcopy(slab, slab, wc_s.at[dx], wc_r.at[dx], at(dc=1))

    def across_in(dx):
        nx = lax.rem(x + dx, RING)
        slab = packs.at[1 - c, nx]
        return rcopy(slab, slab, wc_s.at[dx], wc_r.at[dx], at(dc=1))

    for o in (1, 3, 2):
        go(wy[o])
    for d in (0, 1):
        go(along_x(0, d))
    go(x_right[1])
    go(x_left[1])
    for o in (1, 3, 2):
        from_y(o).wait_recv()
        for d in (0, 1):
            go(along_x(o, d))
    go(across(0))
    for o in (0, 1, 3, 2):
        for d in (0, 1):
            arrived_x(o, d).wait_recv()
            go(far_x(o, d, 3 if d == 0 else 1))
    go(across(3))
    go(across(1))
    cuts = ((0, 64), (64, 32))
    xg_in = lambda d, i: rcopy(
        xg.at[d, (lo, hi)[i if d == 0 else 1 - i]], xg.at[d, (lo, hi)[i if d == 0 else 1 - i]],
        xd_s.at[d, i], xd_r.at[d, i], at(dz=1 if d == 0 else 3),
    )

    def far_z(d, i):
        a, n = cuts[i]
        part = pl.ds(a + (0 if d == 0 else half), n)
        return rcopy(xg.at[d, part], xg.at[2, part], xf_s.at[d, i], xf_r.at[d, i], at(dz=1 if d == 0 else 3))

    def far_in(d, i):
        a, n = cuts[i]
        part = pl.ds(a + (0 if d == 0 else half), n)
        return rcopy(xg.at[2, part], xg.at[2, part], xf_s.at[d, i], xf_r.at[d, i], at(dz=1 if d == 0 else 3))

    for d in (0, 1):
        xg_in(d, 0).wait_recv()
        for i in (0, 1):
            go(far_z(d, i))
    for o in (0, 1, 3, 2):
        for d in (0, 1):
            far_x(o, d, 2).wait_recv()
    go(across(2))
    for dx in (0, 3, 1, 2):
        across_in(dx).wait_recv()

    for n in range(2 * RING):
        p = [packs[n % 2, n // 2, i] for i in range(RING)]
        at_rows = pl.ds(n * depth, depth)
        w_all[at_rows, 0:128] = jnp.concatenate([p[0][:, 0:64], p[1][:, 0:64]], axis=1)
        w_all[at_rows, 128:256] = jnp.concatenate([p[2][:, 0:64], p[3][:, 0:64]], axis=1)
        w_all[at_rows, 256:384] = jnp.concatenate(
            [t[:, 64:80] for t in p] + [t[:, 80:96] for t in p], axis=1
        )

    def chunk(n, source, first, count, stage_at, dz):
        wide = source.astype(F32)
        normed = (
            wide * lax.rsqrt(jnp.mean(wide * wide, axis=-1, keepdims=True) + EPS) * gain_ref[...]
        ).astype(BF16)
        out = jnp.dot(normed, w_all[...], preferred_element_type=F32).astype(BF16)
        v = out[:, 320:384]
        k = out[:, 256:320].reshape(count // 32, 2, 16, HEAD_DIM)
        here = pl.ds(stage_at, count)
        here_k = pl.ds(stage_at // 2, count // 2)
        for i in range(RING):
            stage_qv[i, here] = jnp.concatenate([out[:, i * 64 : i * 64 + 64], v], axis=1)
        stage_k[here_k] = jnp.concatenate([k[:, 0], k[:, 1]], axis=2).reshape(count // 2, 128)
        nz = lax.rem(z + dz, RING)

        def spot(dy, halved):
            ny = lax.rem(y + dy, RING)
            start = (nz * RING + ny) * rows + first
            if halved:
                return pl.ds(pl.multiple_of(lax.div(start, 2), 16), count // 2)
            return pl.ds(pl.multiple_of(start, 32), count)

        for o in (1, 3, 2):
            ny = lax.rem(y + o, RING)
            go(rcopy(stage_qv.at[ny, here], qv_ref.at[spot(0, False)], a_s.at[n, o], a_r.at[n, o], at(dy=o)))
            go(rcopy(stage_k.at[here_k], kk_ref.at[spot(0, True)], b_s.at[n, o], b_r.at[n, o], at(dy=o)))
        qv_ref[spot(0, False)] = stage_qv[y, here]
        kk_ref[spot(0, True)] = stage_k[here_k]
        waits = []
        for o in (1, 3, 2):
            s, t = qv_ref.at[spot(RING - o, False)], kk_ref.at[spot(RING - o, True)]
            waits.append(rcopy(s, s, a_s.at[n, o], a_r.at[n, o], at(dy=o)))
            waits.append(rcopy(t, t, b_s.at[n, o], b_r.at[n, o], at(dy=o)))
        return waits

    pending = chunk(0, x_ref[...], 0, rows, 0, 0)
    pending += chunk(1, xg[0, lo], 0, half, rows, 3)
    pending += chunk(2, xg[1, hi], half, half, rows + half, 1)
    xg_in(0, 1).wait_recv()
    pending += chunk(3, xg[0, hi], half, half, 2 * rows, 3)
    xg_in(1, 1).wait_recv()
    pending += chunk(4, xg[1, lo], 0, half, 2 * rows + half, 1)
    n, place = 5, 3 * rows
    for i in (0, 1):
        a, count = cuts[i]
        for d in (0, 1):
            far_in(d, i).wait_recv()
            first = a + (0 if d == 0 else half)
            pending += chunk(n, xg[2, pl.ds(first, count)], first, count, place, 2)
            n, place = n + 1, place + count
    for w in pending:
        w.wait_recv()
    for s in sent:
        s.wait_send()


def project(x, gain, wq, wk, wv):
    rows, width = x.shape
    length = rows * RING * RING
    depth = wq.shape[0]
    dma = pltpu.SemaphoreType.DMA
    vmem = pl.BlockSpec(memory_space=pltpu.VMEM)
    return pl.pallas_call(
        project_kernel,
        name="project",
        out_shape=(
            jax.ShapeDtypeStruct((length, 128), BF16),
            jax.ShapeDtypeStruct((length // 2, 128), BF16),
        ),
        in_specs=[vmem] * 5,
        out_specs=(vmem, vmem),
        scratch_shapes=[
            pltpu.VMEM((2, RING, RING, depth, 128), BF16),
            pltpu.VMEM((width, 384), BF16),
            pltpu.VMEM((3, rows, width), BF16),
            pltpu.VMEM((RING, RING * rows, 128), BF16),
            pltpu.VMEM((RING * rows // 2, 128), BF16),
            dma((4,)), dma((4,)), dma((2, 4)), dma((2, 4)), dma((2, 4)), dma((2, 4)), dma((4,)), dma((4,)),
            dma((2, 2)), dma((2, 2)), dma((2, 2)), dma((2, 2)),
            dma((9, 4)), dma((9, 4)), dma((9, 4)), dma((9, 4)),
        ],
        compiler_params=pltpu.CompilerParams(
            collective_id=0, has_side_effects=True, vmem_limit_bytes=48 << 20
        ),
    )(x, gain, wq, wk, wv)


BLOCK_Q = 768
BLOCK_K = 256


def attend_kernel(qv_ref, kk_ref, b_ref, g_ref, o_ref, keys_t, qa, vv, tri, acc, car):
    length = qv_ref.shape[0]
    r = lax.broadcasted_iota(jnp.int32, (BLOCK_K, BLOCK_K), 0)
    c = lax.broadcasted_iota(jnp.int32, (BLOCK_K, BLOCK_K), 1)
    tri[...] = jnp.where(r > c, 1.0, 0.0).astype(BF16)
    step = 512

    @pl.loop(0, length // step)
    def _(i):
        rows = pl.ds(pl.multiple_of(i * step, step), step)
        packed = kk_ref[pl.ds(pl.multiple_of(i * (step // 2), step // 2), step // 2), :]
        packed = packed.reshape(step // 32, 16, 128)
        k = jnp.concatenate([packed[:, :, 0:64], packed[:, :, 64:128]], axis=1).reshape(step, HEAD_DIM)
        kk = k.astype(F32) * (LOG2E / 8.0)
        hi = kk.astype(BF16)
        lo = (kk - hi.astype(F32)).astype(BF16)
        keys_t[0:128, rows] = jnp.concatenate([hi, lo], axis=1).T
        bb = b_ref[0:1, rows] * LOG2E
        bh = bb.astype(BF16)
        r1 = bb - bh.astype(F32)
        bm = r1.astype(BF16)
        bl = (r1 - bm.astype(F32)).astype(BF16)
        keys_t[128:144, rows] = jnp.concatenate([bh, bm, bl, jnp.zeros((13, step), BF16)], axis=0)
        both = qv_ref[rows, :]
        qq = both[:, 0:64]
        lane = lax.broadcasted_iota(jnp.int32, (step, 128), 1)
        qa[rows, 0:128] = jnp.concatenate([qq, qq], axis=1)
        qa[rows, 128:256] = jnp.where(lane < 3, 1.0, 0.0).astype(BF16)
        vv[rows, :] = both[:, 64:128]

    ratio = BLOCK_Q // BLOCK_K

    @pl.loop(0, length // BLOCK_Q)
    def _(i):
        rows = pl.ds(pl.multiple_of(i * BLOCK_Q, BLOCK_Q), BLOCK_Q)
        q = qa[rows, 0:144]

        def one(j, carry, diagonal=None):
            cols = pl.ds(pl.multiple_of(j * BLOCK_K, BLOCK_K), BLOCK_K)
            l2 = jnp.dot(q, keys_t[:, cols], preferred_element_type=F32)
            if diagonal is not None:
                t = lax.broadcasted_iota(jnp.int32, (BLOCK_Q, BLOCK_K), 0)
                s = lax.broadcasted_iota(jnp.int32, (BLOCK_Q, BLOCK_K), 1)
                l2 = jnp.where(s + diagonal < t, l2, -1e30)
            mx = jnp.maximum(l2, 0.0)
            mn = jnp.minimum(l2, 0.0)
            log_part = jnp.log2(1.0 + jnp.exp2(mn - mx))
            drop = (mx + log_part).astype(BF16)
            after = jnp.dot(drop, tri[...], preferred_element_type=F32)
            x = (mn - log_part) - after - jnp.concatenate([carry] * (BLOCK_K // 128), axis=1)
            sticks = jnp.exp2(x).astype(BF16)
            pv = jnp.dot(sticks, vv[cols, :], preferred_element_type=F32)
            whole = after[:, 0:1] + drop[:, 0:128].astype(F32)[:, 0:1]
            return pv, carry + jnp.broadcast_to(whole, carry.shape)

        carry = jnp.zeros((BLOCK_Q, 128), F32)
        total = jnp.zeros((BLOCK_Q, HEAD_DIM), F32)
        for d in reversed(range(ratio)):
            pv, carry = one(i * ratio + d, carry, d * BLOCK_K)
            total = total + pv
        acc[...] = total
        car[...] = carry
        full = i * ratio
        odd = lax.rem(full, 2)

        def single(n, _):
            pv, after = one(full - 1 - n, car[...])
            acc[...] += pv
            car[...] = after
            return 0

        lax.fori_loop(0, odd, single, 0)

        def double(n, _):
            base = full - 1 - odd - n * 2
            pv0, cc = one(base, car[...])
            pv1, cc = one(base - 1, cc)
            acc[...] += pv0 + pv1
            car[...] = cc
            return 0

        lax.fori_loop(0, lax.div(full, 2), double, 0)
        a = acc[...]
        scaled = a * lax.rsqrt(jnp.mean(a * a, axis=-1, keepdims=True) + EPS)
        o_ref[rows, :] = (scaled * g_ref[...]).astype(BF16)


def attend(qv, kk, bias, gain):
    length = qv.shape[0]
    vmem = pl.BlockSpec(memory_space=pltpu.VMEM)
    return pl.pallas_call(
        attend_kernel,
        name="attend",
        out_shape=jax.ShapeDtypeStruct((length, HEAD_DIM), BF16),
        in_specs=[vmem] * 4,
        out_specs=vmem,
        scratch_shapes=[
            pltpu.VMEM((144, length), BF16),
            pltpu.VMEM((length, 256), BF16),
            pltpu.VMEM((length, HEAD_DIM), BF16),
            pltpu.VMEM((BLOCK_K, BLOCK_K), BF16),
            pltpu.VMEM((BLOCK_Q, HEAD_DIM), F32),
            pltpu.VMEM((BLOCK_Q, 128), F32),
        ],
        compiler_params=pltpu.CompilerParams(vmem_limit_bytes=48 << 20),
    )(qv, kk, bias, gain)


def body(inputs, in_gain, w_query, w_key, w_value, key_bias, out_gain, w_out):
    rows = inputs.shape[1]
    width_sp = lax.axis_size("sp")
    own = lax.axis_index("sp")
    qv, kk = project(inputs[0], in_gain[None], w_query, w_key, w_value)
    gain = lax.dynamic_slice_in_dim(out_gain, own * HEAD_DIM, HEAD_DIM, 0)[None]
    head_out = attend(qv, kk, key_bias[0].T, gain)
    returned = lax.all_to_all(head_out, "sp", split_axis=0, concat_axis=1, tiled=True)
    w_out = lax.all_gather(w_out, "dp", axis=1, tiled=True)
    w_out = lax.all_gather(w_out, "sp", axis=0, tiled=True)
    mixed = jnp.dot(returned, w_out, preferred_element_type=F32)
    return mixed.astype(BF16)[None]


def solution(mesh):
    placed = (
        P("dp", "sp", None), P(), P("dp", "sp"), P("dp", "sp"), P("dp", "sp"),
        P("dp", None, "sp"), P(), P("sp", "dp"),
    )
    return jax.shard_map(body, mesh=mesh, in_specs=placed, out_specs=P("dp", "sp", None), check_vma=False)
```

```python
import functools

import jax
import jax.numpy as jnp
from jax import lax
from jax.experimental import pallas as pl
from jax.experimental.pallas import tpu as pltpu
from jax.sharding import PartitionSpec as P

HEAD_DIM = 64
RING = 4
EPS = 1e-06
LOG2E = 1.4426950408889634
F32 = jnp.float32
BF16 = jnp.bfloat16
MESH = pl.DeviceIdType.MESH


def rcopy(src, dst, send, recv, device):
    return pltpu.make_async_remote_copy(
        src_ref=src, dst_ref=dst, send_sem=send, recv_sem=recv, device_id=device, device_id_type=MESH
    )


def places():
    sp, dp = lax.axis_index("sp"), lax.axis_index("dp")
    z, y = lax.div(sp, RING), lax.rem(sp, RING)
    x, c = lax.div(dp, 2), lax.rem(dp, 2)

    def at(dz=0, dy=0, dx=0, dc=0):
        nz, ny = lax.rem(z + dz, RING), lax.rem(y + dy, RING)
        nx, nc = lax.rem(x + dx, RING), lax.rem(c + dc, 2)
        return {"sp": nz * RING + ny, "dp": nx * 2 + nc}

    return z, y, x, c, at


def project_kernel(
    x_ref, gain_ref, wq_ref, wk_ref, wv_ref, wo_in,
    qv_ref, kk_ref, wo_ref,
    packs, w_all, xg, stage_qv, stage_k,
    wy_s, wy_r, wx_s, wx_r, wf_s, wf_r, wc_s, wc_r, xd_s, xd_r, xf_s, xf_r, a_s, a_r, b_s, b_r,
    oz_s, oz_r, oy_s, oy_r, ox_s, ox_r, of_s, of_r, oc_s, oc_r, local_sem,
):
    z, y, x, c, at = places()
    rows = x_ref.shape[0]
    half = rows // 2
    depth = wq_ref.shape[1]
    qn, kn = wq_ref.shape[0], wk_ref.shape[0]
    piece_rows = qn + 2 * kn
    packs[c, x, y] = jnp.concatenate([wq_ref[...], wk_ref[...], wv_ref[...]], axis=0)
    friends = [at(dz=1), at(dz=3), at(dy=1), at(dy=2), at(dy=3), at(dx=1), at(dx=3), at(dc=1)]
    barrier = pltpu.get_barrier_semaphore()
    for f in friends:
        pl.semaphore_signal(barrier, inc=1, device_id=f, device_id_type=MESH)

    def wo_cols(dx, cc):
        return pl.ds(pl.multiple_of((lax.rem(x + dx, RING) * 2 + cc) * depth, depth), depth)

    own_wo = pltpu.make_async_copy(wo_in, wo_ref.at[y, z, :, wo_cols(0, c)], local_sem)
    own_wo.start()
    pl.semaphore_wait(barrier, len(friends))

    sent = []

    def go(copy):
        copy.start()
        sent.append(copy)

    def near(d, axis):
        return at(**{axis: 1 if d == 0 else 3})

    def back(d):
        return 3 if d == 0 else 1

    lo, hi = pl.ds(0, half), pl.ds(half, half)
    halves = (lo, hi)

    def oz(dz, n):
        return wo_ref.at[y, lax.rem(z + dz, RING), n, wo_cols(0, c)]

    every, top, low = pl.ds(0, 64), pl.ds(0, 32), pl.ds(32, 32)
    go_oz = [rcopy(wo_in, oz(0, every), oz_s.at[d, 0], oz_r.at[d, 0], near(d, "dz")) for d in (0, 1)]

    def oz_in(d):
        s = oz(back(d), every)
        return rcopy(s, s, oz_s.at[d, 0], oz_r.at[d, 0], near(d, "dz"))

    def oz_far(d, dz):
        s = oz(dz, top if d == 0 else low)
        return rcopy(s, s, oz_s.at[d, 1], oz_r.at[d, 1], near(d, "dz"))

    def x_out(d, i):
        p = halves[i if d == 0 else 1 - i]
        return rcopy(x_ref.at[p], xg.at[d, p], xd_s.at[d, i], xd_r.at[d, i], near(d, "dz"))

    def x_in(d, i):
        p = halves[i if d == 0 else 1 - i]
        return rcopy(xg.at[d, p], xg.at[d, p], xd_s.at[d, i], xd_r.at[d, i], near(d, "dz"))

    cuts = ((0, 64), (64, 32))

    def far_z(d, i, arrived):
        a, n = cuts[i]
        part = pl.ds(a + (0 if d == 0 else half), n)
        return rcopy(xg.at[2 if arrived else d, part], xg.at[2, part], xf_s.at[d, i], xf_r.at[d, i], near(d, "dz"))

    def piece(o):
        return lax.rem(y + RING - o, RING)

    def w_y(o, arrived):
        p = packs.at[c, x, piece(o) if arrived else y]
        return rcopy(p, p, wy_s.at[o], wy_r.at[o], at(dy=o))

    def w_x(o, d, arrived):
        p = packs.at[c, lax.rem(x + back(d), RING) if arrived else x, piece(o)]
        return rcopy(p, p, wx_s.at[d, o], wx_r.at[d, o], near(d, "dx"))

    def w_far(o, d, dx):
        part = packs.at[c, lax.rem(x + dx, RING), piece(o), pl.ds(0 if d == 0 else piece_rows // 2, piece_rows // 2)]
        return rcopy(part, part, wf_s.at[d, o], wf_r.at[d, o], near(d, "dx"))

    def w_c(dx, arrived):
        slab = packs.at[1 - c if arrived else c, lax.rem(x + dx, RING)]
        return rcopy(slab, slab, wc_s.at[dx], wc_r.at[dx], at(dc=1))

    def oy(d, arrived):
        s = wo_ref.at[lax.rem(y + back(d), RING) if arrived else y, :, :, wo_cols(0, c)]
        return rcopy(s, s, oy_s.at[d, 0], oy_r.at[d, 0], near(d, "dy"))

    def oy_far(d, dy):
        s = wo_ref.at[lax.rem(y + dy, RING), pl.ds(0 if d == 0 else 2, 2), :, wo_cols(0, c)]
        return rcopy(s, s, oy_s.at[d, 1], oy_r.at[d, 1], near(d, "dy"))

    def ox(o, d, arrived):
        s = wo_ref.at[piece(o), :, :, wo_cols(back(d) if arrived else 0, c)]
        return rcopy(s, s, ox_s.at[d, o], ox_r.at[d, o], near(d, "dx"))

    def ox_far(o, d, dx):
        s = wo_ref.at[piece(o), pl.ds(0 if d == 0 else 2, 2), :, wo_cols(dx, c)]
        return rcopy(s, s, of_s.at[d, o], of_r.at[d, o], near(d, "dx"))

    def oc(dx, arrived):
        s = wo_ref.at[:, :, :, wo_cols(dx, 1 - c if arrived else c)]
        return rcopy(s, s, oc_s.at[dx], oc_r.at[dx], at(dc=1))

    with jax.named_scope("issue"):
        for o in (1, 3, 2):
            go(w_y(o, False))
        for d in (0, 1):
            go(w_x(0, d, False))
        for d in (0, 1):
            go(go_oz[d])
        for i in (0, 1):
            for d in (0, 1):
                go(x_out(d, i))
    with jax.named_scope("wait_wy"):
        for o in (1, 3, 2):
            w_y(o, True).wait_recv()
            for d in (0, 1):
                go(w_x(o, d, False))
        go(w_c(0, False))
    with jax.named_scope("wait_oz"):
        own_wo.wait()
        for d in (0, 1):
            oz_in(d).wait_recv()
            go(oz_far(d, back(d)))
    with jax.named_scope("wait_wx"):
        for o in (0, 1, 3, 2):
            for d in (0, 1):
                w_x(o, d, True).wait_recv()
                go(w_far(o, d, back(d)))
        go(w_c(3, False))
        go(w_c(1, False))
    with jax.named_scope("wait_ozfar"):
        for d in (0, 1):
            oz_far(d, 2).wait_recv()
        for d in (0, 1):
            go(oy(d, False))
            go(ox(0, d, False))
    with jax.named_scope("wait_wfar"):
        for o in (0, 1, 3, 2):
            for d in (0, 1):
                w_far(o, d, 2).wait_recv()
        go(w_c(2, False))
    with jax.named_scope("wait_x0"):
        for d in (0, 1):
            x_in(d, 0).wait_recv()
            for i in (0, 1):
                go(far_z(d, i, False))
    with jax.named_scope("wait_wc"):
        for dx in (0, 3, 1, 2):
            w_c(dx, True).wait_recv()

    with jax.named_scope("assemble"):
        for n in range(2 * RING):
            cols = pl.ds(n * depth, depth)
            for i in range(RING):
                p = packs[n % 2, n // 2, i]
                w_all[i * qn : (i + 1) * qn, cols] = p[0:qn]
                w_all[RING * qn + i * kn : RING * qn + (i + 1) * kn, cols] = p[qn : qn + kn]
                w_all[RING * (qn + kn) + i * kn : RING * (qn + kn) + (i + 1) * kn, cols] = p[qn + kn :]

    def chunk(n, source, first, count, stage_at, dz):
        wide = source.astype(F32)
        normed = (
            wide * lax.rsqrt(jnp.mean(wide * wide, axis=-1, keepdims=True) + EPS) * gain_ref[...]
        ).astype(BF16)
        out = lax.dot_general(
            normed, w_all[...], (((1,), (1,)), ((), ())), preferred_element_type=F32
        ).astype(BF16)
        v = out[:, 320:384]
        k = out[:, 256:320].reshape(count // 32, 2, 16, HEAD_DIM)
        here = pl.ds(stage_at, count)
        here_k = pl.ds(stage_at // 2, count // 2)
        for i in range(RING):
            stage_qv[i, here] = jnp.concatenate([out[:, i * 64 : i * 64 + 64], v], axis=1)
        stage_k[here_k] = jnp.concatenate([k[:, 0], k[:, 1]], axis=2).reshape(count // 2, 128)
        nz = lax.rem(z + dz, RING)

        def spot(dy, halved):
            ny = lax.rem(y + dy, RING)
            start = (nz * RING + ny) * rows + first
            if halved:
                return pl.ds(pl.multiple_of(lax.div(start, 2), 16), count // 2)
            return pl.ds(pl.multiple_of(start, 32), count)

        for o in (1, 3, 2):
            ny = lax.rem(y + o, RING)
            go(rcopy(stage_qv.at[ny, here], qv_ref.at[spot(0, False)], a_s.at[n, o], a_r.at[n, o], at(dy=o)))
            go(rcopy(stage_k.at[here_k], kk_ref.at[spot(0, True)], b_s.at[n, o], b_r.at[n, o], at(dy=o)))
        qv_ref[spot(0, False)] = stage_qv[y, here]
        kk_ref[spot(0, True)] = stage_k[here_k]
        waits = []
        for o in (1, 3, 2):
            s, t = qv_ref.at[spot(RING - o, False)], kk_ref.at[spot(RING - o, True)]
            waits.append(rcopy(s, s, a_s.at[n, o], a_r.at[n, o], at(dy=o)))
            waits.append(rcopy(t, t, b_s.at[n, o], b_r.at[n, o], at(dy=o)))
        return waits

    with jax.named_scope("chunk012"):
        pending = chunk(0, x_ref[...], 0, rows, 0, 0)
        pending += chunk(1, xg[0, lo], 0, half, rows, 3)
        pending += chunk(2, xg[1, hi], half, half, rows + half, 1)
    with jax.named_scope("wait_oy"):
        for d in (0, 1):
            oy(d, True).wait_recv()
            go(oy_far(d, back(d)))
        for o in (1, 3):
            for d in (0, 1):
                go(ox(o, d, False))
    with jax.named_scope("wait_oyfar"):
        for d in (0, 1):
            oy_far(d, 2).wait_recv()
        for d in (0, 1):
            go(ox(2, d, False))
        go(oc(0, False))
    with jax.named_scope("wait_x1"):
        x_in(0, 1).wait_recv()
        pending += chunk(3, xg[0, hi], half, half, 2 * rows, 3)
        x_in(1, 1).wait_recv()
        pending += chunk(4, xg[1, lo], 0, half, 2 * rows + half, 1)
    with jax.named_scope("wait_ox"):
        for o in (0, 1, 3):
            for d in (0, 1):
                ox(o, d, True).wait_recv()
                go(ox_far(o, d, back(d)))
    n, place = 5, 3 * rows
    for i in (0, 1):
        a, count = cuts[i]
        for d in (0, 1):
            with jax.named_scope("wait_far%d%d" % (i, d)):
                far_z(d, i, True).wait_recv()
                first = a + (0 if d == 0 else half)
                pending += chunk(n, xg[2, pl.ds(first, count)], first, count, place, 2)
                n, place = n + 1, place + count
        if i == 0:
            with jax.named_scope("wait_ox2"):
                for d in (0, 1):
                    ox(2, d, True).wait_recv()
                    go(ox_far(2, d, back(d)))
                go(oc(3, False))
                go(oc(1, False))
    with jax.named_scope("wait_oxfar"):
        for o in (0, 1, 3, 2):
            for d in (0, 1):
                ox_far(o, d, 2).wait_recv()
        go(oc(2, False))
    with jax.named_scope("wait_qkv"):
        for w in pending:
            w.wait_recv()
    with jax.named_scope("wait_oc"):
        for dx in (0, 3, 1, 2):
            oc(dx, True).wait_recv()
    with jax.named_scope("wait_send"):
        for s in sent:
            s.wait_send()


def project(x, gain, wq, wk, wv, wo):
    rows, width = x.shape
    length = rows * RING * RING
    depth = wq.shape[1]
    dma = pltpu.SemaphoreType.DMA
    vmem = pl.BlockSpec(memory_space=pltpu.VMEM)
    return pl.pallas_call(
        project_kernel,
        name="project",
        out_shape=(
            jax.ShapeDtypeStruct((length, 128), BF16),
            jax.ShapeDtypeStruct((length // 2, 128), BF16),
            jax.ShapeDtypeStruct((RING, RING, wo.shape[0], wo.shape[1] * 2 * RING), BF16),
        ),
        in_specs=[vmem] * 6,
        out_specs=(vmem, vmem, vmem),
        scratch_shapes=[
            pltpu.VMEM((2, RING, RING, 96, depth), BF16),
            pltpu.VMEM((384, width), BF16),
            pltpu.VMEM((3, rows, width), BF16),
            pltpu.VMEM((RING, RING * rows, 128), BF16),
            pltpu.VMEM((RING * rows // 2, 128), BF16),
            dma((4,)), dma((4,)), dma((2, 4)), dma((2, 4)), dma((2, 4)), dma((2, 4)), dma((4,)), dma((4,)),
            dma((2, 2)), dma((2, 2)), dma((2, 2)), dma((2, 2)),
            dma((9, 4)), dma((9, 4)), dma((9, 4)), dma((9, 4)),
            dma((2, 2)), dma((2, 2)), dma((2, 2)), dma((2, 2)), dma((2, 4)), dma((2, 4)),
            dma((2, 4)), dma((2, 4)), dma((4,)), dma((4,)), dma(()),
        ],
        compiler_params=pltpu.CompilerParams(
            collective_id=0, has_side_effects=True, vmem_limit_bytes=48 << 20
        ),
    )(x, gain, wq, wk, wv, wo)


BLOCK_Q = 768
BLOCK_K = 256


def attend_kernel(
    qv_ref, kk_ref, b_ref, g_ref, ho_ref, keys_t, qa, vv, tri, acc, car, stage, h_s, h_r
):
    length = qv_ref.shape[0]
    rows_each = length // (RING * RING)
    z, y, x, c, at = places()
    me = z * RING + y
    barrier = pltpu.get_barrier_semaphore()
    for dz in range(RING):
        for dy in range(RING):
            if dz or dy:
                pl.semaphore_signal(barrier, inc=1, device_id=at(dz=dz, dy=dy), device_id_type=MESH)
    r = lax.broadcasted_iota(jnp.int32, (BLOCK_K, BLOCK_K), 0)
    c = lax.broadcasted_iota(jnp.int32, (BLOCK_K, BLOCK_K), 1)
    tri[...] = jnp.where(r > c, 1.0, 0.0).astype(BF16)
    step = 512

    @pl.loop(0, length // step)
    def _(i):
        rows = pl.ds(pl.multiple_of(i * step, step), step)
        packed = kk_ref[pl.ds(pl.multiple_of(i * (step // 2), step // 2), step // 2), :]
        packed = packed.reshape(step // 32, 16, 128)
        k = jnp.concatenate([packed[:, :, 0:64], packed[:, :, 64:128]], axis=1).reshape(step, HEAD_DIM)
        kk = k.astype(F32) * (LOG2E / 8.0)
        hi = kk.astype(BF16)
        lo = (kk - hi.astype(F32)).astype(BF16)
        keys_t[0:128, rows] = jnp.concatenate([hi, lo], axis=1).T
        bb = b_ref[0:1, rows] * LOG2E
        bh = bb.astype(BF16)
        r1 = bb - bh.astype(F32)
        bm = r1.astype(BF16)
        bl = (r1 - bm.astype(F32)).astype(BF16)
        keys_t[128:144, rows] = jnp.concatenate([bh, bm, bl, jnp.zeros((13, step), BF16)], axis=0)
        both = qv_ref[rows, :]
        qq = both[:, 0:64]
        lane = lax.broadcasted_iota(jnp.int32, (step, 128), 1)
        qa[rows, 0:128] = jnp.concatenate([qq, qq], axis=1)
        qa[rows, 128:256] = jnp.where(lane < 3, 1.0, 0.0).astype(BF16)
        vv[rows, :] = both[:, 64:128]

    pl.semaphore_wait(barrier, RING * RING - 1)
    ratio = BLOCK_Q // BLOCK_K

    @pl.loop(0, length // BLOCK_Q)
    def _(i):
        rows = pl.ds(pl.multiple_of(i * BLOCK_Q, BLOCK_Q), BLOCK_Q)
        q = qa[rows, 0:144]

        def one(q, j, carry, diagonal=False):
            count = q.shape[0]
            cols = pl.ds(pl.multiple_of(j * BLOCK_K, BLOCK_K), BLOCK_K)
            l2 = jnp.dot(q, keys_t[:, cols], preferred_element_type=F32)
            if diagonal:
                t = lax.broadcasted_iota(jnp.int32, (BLOCK_K, BLOCK_K), 0)
                s = lax.broadcasted_iota(jnp.int32, (BLOCK_K, BLOCK_K), 1)
                first = jnp.where(s < t, l2[0:BLOCK_K], -1e30)
                l2 = first if count == BLOCK_K else jnp.concatenate([first, l2[BLOCK_K:]], axis=0)
            mx = jnp.maximum(l2, 0.0)
            mn = jnp.minimum(l2, 0.0)
            log_part = jnp.log2(1.0 + jnp.exp2(mn - mx))
            drop = (mx + log_part).astype(BF16)
            after = jnp.dot(drop, tri[...], preferred_element_type=F32)
            x = (mn - log_part) - after - jnp.concatenate([carry] * (BLOCK_K // 128), axis=1)
            sticks = jnp.exp2(x).astype(BF16)
            pv = jnp.dot(sticks, vv[cols, :], preferred_element_type=F32)
            whole = after[:, 0:1] + drop[:, 0:128].astype(F32)[:, 0:1]
            return pv, carry + jnp.broadcast_to(whole, carry.shape)

        carry = None
        total = None
        for d in reversed(range(ratio)):
            fresh = jnp.zeros((BLOCK_K, 128), F32)
            carry = fresh if carry is None else jnp.concatenate([fresh, carry], axis=0)
            pv, carry = one(q[d * BLOCK_K :], i * ratio + d, carry, True)
            if total is None:
                total = pv
            else:
                total = jnp.concatenate([pv[:BLOCK_K], pv[BLOCK_K:] + total], axis=0)
        acc[...] = total
        car[...] = carry

        def several(n, _):
            base = i * ratio - 1 - n * ratio
            cc, a = car[...], acc[...]
            for u in range(ratio):
                pv, cc = one(q, base - u, cc)
                a = a + pv
            acc[...] = a
            car[...] = cc
            return 0

        lax.fori_loop(0, i, several, 0)
        a = acc[...]
        scaled = a * lax.rsqrt(jnp.mean(a * a, axis=-1, keepdims=True) + EPS)
        head = (scaled * g_ref[...]).astype(BF16)
        for yy in range(RING):
            part = head[yy * rows_each : (yy + 1) * rows_each]
            half = rows_each // 2
            stage[i * RING + yy] = jnp.concatenate([part[:half], part[half:]], axis=1)
        for yy in range(RING):
            dest = i * RING + yy

            @pl.when(dest != me)
            def _():
                rcopy(
                    stage.at[dest], ho_ref.at[y * RING + z], h_s.at[dest], h_r.at[me],
                    {"sp": dest, "dp": lax.axis_index("dp")},
                ).start()

            @pl.when(dest == me)
            def _():
                ho_ref[y * RING + z] = stage[dest]

    for dz in range(RING):
        for dy in range(RING):
            if dz or dy:
                nz, ny = lax.rem(z + dz, RING), lax.rem(y + dy, RING)
                other = nz * RING + ny
                slot = ho_ref.at[ny * RING + nz]
                w = rcopy(slot, slot, h_s.at[other], h_r.at[other], at(dz=dz, dy=dy))
                w.wait_recv()
                w.wait_send()


def attend(qv, kk, bias, gain):
    length = qv.shape[0]
    each = length // (RING * RING)
    vmem = pl.BlockSpec(memory_space=pltpu.VMEM)
    dma = pltpu.SemaphoreType.DMA
    return pl.pallas_call(
        attend_kernel,
        name="attend",
        out_shape=jax.ShapeDtypeStruct((RING * RING, each // 2, 2 * HEAD_DIM), BF16),
        in_specs=[vmem] * 4,
        out_specs=vmem,
        scratch_shapes=[
            pltpu.VMEM((144, length), BF16),
            pltpu.VMEM((length, 256), BF16),
            pltpu.VMEM((length, HEAD_DIM), BF16),
            pltpu.VMEM((BLOCK_K, BLOCK_K), BF16),
            pltpu.VMEM((BLOCK_Q, HEAD_DIM), F32),
            pltpu.VMEM((BLOCK_Q, 128), F32),
            pltpu.VMEM((RING * RING, each // 2, 2 * HEAD_DIM), BF16),
            dma((RING * RING,)), dma((RING * RING,)),
        ],
        compiler_params=pltpu.CompilerParams(
            collective_id=1, has_side_effects=True, vmem_limit_bytes=48 << 20
        ),
    )(qv, kk, bias, gain)


def mix_kernel(ho_ref, wo_ref, o_ref, lhs):
    heads, half, _ = ho_ref.shape
    for n in range(0, heads, 2):
        a, b = ho_ref[n], ho_ref[n + 1]
        cols = pl.ds(n * HEAD_DIM, 2 * HEAD_DIM)
        lhs[0:half, cols] = jnp.concatenate([a[:, 0:64], b[:, 0:64]], axis=1)
        lhs[half : 2 * half, cols] = jnp.concatenate([a[:, 64:128], b[:, 64:128]], axis=1)
    width = o_ref.shape[1]
    for n in range(0, width, 512):
        o_ref[:, n : n + 512] = jnp.dot(
            lhs[...], wo_ref[:, n : n + 512], preferred_element_type=F32
        ).astype(BF16)


def mix(ho, wo):
    heads, half, _ = ho.shape
    vmem = pl.BlockSpec(memory_space=pltpu.VMEM)
    return pl.pallas_call(
        mix_kernel,
        name="mix",
        out_shape=jax.ShapeDtypeStruct((2 * half, wo.shape[1]), BF16),
        in_specs=[vmem] * 2,
        out_specs=vmem,
        scratch_shapes=[pltpu.VMEM((2 * half, heads * HEAD_DIM), BF16)],
        compiler_params=pltpu.CompilerParams(vmem_limit_bytes=48 << 20),
    )(ho, wo)


def body(inputs, in_gain, w_query, w_key, w_value, key_bias, out_gain, w_out):
    own = lax.axis_index("sp")
    qv, kk, wo = project(inputs[0], in_gain[None], w_query.T, w_key.T, w_value.T, w_out)
    gain = lax.dynamic_slice_in_dim(out_gain, own * HEAD_DIM, HEAD_DIM, 0)[None]
    ho = attend(qv, kk, key_bias[0].T, gain)
    return mix(ho, wo.reshape(-1, wo.shape[-1]))[None]


def solution(mesh):
    placed = (
        P("dp", "sp", None), P(), P("dp", "sp"), P("dp", "sp"), P("dp", "sp"),
        P("dp", None, "sp"), P(), P("sp", "dp"),
    )
    return jax.shard_map(body, mesh=mesh, in_specs=placed, out_specs=P("dp", "sp", None), check_vma=False)
```

```python
import functools

import jax
import jax.numpy as jnp
from jax import lax
from jax.experimental import pallas as pl
from jax.experimental.pallas import tpu as pltpu
from jax.sharding import PartitionSpec as P

HEAD_DIM = 64
RING = 4
EPS = 1e-06
LOG2E = 1.4426950408889634
F32 = jnp.float32
BF16 = jnp.bfloat16
MESH = pl.DeviceIdType.MESH


def rcopy(src, dst, send, recv, device):
    return pltpu.make_async_remote_copy(
        src_ref=src, dst_ref=dst, send_sem=send, recv_sem=recv, device_id=device, device_id_type=MESH
    )


def places():
    sp, dp = lax.axis_index("sp"), lax.axis_index("dp")
    z, y = lax.div(sp, RING), lax.rem(sp, RING)
    x, c = lax.div(dp, 2), lax.rem(dp, 2)

    def at(dz=0, dy=0, dx=0, dc=0):
        nz, ny = lax.rem(z + dz, RING), lax.rem(y + dy, RING)
        nx, nc = lax.rem(x + dx, RING), lax.rem(c + dc, 2)
        return {"sp": nz * RING + ny, "dp": nx * 2 + nc}

    return z, y, x, c, at


def project_kernel(
    x_hbm, gain_hbm, wq_hbm, wk_hbm, wv_hbm, wo_hbm,
    qv_ref, kk_ref, wo_ref,
    packs, w_all, xg, stage_qv, stage_k,
    wy_s, wy_r, wx_s, wx_r, wf_s, wf_r, wc_s, wc_r, xd_s, xd_r, xf_s, xf_r, a_s, a_r, b_s, b_r,
    oz_s, oz_r, oy_s, oy_r, ox_s, ox_r, of_s, of_r, oc_s, oc_r, local_sem,
    x_ref, gain_ref, wq_ref, wk_ref, wv_ref, wo_in,
):
    z, y, x, c, at = places()
    loads = [
        pltpu.make_async_copy(s, d, local_sem.at[i])
        for i, (s, d) in enumerate(
            (
                (wq_hbm, wq_ref), (wk_hbm, wk_ref), (wv_hbm, wv_ref), (wo_hbm, wo_in),
                (gain_hbm, gain_ref), (x_hbm, x_ref),
            )
        )
    ]
    for load in loads:
        load.start()
    friends = [at(dz=1), at(dz=2), at(dz=3), at(dy=1), at(dy=2), at(dy=3), at(dx=1), at(dx=3), at(dc=1)]
    barrier = pltpu.get_barrier_semaphore()
    for f in friends:
        pl.semaphore_signal(barrier, inc=1, device_id=f, device_id_type=MESH)
    for load in loads:
        load.wait()
    rows = x_ref.shape[0]
    half = rows // 2
    depth = wq_ref.shape[1]
    qn, kn = wq_ref.shape[0], wk_ref.shape[0]
    piece_rows = qn + 2 * kn
    packs[c, x, y] = jnp.concatenate([wq_ref[...], wk_ref[...], wv_ref[...]], axis=0)

    def wo_cols(dx, cc):
        return pl.ds(pl.multiple_of((lax.rem(x + dx, RING) * 2 + cc) * depth, depth), depth)

    wo_ref[y, z, :, wo_cols(0, c)] = wo_in[...]
    pl.semaphore_wait(barrier, len(friends))

    sent = []

    def go(copy):
        copy.start()
        sent.append(copy)

    def near(d, axis):
        return at(**{axis: 1 if d == 0 else 3})

    def back(d):
        return 3 if d == 0 else 1

    lo, hi = pl.ds(0, half), pl.ds(half, half)
    halves = (lo, hi)

    def oz(dz, n):
        return wo_ref.at[y, lax.rem(z + dz, RING), n, wo_cols(0, c)]

    every = slice(None)

    def oz_out(dz):
        return rcopy(wo_in, oz(0, every), oz_s.at[dz], oz_r.at[dz], at(dz=dz))

    def oz_in(dz):
        s = oz(RING - dz, every)
        return rcopy(s, s, oz_s.at[dz], oz_r.at[dz], at(dz=dz))

    def x_out(d, i):
        p = halves[i if d == 0 else 1 - i]
        return rcopy(x_ref.at[p], xg.at[d, p], xd_s.at[d, i], xd_r.at[d, i], near(d, "dz"))

    def x_in(d, i):
        p = halves[i if d == 0 else 1 - i]
        return rcopy(xg.at[d, p], xg.at[d, p], xd_s.at[d, i], xd_r.at[d, i], near(d, "dz"))

    cuts = ((0, 64), (64, 32))

    def far_z(d, i, arrived):
        a, n = cuts[i]
        part = pl.ds(a + (0 if d == 0 else half), n)
        return rcopy(xg.at[2 if arrived else d, part], xg.at[2, part], xf_s.at[d, i], xf_r.at[d, i], near(d, "dz"))

    def piece(o):
        return lax.rem(y + RING - o, RING)

    def w_y(o, arrived):
        p = packs.at[c, x, piece(o) if arrived else y]
        return rcopy(p, p, wy_s.at[o], wy_r.at[o], at(dy=o))

    def w_x(o, d, arrived):
        p = packs.at[c, lax.rem(x + back(d), RING) if arrived else x, piece(o)]
        return rcopy(p, p, wx_s.at[d, o], wx_r.at[d, o], near(d, "dx"))

    def w_far(o, d, dx):
        part = packs.at[c, lax.rem(x + dx, RING), piece(o), pl.ds(0 if d == 0 else piece_rows // 2, piece_rows // 2)]
        return rcopy(part, part, wf_s.at[d, o], wf_r.at[d, o], near(d, "dx"))

    def w_c(dx, arrived):
        slab = packs.at[1 - c if arrived else c, lax.rem(x + dx, RING)]
        return rcopy(slab, slab, wc_s.at[dx], wc_r.at[dx], at(dc=1))

    def oy(d, arrived):
        s = wo_ref.at[lax.rem(y + back(d), RING) if arrived else y, :, :, wo_cols(0, c)]
        return rcopy(s, s, oy_s.at[d, 0], oy_r.at[d, 0], near(d, "dy"))

    def oy_far(d, dy):
        s = wo_ref.at[lax.rem(y + dy, RING), pl.ds(0 if d == 0 else 2, 2), :, wo_cols(0, c)]
        return rcopy(s, s, oy_s.at[d, 1], oy_r.at[d, 1], near(d, "dy"))

    def ox(o, d, arrived):
        s = wo_ref.at[piece(o), :, :, wo_cols(back(d) if arrived else 0, c)]
        return rcopy(s, s, ox_s.at[d, o], ox_r.at[d, o], near(d, "dx"))

    def ox_far(o, d, dx):
        s = wo_ref.at[piece(o), pl.ds(0 if d == 0 else 2, 2), :, wo_cols(dx, c)]
        return rcopy(s, s, of_s.at[d, o], of_r.at[d, o], near(d, "dx"))

    def oc(dx, arrived):
        s = wo_ref.at[:, :, :, wo_cols(dx, 1 - c if arrived else c)]
        return rcopy(s, s, oc_s.at[dx], oc_r.at[dx], at(dc=1))

    with jax.named_scope("issue"):
        for o in (1, 3, 2):
            go(w_y(o, False))
        for d in (0, 1):
            go(w_x(0, d, False))
        for dz in (2, 1, 3):
            go(oz_out(dz))
        for i in (0, 1):
            for d in (0, 1):
                go(x_out(d, i))
    with jax.named_scope("wait_wy"):
        for o in (1, 3, 2):
            w_y(o, True).wait_recv()
            for d in (0, 1):
                go(w_x(o, d, False))
        go(w_c(0, False))
    with jax.named_scope("wait_oz"):
        for dz in (1, 3, 2):
            oz_in(dz).wait_recv()
        for d in (0, 1):
            go(oy(d, False))
    with jax.named_scope("wait_wx"):
        for o in (0, 1, 3, 2):
            for d in (0, 1):
                w_x(o, d, True).wait_recv()
                go(w_far(o, d, back(d)))
        go(w_c(3, False))
        go(w_c(1, False))
        for d in (0, 1):
            go(ox(0, d, False))
    with jax.named_scope("wait_oy"):
        for d in (0, 1):
            oy(d, True).wait_recv()
            go(oy_far(d, back(d)))
        for o in (1, 3):
            for d in (0, 1):
                go(ox(o, d, False))
    with jax.named_scope("wait_wfar"):
        for o in (0, 1, 3, 2):
            for d in (0, 1):
                w_far(o, d, 2).wait_recv()
        go(w_c(2, False))
    with jax.named_scope("wait_x0"):
        for d in (0, 1):
            x_in(d, 0).wait_recv()
            for i in (0, 1):
                go(far_z(d, i, False))
    with jax.named_scope("wait_oyfar"):
        for d in (0, 1):
            oy_far(d, 2).wait_recv()
        for d in (0, 1):
            go(ox(2, d, False))
        go(oc(0, False))
    with jax.named_scope("wait_wc"):
        for dx in (0, 3, 1, 2):
            w_c(dx, True).wait_recv()

    with jax.named_scope("assemble"):
        for n in range(2 * RING):
            p = [packs[n % 2, n // 2, i] for i in range(RING)]
            w_all[n * depth : (n + 1) * depth, :] = jnp.concatenate(
                [t[0:qn] for t in p] + [t[qn : qn + kn] for t in p] + [t[qn + kn :] for t in p], axis=0
            ).T

    def chunk(n, source, segments, stage_at):
        wide = source.astype(F32)
        normed = (
            wide * lax.rsqrt(jnp.mean(wide * wide, axis=-1, keepdims=True) + EPS) * gain_ref[...]
        ).astype(BF16)
        out = jnp.dot(normed, w_all[...], preferred_element_type=F32).astype(BF16)
        total = out.shape[0]
        v = out[:, 320:384]
        k = out[:, 256:320].reshape(total // 32, 2, 16, HEAD_DIM)
        for i in range(RING):
            stage_qv[i, pl.ds(stage_at, total)] = jnp.concatenate([out[:, i * 64 : i * 64 + 64], v], axis=1)
        stage_k[pl.ds(stage_at // 2, total // 2)] = jnp.concatenate([k[:, 0], k[:, 1]], axis=2).reshape(
            total // 2, 128
        )
        waits = []
        for dz, first, count in segments:
            here, here_k = pl.ds(stage_at, count), pl.ds(stage_at // 2, count // 2)
            nz = lax.rem(z + dz, RING)

            def spot(dy, halved):
                start = (nz * RING + lax.rem(y + dy, RING)) * rows + first
                if halved:
                    return pl.ds(pl.multiple_of(lax.div(start, 2), 16), count // 2)
                return pl.ds(pl.multiple_of(start, 32), count)

            for o in (2, 1, 3):
                ny = lax.rem(y + o, RING)
                go(rcopy(stage_qv.at[ny, here], qv_ref.at[spot(0, False)], a_s.at[n, o], a_r.at[n, o], at(dy=o)))
                go(rcopy(stage_k.at[here_k], kk_ref.at[spot(0, True)], b_s.at[n, o], b_r.at[n, o], at(dy=o)))
            qv_ref[spot(0, False)] = stage_qv[y, here]
            kk_ref[spot(0, True)] = stage_k[here_k]
            for o in (1, 3, 2):
                s, t = qv_ref.at[spot(RING - o, False)], kk_ref.at[spot(RING - o, True)]
                waits.append(rcopy(s, s, a_s.at[n, o], a_r.at[n, o], at(dy=o)))
                waits.append(rcopy(t, t, b_s.at[n, o], b_r.at[n, o], at(dy=o)))
            n, stage_at = n + 1, stage_at + count
        return waits

    with jax.named_scope("chunk012"):
        pending = chunk(0, x_ref[...], ((0, 0, rows),), 0)
        pending += chunk(
            1, jnp.concatenate([xg[0, lo], xg[1, hi]], axis=0), ((3, 0, half), (1, half, half)), rows
        )
    with jax.named_scope("wait_ox"):
        for o in (0, 1, 3):
            for d in (0, 1):
                ox(o, d, True).wait_recv()
                go(ox_far(o, d, back(d)))
    with jax.named_scope("wait_x1"):
        x_in(0, 1).wait_recv()
        x_in(1, 1).wait_recv()
        pending += chunk(
            3, jnp.concatenate([xg[0, hi], xg[1, lo]], axis=0), ((3, half, half), (1, 0, half)), 2 * rows
        )
    with jax.named_scope("wait_ox2"):
        for d in (0, 1):
            ox(2, d, True).wait_recv()
            go(ox_far(2, d, back(d)))
        go(oc(3, False))
        go(oc(1, False))
    place = 3 * rows
    for i in (0, 1):
        a, count = cuts[i]
        with jax.named_scope("wait_far%d" % i):
            for d in (0, 1):
                far_z(d, i, True).wait_recv()
        with jax.named_scope("chunk_far%d" % i):
            pending += chunk(
                5 + 2 * i,
                jnp.concatenate([xg[2, pl.ds(a, count)], xg[2, pl.ds(a + half, count)]], axis=0),
                ((2, a, count), (2, a + half, count)),
                place,
            )
            place += 2 * count
    with jax.named_scope("wait_oxfar"):
        for o in (0, 1, 3, 2):
            for d in (0, 1):
                ox_far(o, d, 2).wait_recv()
        go(oc(2, False))
    with jax.named_scope("wait_qkv"):
        for w in pending:
            w.wait_recv()
    with jax.named_scope("wait_oc"):
        for dx in (0, 3, 1, 2):
            oc(dx, True).wait_recv()
    with jax.named_scope("wait_send"):
        for s in sent:
            s.wait_send()


def project(x, gain, wq, wk, wv, wo):
    rows, width = x.shape
    length = rows * RING * RING
    depth = wq.shape[1]
    dma = pltpu.SemaphoreType.DMA
    vmem = pl.BlockSpec(memory_space=pltpu.VMEM)
    return pl.pallas_call(
        project_kernel,
        name="project",
        out_shape=(
            jax.ShapeDtypeStruct((length, 128), BF16),
            jax.ShapeDtypeStruct((length // 2, 128), BF16),
            jax.ShapeDtypeStruct((RING, RING, wo.shape[0], wo.shape[1] * 2 * RING), BF16),
        ),
        in_specs=[pl.BlockSpec(memory_space=pltpu.HBM)] * 6,
        out_specs=(vmem, vmem, vmem),
        scratch_shapes=[
            pltpu.VMEM((2, RING, RING, 96, depth), BF16),
            pltpu.VMEM((width, 384), BF16),
            pltpu.VMEM((3, rows, width), BF16),
            pltpu.VMEM((RING, RING * rows, 128), BF16),
            pltpu.VMEM((RING * rows // 2, 128), BF16),
            dma((4,)), dma((4,)), dma((2, 4)), dma((2, 4)), dma((2, 4)), dma((2, 4)), dma((4,)), dma((4,)),
            dma((2, 2)), dma((2, 2)), dma((2, 2)), dma((2, 2)),
            dma((9, 4)), dma((9, 4)), dma((9, 4)), dma((9, 4)),
            dma((4,)), dma((4,)), dma((2, 2)), dma((2, 2)), dma((2, 4)), dma((2, 4)),
            dma((2, 4)), dma((2, 4)), dma((4,)), dma((4,)), dma((6,)),
            pltpu.VMEM(x.shape, BF16), pltpu.VMEM(gain.shape, F32), pltpu.VMEM(wq.shape, BF16),
            pltpu.VMEM(wk.shape, BF16), pltpu.VMEM(wv.shape, BF16), pltpu.VMEM(wo.shape, BF16),
        ],
        compiler_params=pltpu.CompilerParams(
            collective_id=0, has_side_effects=True, vmem_limit_bytes=24 << 20
        ),
    )(x, gain, wq, wk, wv, wo)


BLOCK_Q = 768
BLOCK_K = 256


def attend_kernel(
    qv_ref, kk_ref, b_hbm, g_hbm, ho_ref, keys_t, qa, vv, tri, acc, car, stage, h_s, h_r,
    b_ref, g_all, local_sem,
):
    loads = [
        pltpu.make_async_copy(b_hbm, b_ref, local_sem.at[0]),
        pltpu.make_async_copy(g_hbm, g_all, local_sem.at[1]),
    ]
    for load in loads:
        load.start()
    length = qv_ref.shape[0]
    rows_each = length // (RING * RING)
    z, y, x, c, at = places()
    me = z * RING + y
    barrier = pltpu.get_barrier_semaphore()
    for dz in range(RING):
        for dy in range(RING):
            if dz or dy:
                pl.semaphore_signal(barrier, inc=1, device_id=at(dz=dz, dy=dy), device_id_type=MESH)
    r = lax.broadcasted_iota(jnp.int32, (BLOCK_K, BLOCK_K), 0)
    c = lax.broadcasted_iota(jnp.int32, (BLOCK_K, BLOCK_K), 1)
    tri[...] = jnp.where(r > c, 1.0, 0.0).astype(BF16)
    step = 512

    @pl.loop(0, length // step)
    def _(i):
        rows = pl.ds(pl.multiple_of(i * step, step), step)
        packed = kk_ref[pl.ds(pl.multiple_of(i * (step // 2), step // 2), step // 2), :]
        packed = packed.reshape(step // 32, 16, 128)
        k = jnp.concatenate([packed[:, :, 0:64], packed[:, :, 64:128]], axis=1).reshape(step, HEAD_DIM)
        kk = k.astype(F32) * (LOG2E / 8.0)
        hi = kk.astype(BF16)
        lo = (kk - hi.astype(F32)).astype(BF16)
        keys_t[0:128, rows] = jnp.concatenate([hi, lo], axis=1).T
        both = qv_ref[rows, :]
        qq = both[:, 0:64]
        lane = lax.broadcasted_iota(jnp.int32, (step, 128), 1)
        qa[rows, 0:128] = jnp.concatenate([qq, qq], axis=1)
        qa[rows, 128:256] = jnp.where(lane < 3, 1.0, 0.0).astype(BF16)
        vv[rows, :] = both[:, 64:128]

    for load in loads:
        load.wait()
    bb = b_ref[...] * LOG2E
    bh = bb.astype(BF16)
    r1 = bb - bh.astype(F32)
    bm = r1.astype(BF16)
    bl = (r1 - bm.astype(F32)).astype(BF16)
    keys_t[128:144, :] = jnp.concatenate([bh, bm, bl, jnp.zeros((13, length), BF16)], axis=0)
    pair = g_all[0:1, pl.ds(pl.multiple_of(lax.div(me, 2) * 128, 128), 128)]
    gain = jnp.where(lax.rem(me, 2) == 0, pair[:, 0:64], pair[:, 64:128])
    pl.semaphore_wait(barrier, RING * RING - 1)
    ratio = BLOCK_Q // BLOCK_K

    @pl.loop(0, length // BLOCK_Q)
    def _(i):
        rows = pl.ds(pl.multiple_of(i * BLOCK_Q, BLOCK_Q), BLOCK_Q)
        q = qa[rows, 0:144]

        def one(q, j, carry, diagonal=False):
            count = q.shape[0]
            cols = pl.ds(pl.multiple_of(j * BLOCK_K, BLOCK_K), BLOCK_K)
            l2 = jnp.dot(q, keys_t[:, cols], preferred_element_type=F32)
            if diagonal:
                t = lax.broadcasted_iota(jnp.int32, (BLOCK_K, BLOCK_K), 0)
                s = lax.broadcasted_iota(jnp.int32, (BLOCK_K, BLOCK_K), 1)
                first = jnp.where(s < t, l2[0:BLOCK_K], -1e30)
                l2 = first if count == BLOCK_K else jnp.concatenate([first, l2[BLOCK_K:]], axis=0)
            mx = jnp.maximum(l2, 0.0)
            mn = jnp.minimum(l2, 0.0)
            log_part = jnp.log2(1.0 + jnp.exp2(mn - mx))
            drop = (mx + log_part).astype(BF16)
            after = jnp.dot(drop, tri[...], preferred_element_type=F32)
            x = (mn - log_part) - after - jnp.concatenate([carry] * (BLOCK_K // 128), axis=1)
            sticks = jnp.exp2(x).astype(BF16)
            pv = jnp.dot(sticks, vv[cols, :], preferred_element_type=F32)
            whole = after[:, 0:1] + drop[:, 0:128].astype(F32)[:, 0:1]
            return pv, carry + jnp.broadcast_to(whole, carry.shape)

        carry = None
        total = None
        for d in reversed(range(ratio)):
            fresh = jnp.zeros((BLOCK_K, 128), F32)
            carry = fresh if carry is None else jnp.concatenate([fresh, carry], axis=0)
            pv, carry = one(q[d * BLOCK_K :], i * ratio + d, carry, True)
            if total is None:
                total = pv
            else:
                total = jnp.concatenate([pv[:BLOCK_K], pv[BLOCK_K:] + total], axis=0)
        acc[...] = total
        car[...] = carry

        def several(n, _):
            base = i * ratio - 1 - n * ratio
            cc, a = car[...], acc[...]
            for u in range(ratio):
                pv, cc = one(q, base - u, cc)
                a = a + pv
            acc[...] = a
            car[...] = cc
            return 0

        lax.fori_loop(0, i, several, 0)
        a = acc[...]
        scaled = a * lax.rsqrt(jnp.mean(a * a, axis=-1, keepdims=True) + EPS)
        head = (scaled * gain).astype(BF16)
        for yy in range(RING):
            part = head[yy * rows_each : (yy + 1) * rows_each]
            half = rows_each // 2
            stage[i * RING + yy] = jnp.concatenate([part[:half], part[half:]], axis=1)
        for yy in range(RING):
            dest = i * RING + yy

            @pl.when(dest != me)
            def _():
                rcopy(
                    stage.at[dest], ho_ref.at[y * RING + z], h_s.at[dest], h_r.at[me],
                    {"sp": dest, "dp": lax.axis_index("dp")},
                ).start()

            @pl.when(dest == me)
            def _():
                ho_ref[y * RING + z] = stage[dest]

    for dz in range(RING):
        for dy in range(RING):
            if dz or dy:
                nz, ny = lax.rem(z + dz, RING), lax.rem(y + dy, RING)
                other = nz * RING + ny
                slot = ho_ref.at[ny * RING + nz]
                w = rcopy(slot, slot, h_s.at[other], h_r.at[other], at(dz=dz, dy=dy))
                w.wait_recv()
                w.wait_send()


def attend(qv, kk, bias, gain):
    length = qv.shape[0]
    each = length // (RING * RING)
    vmem = pl.BlockSpec(memory_space=pltpu.VMEM)
    dma = pltpu.SemaphoreType.DMA
    return pl.pallas_call(
        attend_kernel,
        name="attend",
        out_shape=jax.ShapeDtypeStruct((RING * RING, each // 2, 2 * HEAD_DIM), BF16),
        in_specs=[vmem] * 2 + [pl.BlockSpec(memory_space=pltpu.HBM)] * 2,
        out_specs=vmem,
        scratch_shapes=[
            pltpu.VMEM((144, length), BF16),
            pltpu.VMEM((length, 256), BF16),
            pltpu.VMEM((length, HEAD_DIM), BF16),
            pltpu.VMEM((BLOCK_K, BLOCK_K), BF16),
            pltpu.VMEM((BLOCK_Q, HEAD_DIM), F32),
            pltpu.VMEM((BLOCK_Q, 128), F32),
            pltpu.VMEM((RING * RING, each // 2, 2 * HEAD_DIM), BF16),
            dma((RING * RING,)), dma((RING * RING,)),
            pltpu.VMEM(bias.shape, F32), pltpu.VMEM(gain.shape, F32), dma((2,)),
        ],
        compiler_params=pltpu.CompilerParams(
            collective_id=1, has_side_effects=True, vmem_limit_bytes=24 << 20
        ),
    )(qv, kk, bias, gain)


def mix_kernel(ho_ref, wo_ref, o_ref, lhs):
    heads, half, _ = ho_ref.shape
    for n in range(0, heads, 2):
        a, b = ho_ref[n], ho_ref[n + 1]
        cols = pl.ds(n * HEAD_DIM, 2 * HEAD_DIM)
        lhs[0:half, cols] = jnp.concatenate([a[:, 0:64], b[:, 0:64]], axis=1)
        lhs[half : 2 * half, cols] = jnp.concatenate([a[:, 64:128], b[:, 64:128]], axis=1)
    width = o_ref.shape[1]
    for n in range(0, width, 512):
        o_ref[:, n : n + 512] = jnp.dot(
            lhs[...], wo_ref[:, n : n + 512], preferred_element_type=F32
        ).astype(BF16)


def mix(ho, wo):
    heads, half, _ = ho.shape
    vmem = pl.BlockSpec(memory_space=pltpu.VMEM)
    return pl.pallas_call(
        mix_kernel,
        name="mix",
        out_shape=jax.ShapeDtypeStruct((2 * half, wo.shape[1]), BF16),
        in_specs=[vmem] * 2,
        out_specs=vmem,
        scratch_shapes=[pltpu.VMEM((2 * half, heads * HEAD_DIM), BF16)],
        compiler_params=pltpu.CompilerParams(vmem_limit_bytes=16 << 20),
    )(ho, wo)


def body(inputs, in_gain, w_query, w_key, w_value, key_bias, out_gain, w_out):
    qv, kk, wo = project(inputs[0], in_gain[None], w_query.T, w_key.T, w_value.T, w_out)
    ho = attend(qv, kk, key_bias[0].T, out_gain[None])
    return mix(ho, wo.reshape(-1, wo.shape[-1]))[None]


def solution(mesh):
    placed = (
        P("dp", "sp", None), P(), P("dp", "sp"), P("dp", "sp"), P("dp", "sp"),
        P("dp", None, "sp"), P(), P("sp", "dp"),
    )
    return jax.shard_map(body, mesh=mesh, in_specs=placed, out_specs=P("dp", "sp", None), check_vma=False)
```

```python
import functools

import jax
import jax.numpy as jnp
from jax import lax
from jax.experimental import pallas as pl
from jax.experimental.pallas import tpu as pltpu
from jax.sharding import PartitionSpec as P

HEAD_DIM = 64
RING = 4
EPS = 1e-06
LOG2E = 1.4426950408889634
F32 = jnp.float32
BF16 = jnp.bfloat16
MESH = pl.DeviceIdType.MESH


def rcopy(src, dst, send, recv, device):
    return pltpu.make_async_remote_copy(
        src_ref=src, dst_ref=dst, send_sem=send, recv_sem=recv, device_id=device, device_id_type=MESH
    )


def places():
    sp, dp = lax.axis_index("sp"), lax.axis_index("dp")
    z, y = lax.div(sp, RING), lax.rem(sp, RING)
    x, c = lax.div(dp, 2), lax.rem(dp, 2)

    def at(dz=0, dy=0, dx=0, dc=0):
        nz, ny = lax.rem(z + dz, RING), lax.rem(y + dy, RING)
        nx, nc = lax.rem(x + dx, RING), lax.rem(c + dc, 2)
        return {"sp": nz * RING + ny, "dp": nx * 2 + nc}

    return z, y, x, c, at


def layer_kernel(
    x_hbm, gain_hbm, wq_hbm, wk_hbm, wv_hbm, wo_hbm, b_hbm, g_hbm,
    ho_ref, wo_ref,
    qv_ref, kk_ref, keys_t, qa, vv, tri, part, rsum, acc, car, stage, h_s, h_r, b_ref, g_all,
    packs, w_all, xg, stage_qv, stage_k,
    wy_s, wy_r, wx_s, wx_r, wf_s, wf_r, wc_s, wc_r, xd_s, xd_r, xf_s, xf_r, a_s, a_r, b_s, b_r,
    oz_s, oz_r, oy_s, oy_r, ox_s, ox_r, of_s, of_r, oc_s, oc_r, local_sem,
    x_ref, gain_ref, wq_ref, wk_ref, wv_ref, wo_in,
):
    z, y, x, c, at = places()
    loads = [
        pltpu.make_async_copy(s, d, local_sem.at[i])
        for i, (s, d) in enumerate(
            (
                (wq_hbm, wq_ref), (wk_hbm, wk_ref), (wv_hbm, wv_ref), (wo_hbm, wo_in),
                (gain_hbm, gain_ref), (x_hbm, x_ref), (b_hbm, b_ref), (g_hbm, g_all),
            )
        )
    ]
    for load in loads:
        load.start()
    friends = [at(dz=i, dy=j) for i in range(RING) for j in range(RING) if i or j]
    friends += [at(dx=1), at(dx=3), at(dc=1)]
    barrier = pltpu.get_barrier_semaphore()
    for f in friends:
        pl.semaphore_signal(barrier, inc=1, device_id=f, device_id_type=MESH)
    for load in loads:
        load.wait()
    rows = x_ref.shape[0]
    half = rows // 2
    depth = wq_ref.shape[1]
    qn, kn = wq_ref.shape[0], wk_ref.shape[0]
    piece_rows = qn + 2 * kn
    packs[c, x, y] = jnp.concatenate([wq_ref[...], wk_ref[...], wv_ref[...]], axis=0)

    def wo_cols(dx, cc):
        return pl.ds(pl.multiple_of((lax.rem(x + dx, RING) * 2 + cc) * depth, depth), depth)

    wo_ref[y, z, :, wo_cols(0, c)] = wo_in[...]
    pl.semaphore_wait(barrier, len(friends))

    sent = []

    def go(copy):
        copy.start()
        sent.append(copy)

    def near(d, axis):
        return at(**{axis: 1 if d == 0 else 3})

    def back(d):
        return 3 if d == 0 else 1

    lo, hi = pl.ds(0, half), pl.ds(half, half)
    halves = (lo, hi)

    def oz(dz, n):
        return wo_ref.at[y, lax.rem(z + dz, RING), n, wo_cols(0, c)]

    every = slice(None)

    def oz_out(dz):
        return rcopy(wo_in, oz(0, every), oz_s.at[dz], oz_r.at[dz], at(dz=dz))

    def oz_in(dz):
        s = oz(RING - dz, every)
        return rcopy(s, s, oz_s.at[dz], oz_r.at[dz], at(dz=dz))

    def x_out(d, i):
        p = halves[i if d == 0 else 1 - i]
        return rcopy(x_ref.at[p], xg.at[d, p], xd_s.at[d, i], xd_r.at[d, i], near(d, "dz"))

    def x_in(d, i):
        p = halves[i if d == 0 else 1 - i]
        return rcopy(xg.at[d, p], xg.at[d, p], xd_s.at[d, i], xd_r.at[d, i], near(d, "dz"))

    cuts = ((0, 64), (64, 32))

    def far_z(d, i, arrived):
        a, n = cuts[i]
        part = pl.ds(a + (0 if d == 0 else half), n)
        return rcopy(xg.at[2 if arrived else d, part], xg.at[2, part], xf_s.at[d, i], xf_r.at[d, i], near(d, "dz"))

    def piece(o):
        return lax.rem(y + RING - o, RING)

    def w_y(o, arrived):
        p = packs.at[c, x, piece(o) if arrived else y]
        return rcopy(p, p, wy_s.at[o], wy_r.at[o], at(dy=o))

    def w_x(o, d, arrived):
        p = packs.at[c, lax.rem(x + back(d), RING) if arrived else x, piece(o)]
        return rcopy(p, p, wx_s.at[d, o], wx_r.at[d, o], near(d, "dx"))

    def w_far(o, d, dx):
        part = packs.at[c, lax.rem(x + dx, RING), piece(o), pl.ds(0 if d == 0 else piece_rows // 2, piece_rows // 2)]
        return rcopy(part, part, wf_s.at[d, o], wf_r.at[d, o], near(d, "dx"))

    def w_c(dx, arrived):
        slab = packs.at[1 - c if arrived else c, lax.rem(x + dx, RING)]
        return rcopy(slab, slab, wc_s.at[dx], wc_r.at[dx], at(dc=1))

    def oy(d, arrived):
        s = wo_ref.at[lax.rem(y + back(d), RING) if arrived else y, :, :, wo_cols(0, c)]
        return rcopy(s, s, oy_s.at[d, 0], oy_r.at[d, 0], near(d, "dy"))

    def oy_far(d, dy):
        s = wo_ref.at[lax.rem(y + dy, RING), pl.ds(0 if d == 0 else 2, 2), :, wo_cols(0, c)]
        return rcopy(s, s, oy_s.at[d, 1], oy_r.at[d, 1], near(d, "dy"))

    def ox(o, d, arrived):
        s = wo_ref.at[piece(o), :, :, wo_cols(back(d) if arrived else 0, c)]
        return rcopy(s, s, ox_s.at[d, o], ox_r.at[d, o], near(d, "dx"))

    def ox_far(o, d, dx):
        s = wo_ref.at[piece(o), pl.ds(0 if d == 0 else 2, 2), :, wo_cols(dx, c)]
        return rcopy(s, s, of_s.at[d, o], of_r.at[d, o], near(d, "dx"))

    def oc(dx, arrived):
        s = wo_ref.at[:, :, :, wo_cols(dx, 1 - c if arrived else c)]
        return rcopy(s, s, oc_s.at[dx], oc_r.at[dx], at(dc=1))

    with jax.named_scope("issue"):
        for o in (1, 3, 2):
            go(w_y(o, False))
        for d in (0, 1):
            go(w_x(0, d, False))
        for dz in (2, 1, 3):
            go(oz_out(dz))
        for i in (0, 1):
            for d in (0, 1):
                go(x_out(d, i))
    with jax.named_scope("wait_wy"):
        for o in (1, 3, 2):
            w_y(o, True).wait_recv()
            for d in (0, 1):
                go(w_x(o, d, False))
        go(w_c(0, False))
    with jax.named_scope("wait_oz"):
        for dz in (1, 3, 2):
            oz_in(dz).wait_recv()
        for d in (0, 1):
            go(oy(d, False))
    with jax.named_scope("wait_wx"):
        for o in (0, 1, 3, 2):
            for d in (0, 1):
                w_x(o, d, True).wait_recv()
                go(w_far(o, d, back(d)))
        go(w_c(3, False))
        go(w_c(1, False))
        for d in (0, 1):
            go(ox(0, d, False))
    with jax.named_scope("wait_oy"):
        for d in (0, 1):
            oy(d, True).wait_recv()
            go(oy_far(d, back(d)))
        for o in (1, 3):
            for d in (0, 1):
                go(ox(o, d, False))
    pending = [[], [], [], []]

    def chunk(n, source, segments, stage_at):
        wide = source.astype(F32)
        normed = (
            wide * lax.rsqrt(jnp.mean(wide * wide, axis=-1, keepdims=True) + EPS) * gain_ref[...]
        ).astype(BF16)
        out = jnp.dot(normed, w_all[...], preferred_element_type=F32).astype(BF16)
        total = out.shape[0]
        v = out[:, 320:384]
        k = out[:, 256:320].reshape(total // 32, 2, 16, HEAD_DIM)
        for i in range(RING):
            stage_qv[i, pl.ds(stage_at, total)] = jnp.concatenate([out[:, i * 64 : i * 64 + 64], v], axis=1)
        stage_k[pl.ds(stage_at // 2, total // 2)] = jnp.concatenate([k[:, 0], k[:, 1]], axis=2).reshape(
            total // 2, 128
        )
        for dz, first, count in segments:
            here, here_k = pl.ds(stage_at, count), pl.ds(stage_at // 2, count // 2)
            nz = lax.rem(z + dz, RING)

            def spot(dy, halved):
                start = (nz * RING + lax.rem(y + dy, RING)) * rows + first
                if halved:
                    return pl.ds(pl.multiple_of(lax.div(start, 2), 16), count // 2)
                return pl.ds(pl.multiple_of(start, 32), count)

            for o in (2, 1, 3):
                ny = lax.rem(y + o, RING)
                go(rcopy(stage_qv.at[ny, here], qv_ref.at[spot(0, False)], a_s.at[n, o], a_r.at[n, o], at(dy=o)))
                go(rcopy(stage_k.at[here_k], kk_ref.at[spot(0, True)], b_s.at[n, o], b_r.at[n, o], at(dy=o)))
            qv_ref[spot(0, False)] = stage_qv[y, here]
            kk_ref[spot(0, True)] = stage_k[here_k]
            for o in (1, 3, 2):
                s, t = qv_ref.at[spot(RING - o, False)], kk_ref.at[spot(RING - o, True)]
                pending[dz].append(rcopy(s, s, a_s.at[n, o], a_r.at[n, o], at(dy=o)))
                pending[dz].append(rcopy(t, t, b_s.at[n, o], b_r.at[n, o], at(dy=o)))
            n, stage_at = n + 1, stage_at + count

    ratio = BLOCK_Q // BLOCK_K
    me = z * RING + y

    def place(dz):
        return lax.rem(z + dz, RING)

    def block_rows(i, size):
        return pl.ds(pl.multiple_of(i * size, size), size)

    def prepare(dz):
        for w in pending[dz]:
            w.wait_recv()
        i = place(dz)
        at_rows = block_rows(i, BLOCK_Q)
        packed = kk_ref[block_rows(i, BLOCK_Q // 2), :].reshape(BLOCK_Q // 32, 16, 128)
        k = jnp.concatenate([packed[:, :, 0:64], packed[:, :, 64:128]], axis=1).reshape(BLOCK_Q, HEAD_DIM)
        kk = k.astype(F32) * (LOG2E / 8.0)
        hi_part = kk.astype(BF16)
        lo_part = (kk - hi_part.astype(F32)).astype(BF16)
        keys_t[0:128, at_rows] = jnp.concatenate([hi_part, lo_part], axis=1).T
        both = qv_ref[at_rows, :]
        qa[at_rows, 0:128] = jnp.concatenate([both[:, 0:64], both[:, 0:64]], axis=1)
        vv[at_rows, :] = both[:, 64:128]

    def block(q, j, carry, diagonal=False):
        count = q.shape[0]
        cols = block_rows(j, BLOCK_K)
        l2 = jnp.dot(q, keys_t[:, cols], preferred_element_type=F32)
        if diagonal:
            t = lax.broadcasted_iota(jnp.int32, (BLOCK_K, BLOCK_K), 0)
            u = lax.broadcasted_iota(jnp.int32, (BLOCK_K, BLOCK_K), 1)
            first = jnp.where(u < t, l2[0:BLOCK_K], -1e30)
            l2 = first if count == BLOCK_K else jnp.concatenate([first, l2[BLOCK_K:]], axis=0)
        soft = jnp.maximum(l2, jnp.log2(1.0 + jnp.exp2(jnp.minimum(l2, 100.0))))
        drop = soft.astype(BF16)
        after = jnp.dot(drop, tri[...], preferred_element_type=F32)
        e = (l2 - soft) - after
        if carry is not None:
            e = e - jnp.concatenate([carry] * (BLOCK_K // 128), axis=1)
        pv = jnp.dot(jnp.exp2(e).astype(BF16), vv[cols, :], preferred_element_type=F32)
        whole = jnp.broadcast_to(after[:, 0:1] + soft[:, 0:1], (count, 128))
        return pv, whole if carry is None else carry + whole

    def diagonal(dz):
        i = place(dz)
        q = qa[block_rows(i, BLOCK_Q), 0:144]
        carry, total = None, None
        for d in reversed(range(ratio)):
            if carry is not None:
                carry = jnp.concatenate([jnp.zeros((BLOCK_K, 128), F32), carry], axis=0)
            pv, carry = block(q[d * BLOCK_K :], i * ratio + d, carry, True)
            if total is None:
                total = pv
            else:
                total = jnp.concatenate([pv[:BLOCK_K], pv[BLOCK_K:] + total], axis=0)
        part[i, i] = total
        rsum[i, i] = carry

    def pair(da, db):
        a, b = place(da), place(db)
        i, j = jnp.maximum(a, b), jnp.minimum(a, b)
        q = qa[block_rows(i, BLOCK_Q), 0:144]
        carry, total = None, None
        for d in reversed(range(ratio)):
            pv, carry = block(q, j * ratio + d, carry)
            total = pv if total is None else total + pv
        part[i, j] = total
        rsum[i, j] = carry

    def finish(i):
        acc[...] = part[i, i]
        car[...] = rsum[i, i]

        def add(n, _):
            j = i - 1 - n
            acc[...] += jnp.exp2(-car[...])[:, 0:HEAD_DIM] * part[i, j]
            car[...] += rsum[i, j]
            return 0

        lax.fori_loop(0, i, add, 0)
        pair_gain = g_all[0:1, block_rows(lax.div(me, 2), 128)]
        own_gain = jnp.where(lax.rem(me, 2) == 0, pair_gain[:, 0:64], pair_gain[:, 64:128])
        a = acc[...]
        scaled = a * lax.rsqrt(jnp.mean(a * a, axis=-1, keepdims=True) + EPS)
        head = (scaled * own_gain).astype(BF16)
        for yy in range(RING):
            mine = head[yy * rows : (yy + 1) * rows]
            stage[i * RING + yy] = jnp.concatenate([mine[:half], mine[half:]], axis=1)
        for yy in range(RING):
            dest = i * RING + yy

            @pl.when(dest != me)
            def _():
                rcopy(
                    stage.at[dest], ho_ref.at[y * RING + z], h_s.at[dest], h_r.at[me],
                    {"sp": dest, "dp": lax.axis_index("dp")},
                ).start()

            @pl.when(dest == me)
            def _():
                ho_ref[y * RING + z] = stage[dest]

    with jax.named_scope("constants"):
        r = lax.broadcasted_iota(jnp.int32, (BLOCK_K, BLOCK_K), 0)
        u = lax.broadcasted_iota(jnp.int32, (BLOCK_K, BLOCK_K), 1)
        tri[...] = jnp.where(r > u, 1.0, 0.0).astype(BF16)
        length = qv_ref.shape[0]
        lane = lax.broadcasted_iota(jnp.int32, (length, 128), 1)
        qa[:, 128:256] = jnp.where(lane < 3, 1.0, 0.0).astype(BF16)
        bb = b_ref[...] * LOG2E
        bh = bb.astype(BF16)
        r1 = bb - bh.astype(F32)
        bm = r1.astype(BF16)
        bl = (r1 - bm.astype(F32)).astype(BF16)
        keys_t[128:144, :] = jnp.concatenate([bh, bm, bl, jnp.zeros((13, length), BF16)], axis=0)
    with jax.named_scope("wait_wfar"):
        for o in (0, 1, 3, 2):
            for d in (0, 1):
                w_far(o, d, 2).wait_recv()
        go(w_c(2, False))
    with jax.named_scope("wait_x0"):
        for d in (0, 1):
            x_in(d, 0).wait_recv()
            for i in (0, 1):
                go(far_z(d, i, False))
    with jax.named_scope("wait_oyfar"):
        for d in (0, 1):
            oy_far(d, 2).wait_recv()
        for d in (0, 1):
            go(ox(2, d, False))
        go(oc(0, False))
    with jax.named_scope("wait_wc"):
        for dx in (0, 3, 1, 2):
            w_c(dx, True).wait_recv()
    with jax.named_scope("assemble"):
        for n in range(2 * RING):
            p = [packs[n % 2, n // 2, i] for i in range(RING)]
            w_all[n * depth : (n + 1) * depth, :] = jnp.concatenate(
                [t[0:qn] for t in p] + [t[qn : qn + kn] for t in p] + [t[qn + kn :] for t in p], axis=0
            ).T
    with jax.named_scope("chunk0"):
        chunk(0, x_ref[...], ((0, 0, rows),), 0)
    with jax.named_scope("chunk12"):
        chunk(1, jnp.concatenate([xg[0, lo], xg[1, hi]], axis=0), ((3, 0, half), (1, half, half)), rows)
    with jax.named_scope("wait_ox"):
        for o in (0, 1, 3):
            for d in (0, 1):
                ox(o, d, True).wait_recv()
                go(ox_far(o, d, back(d)))
    with jax.named_scope("wait_x1"):
        x_in(0, 1).wait_recv()
        x_in(1, 1).wait_recv()
    with jax.named_scope("chunk34"):
        chunk(3, jnp.concatenate([xg[0, hi], xg[1, lo]], axis=0), ((3, half, half), (1, 0, half)), 2 * rows)
    with jax.named_scope("wait_ox2"):
        for d in (0, 1):
            ox(2, d, True).wait_recv()
            go(ox_far(2, d, back(d)))
        go(oc(3, False))
        go(oc(1, False))
    with jax.named_scope("prepare_own"):
        prepare(0)
    with jax.named_scope("diagonal_own"):
        diagonal(0)

    def far_chunk(i):
        a, count = cuts[i]
        with jax.named_scope("wait_far%d" % i):
            for d in (0, 1):
                far_z(d, i, True).wait_recv()
        with jax.named_scope("chunk_far%d" % i):
            chunk(
                5 + 2 * i,
                jnp.concatenate([xg[2, pl.ds(a, count)], xg[2, pl.ds(a + half, count)]], axis=0),
                ((2, a, count), (2, a + half, count)),
                3 * rows + 2 * i * cuts[0][1],
            )

    far_chunk(0)
    far_chunk(1)
    with jax.named_scope("wait_oxfar"):
        for o in (0, 1, 3, 2):
            for d in (0, 1):
                ox_far(o, d, 2).wait_recv()
        go(oc(2, False))
    with jax.named_scope("prepare_near"):
        prepare(3)
        prepare(1)
    with jax.named_scope("diagonal_near"):

        @pl.loop(0, 2)
        def _(n):
            diagonal(3 - 2 * n)

    with jax.named_scope("pairs_near"):

        @pl.loop(0, 3)
        def _(n):
            pair(jnp.where(n == 2, 3, 0), jnp.where(n == 0, 3, 1))

    far = place(2)
    with jax.named_scope("finish_early"):

        @pl.loop(0, far)
        def _(i):
            finish(i)

    with jax.named_scope("prepare_far"):
        prepare(2)
    with jax.named_scope("diagonal_far"):
        diagonal(2)
    with jax.named_scope("pairs_far"):

        @pl.loop(0, 3)
        def _(n):
            pair(2, jnp.where(n == 0, 0, jnp.where(n == 1, 3, 1)))

    with jax.named_scope("finish_late"):

        @pl.loop(far, RING)
        def _(i):
            finish(i)

    with jax.named_scope("wait_ho"):
        for dz in range(RING):
            for dy in range(RING):
                if dz or dy:
                    nz, ny = lax.rem(z + dz, RING), lax.rem(y + dy, RING)
                    other = nz * RING + ny
                    slot = ho_ref.at[ny * RING + nz]
                    w = rcopy(slot, slot, h_s.at[other], h_r.at[other], at(dz=dz, dy=dy))
                    w.wait_recv()
                    w.wait_send()
    with jax.named_scope("wait_oc"):
        for dx in (0, 3, 1, 2):
            oc(dx, True).wait_recv()
    with jax.named_scope("wait_send"):
        for t in sent:
            t.wait_send()


BLOCK_Q = 768
BLOCK_K = 256


def layer(x, gain, wq, wk, wv, wo, bias, out_gain):
    rows, width = x.shape
    length = rows * RING * RING
    depth = wq.shape[1]
    dma = pltpu.SemaphoreType.DMA
    vmem = pl.BlockSpec(memory_space=pltpu.VMEM)
    operands = [
        pltpu.with_memory_space_constraint(t, pltpu.HBM) for t in (x, gain, wq, wk, wv, wo, bias, out_gain)
    ]
    return pl.pallas_call(
        layer_kernel,
        name="layer",
        out_shape=(
            jax.ShapeDtypeStruct((RING * RING, rows // 2, 2 * HEAD_DIM), BF16),
            jax.ShapeDtypeStruct((RING, RING, wo.shape[0], wo.shape[1] * 2 * RING), BF16),
        ),
        in_specs=[pl.BlockSpec(memory_space=pltpu.HBM)] * 8,
        out_specs=(vmem, vmem),
        scratch_shapes=[
            pltpu.VMEM((length, 128), BF16),
            pltpu.VMEM((length // 2, 128), BF16),
            pltpu.VMEM((144, length), BF16),
            pltpu.VMEM((length, 256), BF16),
            pltpu.VMEM((length, HEAD_DIM), BF16),
            pltpu.VMEM((BLOCK_K, BLOCK_K), BF16),
            pltpu.VMEM((RING, RING, BLOCK_Q, HEAD_DIM), F32),
            pltpu.VMEM((RING, RING, BLOCK_Q, 128), F32),
            pltpu.VMEM((BLOCK_Q, HEAD_DIM), F32),
            pltpu.VMEM((BLOCK_Q, 128), F32),
            pltpu.VMEM((RING * RING, rows // 2, 2 * HEAD_DIM), BF16),
            dma((RING * RING,)), dma((RING * RING,)),
            pltpu.VMEM(bias.shape, F32), pltpu.VMEM(out_gain.shape, F32),
            pltpu.VMEM((2, RING, RING, 96, depth), BF16),
            pltpu.VMEM((width, 384), BF16),
            pltpu.VMEM((3, rows, width), BF16),
            pltpu.VMEM((RING, RING * rows, 128), BF16),
            pltpu.VMEM((RING * rows // 2, 128), BF16),
            dma((4,)), dma((4,)), dma((2, 4)), dma((2, 4)), dma((2, 4)), dma((2, 4)), dma((4,)), dma((4,)),
            dma((2, 2)), dma((2, 2)), dma((2, 2)), dma((2, 2)),
            dma((9, 4)), dma((9, 4)), dma((9, 4)), dma((9, 4)),
            dma((4,)), dma((4,)), dma((2, 2)), dma((2, 2)), dma((2, 4)), dma((2, 4)),
            dma((2, 4)), dma((2, 4)), dma((4,)), dma((4,)), dma((8,)),
            pltpu.VMEM(x.shape, BF16), pltpu.VMEM(gain.shape, F32), pltpu.VMEM(wq.shape, BF16),
            pltpu.VMEM(wk.shape, BF16), pltpu.VMEM(wv.shape, BF16), pltpu.VMEM(wo.shape, BF16),
        ],
        compiler_params=pltpu.CompilerParams(
            collective_id=0, has_side_effects=True, vmem_limit_bytes=44 << 20
        ),
    )(*operands)


def mix_kernel(ho_ref, wo_ref, o_ref, lhs):
    heads, half, _ = ho_ref.shape
    for n in range(0, heads, 2):
        a, b = ho_ref[n], ho_ref[n + 1]
        cols = pl.ds(n * HEAD_DIM, 2 * HEAD_DIM)
        lhs[0:half, cols] = jnp.concatenate([a[:, 0:64], b[:, 0:64]], axis=1)
        lhs[half : 2 * half, cols] = jnp.concatenate([a[:, 64:128], b[:, 64:128]], axis=1)
    width = o_ref.shape[1]
    for n in range(0, width, 512):
        o_ref[:, n : n + 512] = jnp.dot(
            lhs[...], wo_ref[:, n : n + 512], preferred_element_type=F32
        ).astype(BF16)


def mix(ho, wo):
    heads, half, _ = ho.shape
    vmem = pl.BlockSpec(memory_space=pltpu.VMEM)
    return pl.pallas_call(
        mix_kernel,
        name="mix",
        out_shape=jax.ShapeDtypeStruct((2 * half, wo.shape[1]), BF16),
        in_specs=[vmem] * 2,
        out_specs=vmem,
        scratch_shapes=[pltpu.VMEM((2 * half, heads * HEAD_DIM), BF16)],
        compiler_params=pltpu.CompilerParams(vmem_limit_bytes=16 << 20),
    )(ho, wo)


def body(inputs, in_gain, w_query, w_key, w_value, key_bias, out_gain, w_out):
    ho, wo = layer(
        inputs[0], in_gain[None], w_query.T, w_key.T, w_value.T, w_out, key_bias[0].T, out_gain[None]
    )
    return mix(ho, wo.reshape(-1, wo.shape[-1]))[None]


def solution(mesh):
    placed = (
        P("dp", "sp", None), P(), P("dp", "sp"), P("dp", "sp"), P("dp", "sp"),
        P("dp", None, "sp"), P(), P("sp", "dp"),
    )
    return jax.shard_map(body, mesh=mesh, in_specs=placed, out_specs=P("dp", "sp", None), check_vma=False)
```

```python
import functools

import jax
import jax.numpy as jnp
from jax import lax
from jax.experimental import pallas as pl
from jax.experimental.pallas import tpu as pltpu
from jax.sharding import PartitionSpec as P

HEAD_DIM = 64
RING = 4
EPS = 1e-06
LOG2E = 1.4426950408889634
F32 = jnp.float32
BF16 = jnp.bfloat16
MESH = pl.DeviceIdType.MESH


def rcopy(src, dst, send, recv, device):
    return pltpu.make_async_remote_copy(
        src_ref=src, dst_ref=dst, send_sem=send, recv_sem=recv, device_id=device, device_id_type=MESH
    )


def places():
    sp, dp = lax.axis_index("sp"), lax.axis_index("dp")
    z, y = lax.div(sp, RING), lax.rem(sp, RING)
    x, c = lax.div(dp, 2), lax.rem(dp, 2)

    def at(dz=0, dy=0, dx=0, dc=0):
        nz, ny = lax.rem(z + dz, RING), lax.rem(y + dy, RING)
        nx, nc = lax.rem(x + dx, RING), lax.rem(c + dc, 2)
        return {"sp": nz * RING + ny, "dp": nx * 2 + nc}

    return z, y, x, c, at


def layer_kernel(
    x_hbm, gain_hbm, wq_hbm, wk_hbm, wv_hbm, wo_hbm, b_hbm, g_hbm,
    ho_ref, wo_ref,
    qv_ref, kk_ref, keys_t, qa, vv, tri, part, rsum, acc, car, stage, h_s, h_r, b_ref, g_all,
    packs, w_all, xg, stage_qv, stage_k,
    wa_s, wa_r, wb_s, wb_r, wc_s, wc_r, xd_s, xd_r, xf_s, xf_r, a_s, a_r, b_s, b_r,
    oz_s, oz_r, oy_s, oy_r, ox_s, ox_r, of_s, of_r, oc_s, oc_r, local_sem,
    x_ref, gain_ref, wq_ref, wk_ref, wv_ref, wo_in,
):
    z, y, x, c, at = places()
    loads = [
        pltpu.make_async_copy(s, d, local_sem.at[i])
        for i, (s, d) in enumerate(
            (
                (wq_hbm, wq_ref), (wk_hbm, wk_ref), (wv_hbm, wv_ref), (wo_hbm, wo_in),
                (gain_hbm, gain_ref), (x_hbm, x_ref), (b_hbm, b_ref), (g_hbm, g_all),
            )
        )
    ]
    for load in loads:
        load.start()
    friends = [at(dz=i, dy=j) for i in range(RING) for j in range(RING) if i or j]
    friends += [at(dx=1), at(dx=2), at(dx=3), at(dc=1)]
    barrier = pltpu.get_barrier_semaphore()
    for f in friends:
        pl.semaphore_signal(barrier, inc=1, device_id=f, device_id_type=MESH)
    for load in loads:
        load.wait()
    rows = x_ref.shape[0]
    half = rows // 2
    depth = wq_ref.shape[1]
    qn, kn = wq_ref.shape[0], wk_ref.shape[0]
    split = depth // 2
    own_piece = jnp.concatenate([wq_ref[...], wk_ref[...], wv_ref[...]], axis=0)
    packs[c, x, y, 0] = own_piece[:, 0:split]
    packs[c, x, y, 1] = own_piece[:, split:]

    def wo_cols(dx, cc):
        return pl.ds(pl.multiple_of((lax.rem(x + dx, RING) * 2 + cc) * depth, depth), depth)

    wo_ref[y, z, :, wo_cols(0, c)] = wo_in[...]
    pl.semaphore_wait(barrier, len(friends))

    sent = []

    def go(copy):
        copy.start()
        sent.append(copy)

    def near(d, axis):
        return at(**{axis: 1 if d == 0 else 3})

    def back(d):
        return 3 if d == 0 else 1


    def oz(dz, n):
        return wo_ref.at[y, lax.rem(z + dz, RING), n, wo_cols(0, c)]

    every = slice(None)

    def oz_out(dz):
        return rcopy(wo_in, oz(0, every), oz_s.at[dz], oz_r.at[dz], at(dz=dz))

    def oz_in(dz):
        s = oz(RING - dz, every)
        return rcopy(s, s, oz_s.at[dz], oz_r.at[dz], at(dz=dz))

    third = rows // 3
    parts = (
        (pl.ds(0, 2 * third), pl.ds(2 * third, third)),
        (pl.ds(third, 2 * third), pl.ds(0, third)),
    )

    def x_out(d, i):
        p = parts[d][i]
        return rcopy(x_ref.at[p], xg.at[d, p], xd_s.at[d, i], xd_r.at[d, i], near(d, "dz"))

    def x_in(d, i):
        p = parts[d][i]
        return rcopy(xg.at[d, p], xg.at[d, p], xd_s.at[d, i], xd_r.at[d, i], near(d, "dz"))

    cuts = ((0, 64), (64, 32))

    def far_z(d, i, arrived):
        a, n = cuts[i]
        part = pl.ds(a + (0 if d == 0 else half), n)
        return rcopy(xg.at[2 if arrived else d, part], xg.at[2, part], xf_s.at[d, i], xf_r.at[d, i], near(d, "dz"))

    def piece(o):
        return lax.rem(y + RING - o, RING)

    def w_first(side, o, arrived):
        py = piece(o) if arrived and side == 0 else y
        px = lax.rem(x + RING - o, RING) if arrived and side == 1 else x
        p = packs.at[c, px, py, side]
        return rcopy(p, p, wa_s.at[side, o], wa_r.at[side, o], at(dy=o) if side == 0 else at(dx=o))

    def w_second(side, came, o, arrived):
        py, px = y, x
        if side == 0:
            py = piece(came)
            px = lax.rem(x + RING - o, RING) if arrived else x
        else:
            px = lax.rem(x + RING - came, RING)
            py = piece(o) if arrived else y
        p = packs.at[c, px, py, side]
        return rcopy(
            p, p, wb_s.at[side, came, o], wb_r.at[side, came, o], at(dx=o) if side == 0 else at(dy=o)
        )

    def w_c(dx, arrived):
        slab = packs.at[1 - c if arrived else c, lax.rem(x + dx, RING)]
        return rcopy(slab, slab, wc_s.at[dx], wc_r.at[dx], at(dc=1))

    def oy(d, arrived):
        s = wo_ref.at[lax.rem(y + back(d), RING) if arrived else y, :, :, wo_cols(0, c)]
        return rcopy(s, s, oy_s.at[d, 0], oy_r.at[d, 0], near(d, "dy"))

    def oy_far(d, dy):
        s = wo_ref.at[lax.rem(y + dy, RING), pl.ds(0 if d == 0 else 2, 2), :, wo_cols(0, c)]
        return rcopy(s, s, oy_s.at[d, 1], oy_r.at[d, 1], near(d, "dy"))

    def ox(o, d, arrived):
        s = wo_ref.at[piece(o), :, :, wo_cols(back(d) if arrived else 0, c)]
        return rcopy(s, s, ox_s.at[d, o], ox_r.at[d, o], near(d, "dx"))

    def ox_far(o, d, dx):
        s = wo_ref.at[piece(o), pl.ds(0 if d == 0 else 2, 2), :, wo_cols(dx, c)]
        return rcopy(s, s, of_s.at[d, o], of_r.at[d, o], near(d, "dx"))

    def oc(dx, arrived):
        s = wo_ref.at[:, :, :, wo_cols(dx, 1 - c if arrived else c)]
        return rcopy(s, s, oc_s.at[dx], oc_r.at[dx], at(dc=1))

    with jax.named_scope("issue"):
        for o in (2, 1, 3):
            for side in (0, 1):
                go(w_first(side, o, False))
        for o in (2, 1, 3):
            for side in (0, 1):
                go(w_second(side, 0, o, False))
        for dz in (2, 1, 3):
            go(oz_out(dz))
        for i in (0, 1):
            for d in (0, 1):
                go(x_out(d, i))
    with jax.named_scope("wait_wfirst"):
        for came in (1, 3, 2):
            for side in (0, 1):
                w_first(side, came, True).wait_recv()
                for o in (2, 1, 3):
                    go(w_second(side, came, o, False))
    with jax.named_scope("wait_oz"):
        for dz in (1, 3, 2):
            oz_in(dz).wait_recv()
        for d in (0, 1):
            go(oy(d, False))
    with jax.named_scope("wait_wsecond"):
        for d in (0, 1):
            go(ox(0, d, False))
        for o in (1, 3, 2):
            w_second(1, 0, o, True).wait_recv()
        go(w_c(0, False))
        for px in (1, 3, 2):
            for came in (0, 1, 3, 2):
                w_second(0, came, px, True).wait_recv()
            for o in (1, 3, 2):
                w_second(1, px, o, True).wait_recv()
            go(w_c(RING - px, False))
    pending = [[], [], [], []]

    def chunk(n, source, segments, stage_at):
        wide = source.astype(F32)
        normed = (
            wide * lax.rsqrt(jnp.mean(wide * wide, axis=-1, keepdims=True) + EPS) * gain_ref[...]
        ).astype(BF16)
        out = jnp.dot(normed, w_all[...], preferred_element_type=F32).astype(BF16)
        total = out.shape[0]
        v = out[:, 320:384]
        k = out[:, 256:320].reshape(total // 32, 2, 16, HEAD_DIM)
        for i in range(RING):
            stage_qv[i, pl.ds(stage_at, total)] = jnp.concatenate([out[:, i * 64 : i * 64 + 64], v], axis=1)
        stage_k[pl.ds(stage_at // 2, total // 2)] = jnp.concatenate([k[:, 0], k[:, 1]], axis=2).reshape(
            total // 2, 128
        )
        for dz, first, count in segments:
            here, here_k = pl.ds(stage_at, count), pl.ds(stage_at // 2, count // 2)
            nz = lax.rem(z + dz, RING)

            def spot(dy, halved):
                start = (nz * RING + lax.rem(y + dy, RING)) * rows + first
                if halved:
                    return pl.ds(pl.multiple_of(lax.div(start, 2), 16), count // 2)
                return pl.ds(pl.multiple_of(start, 32), count)

            for o in (2, 1, 3):
                ny = lax.rem(y + o, RING)
                go(rcopy(stage_qv.at[ny, here], qv_ref.at[spot(0, False)], a_s.at[n, o], a_r.at[n, o], at(dy=o)))
                go(rcopy(stage_k.at[here_k], kk_ref.at[spot(0, True)], b_s.at[n, o], b_r.at[n, o], at(dy=o)))
            qv_ref[spot(0, False)] = stage_qv[y, here]
            kk_ref[spot(0, True)] = stage_k[here_k]
            for o in (1, 3, 2):
                s, t = qv_ref.at[spot(RING - o, False)], kk_ref.at[spot(RING - o, True)]
                pending[dz].append(rcopy(s, s, a_s.at[n, o], a_r.at[n, o], at(dy=o)))
                pending[dz].append(rcopy(t, t, b_s.at[n, o], b_r.at[n, o], at(dy=o)))
            n, stage_at = n + 1, stage_at + count

    ratio = BLOCK_Q // BLOCK_K
    me = z * RING + y

    def place(dz):
        return lax.rem(z + dz, RING)

    def block_rows(i, size):
        return pl.ds(pl.multiple_of(i * size, size), size)

    def prepare(dz):
        for w in pending[dz]:
            w.wait_recv()
        i = place(dz)
        at_rows = block_rows(i, BLOCK_Q)
        packed = kk_ref[block_rows(i, BLOCK_Q // 2), :].reshape(BLOCK_Q // 32, 16, 128)
        k = jnp.concatenate([packed[:, :, 0:64], packed[:, :, 64:128]], axis=1).reshape(BLOCK_Q, HEAD_DIM)
        kk = k.astype(F32) * (LOG2E / 8.0)
        hi_part = kk.astype(BF16)
        lo_part = (kk - hi_part.astype(F32)).astype(BF16)
        keys_t[0:128, at_rows] = jnp.concatenate([hi_part, lo_part], axis=1).T
        both = qv_ref[at_rows, :]
        qa[at_rows, 0:128] = jnp.concatenate([both[:, 0:64], both[:, 0:64]], axis=1)
        vv[at_rows, :] = both[:, 64:128]

    def block(q, j, carry, diagonal=False):
        count = q.shape[0]
        cols = block_rows(j, BLOCK_K)
        l2 = jnp.dot(q, keys_t[:, cols], preferred_element_type=F32)
        if diagonal:
            t = lax.broadcasted_iota(jnp.int32, (BLOCK_K, BLOCK_K), 0)
            u = lax.broadcasted_iota(jnp.int32, (BLOCK_K, BLOCK_K), 1)
            first = jnp.where(u < t, l2[0:BLOCK_K], -1e30)
            l2 = first if count == BLOCK_K else jnp.concatenate([first, l2[BLOCK_K:]], axis=0)
        soft = jnp.maximum(l2, jnp.log2(1.0 + jnp.exp2(jnp.minimum(l2, 100.0))))
        drop = soft.astype(BF16)
        after = jnp.dot(drop, tri[...], preferred_element_type=F32)
        e = (l2 - soft) - after
        if carry is not None:
            e = e - jnp.concatenate([carry] * (BLOCK_K // 128), axis=1)
        pv = jnp.dot(jnp.exp2(e).astype(BF16), vv[cols, :], preferred_element_type=F32)
        whole = jnp.broadcast_to(after[:, 0:1] + soft[:, 0:1], (count, 128))
        return pv, whole if carry is None else carry + whole

    def diagonal(dz):
        i = place(dz)
        q = qa[block_rows(i, BLOCK_Q), 0:144]
        carry, total = None, None
        for d in reversed(range(ratio)):
            if carry is not None:
                carry = jnp.concatenate([jnp.zeros((BLOCK_K, 128), F32), carry], axis=0)
            pv, carry = block(q[d * BLOCK_K :], i * ratio + d, carry, True)
            if total is None:
                total = pv
            else:
                total = jnp.concatenate([pv[:BLOCK_K], pv[BLOCK_K:] + total], axis=0)
        part[i, i] = total
        rsum[i, i] = carry

    def pair(da, db):
        a, b = place(da), place(db)
        i, j = jnp.maximum(a, b), jnp.minimum(a, b)
        q = qa[block_rows(i, BLOCK_Q), 0:144]
        carry, total = None, None
        for d in reversed(range(ratio)):
            pv, carry = block(q, j * ratio + d, carry)
            total = pv if total is None else total + pv
        part[i, j] = total
        rsum[i, j] = carry

    def finish(i):
        acc[...] = part[i, i]
        car[...] = rsum[i, i]

        def add(n, _):
            j = i - 1 - n
            acc[...] += jnp.exp2(-car[...])[:, 0:HEAD_DIM] * part[i, j]
            car[...] += rsum[i, j]
            return 0

        lax.fori_loop(0, i, add, 0)
        pair_gain = g_all[0:1, block_rows(lax.div(me, 2), 128)]
        own_gain = jnp.where(lax.rem(me, 2) == 0, pair_gain[:, 0:64], pair_gain[:, 64:128])
        a = acc[...]
        scaled = a * lax.rsqrt(jnp.mean(a * a, axis=-1, keepdims=True) + EPS)
        head = (scaled * own_gain).astype(BF16)
        for yy in range(RING):
            mine = head[yy * rows : (yy + 1) * rows]
            stage[i * RING + yy] = jnp.concatenate([mine[:half], mine[half:]], axis=1)
        for yy in range(RING):
            dest = i * RING + yy

            @pl.when(dest != me)
            def _():
                rcopy(
                    stage.at[dest], ho_ref.at[y * RING + z], h_s.at[dest], h_r.at[me],
                    {"sp": dest, "dp": lax.axis_index("dp")},
                ).start()

            @pl.when(dest == me)
            def _():
                ho_ref[y * RING + z] = stage[dest]

    with jax.named_scope("constants"):
        r = lax.broadcasted_iota(jnp.int32, (BLOCK_K, BLOCK_K), 0)
        u = lax.broadcasted_iota(jnp.int32, (BLOCK_K, BLOCK_K), 1)
        tri[...] = jnp.where(r > u, 1.0, 0.0).astype(BF16)
        length = qv_ref.shape[0]
        lane = lax.broadcasted_iota(jnp.int32, (length, 128), 1)
        qa[:, 128:256] = jnp.where(lane < 3, 1.0, 0.0).astype(BF16)
        bb = b_ref[...] * LOG2E
        bh = bb.astype(BF16)
        r1 = bb - bh.astype(F32)
        bm = r1.astype(BF16)
        bl = (r1 - bm.astype(F32)).astype(BF16)
        keys_t[128:144, :] = jnp.concatenate([bh, bm, bl, jnp.zeros((13, length), BF16)], axis=0)
    with jax.named_scope("wait_wc"):
        for dx in (0, 3, 1, 2):
            w_c(dx, True).wait_recv()
    with jax.named_scope("assemble"):
        for n in range(2 * RING):
            for side in (0, 1):
                p = [packs[n % 2, n // 2, i, side] for i in range(RING)]
                first = n * depth + side * split
                w_all[first : first + split, :] = jnp.concatenate(
                    [t[0:qn] for t in p] + [t[qn : qn + kn] for t in p] + [t[qn + kn :] for t in p], axis=0
                ).T
    with jax.named_scope("chunk0"):
        chunk(0, x_ref[...], ((0, 0, rows),), 0)
    with jax.named_scope("wait_oy"):
        for d in (0, 1):
            oy(d, True).wait_recv()
            go(oy_far(d, back(d)))
        for o in (1, 3):
            for d in (0, 1):
                go(ox(o, d, False))
    with jax.named_scope("wait_x0"):
        for d in (0, 1):
            x_in(d, 0).wait_recv()
            for i in (0, 1):
                go(far_z(d, i, False))
    with jax.named_scope("chunk12"):
        chunk(
            1,
            jnp.concatenate([xg[0, parts[0][0]], xg[1, parts[1][0]]], axis=0),
            ((3, 0, 2 * third), (1, third, 2 * third)),
            rows,
        )
    with jax.named_scope("prepare_own"):
        prepare(0)
    with jax.named_scope("diagonal_own"):
        diagonal(0)
    with jax.named_scope("wait_x1"):
        x_in(0, 1).wait_recv()
        x_in(1, 1).wait_recv()
    with jax.named_scope("chunk34"):
        chunk(
            3,
            jnp.concatenate([xg[0, parts[0][1]], xg[1, parts[1][1]]], axis=0),
            ((3, 2 * third, third), (1, 0, third)),
            rows + 4 * third,
        )
    with jax.named_scope("wait_oyfar"):
        for d in (0, 1):
            oy_far(d, 2).wait_recv()
        for d in (0, 1):
            go(ox(2, d, False))
        go(oc(0, False))
    def far_chunk(i):
        a, count = cuts[i]
        with jax.named_scope("wait_far%d" % i):
            for d in (0, 1):
                far_z(d, i, True).wait_recv()
        with jax.named_scope("chunk_far%d" % i):
            chunk(
                5 + 2 * i,
                jnp.concatenate([xg[2, pl.ds(a, count)], xg[2, pl.ds(a + half, count)]], axis=0),
                ((2, a, count), (2, a + half, count)),
                3 * rows + 2 * i * cuts[0][1],
            )

    with jax.named_scope("wait_ox"):
        for o in (0, 1, 3):
            for d in (0, 1):
                ox(o, d, True).wait_recv()
                go(ox_far(o, d, back(d)))

    with jax.named_scope("prepare_near"):
        prepare(3)
        prepare(1)
    far_chunk(0)
    far_chunk(1)
    with jax.named_scope("wait_ox2"):
        for d in (0, 1):
            ox(2, d, True).wait_recv()
            go(ox_far(2, d, back(d)))
        go(oc(3, False))
        go(oc(1, False))
    with jax.named_scope("blocks_near"):
        diagonal(3)
        diagonal(1)
        pair(0, 3)
        pair(0, 1)
        pair(3, 1)

    far = place(2)
    with jax.named_scope("wait_oxfar"):
        for o in (0, 1, 3, 2):
            for d in (0, 1):
                ox_far(o, d, 2).wait_recv()
        go(oc(2, False))
    with jax.named_scope("finish_early"):

        @pl.loop(0, far)
        def _(i):
            finish(i)

    with jax.named_scope("prepare_far"):
        prepare(2)
    with jax.named_scope("blocks_far"):
        diagonal(2)
        pair(2, 0)
        pair(2, 3)
        pair(2, 1)
    with jax.named_scope("finish_late"):

        @pl.loop(far, RING)
        def _(i):
            finish(i)

    with jax.named_scope("wait_ho"):
        for dz in range(RING):
            for dy in range(RING):
                if dz or dy:
                    nz, ny = lax.rem(z + dz, RING), lax.rem(y + dy, RING)
                    other = nz * RING + ny
                    slot = ho_ref.at[ny * RING + nz]
                    w = rcopy(slot, slot, h_s.at[other], h_r.at[other], at(dz=dz, dy=dy))
                    w.wait_recv()
                    w.wait_send()
    with jax.named_scope("wait_oc"):
        for dx in (0, 3, 1, 2):
            oc(dx, True).wait_recv()
    with jax.named_scope("wait_send"):
        for t in sent:
            t.wait_send()


BLOCK_Q = 768
BLOCK_K = 256


def layer(x, gain, wq, wk, wv, wo, bias, out_gain):
    rows, width = x.shape
    length = rows * RING * RING
    depth = wq.shape[1]
    dma = pltpu.SemaphoreType.DMA
    vmem = pl.BlockSpec(memory_space=pltpu.VMEM)
    operands = [
        pltpu.with_memory_space_constraint(t, pltpu.HBM) for t in (x, gain, wq, wk, wv, wo, bias, out_gain)
    ]
    return pl.pallas_call(
        layer_kernel,
        name="layer",
        out_shape=(
            jax.ShapeDtypeStruct((RING * RING, rows // 2, 2 * HEAD_DIM), BF16),
            jax.ShapeDtypeStruct((RING, RING, wo.shape[0], wo.shape[1] * 2 * RING), BF16),
        ),
        in_specs=[pl.BlockSpec(memory_space=pltpu.HBM)] * 8,
        out_specs=(vmem, vmem),
        scratch_shapes=[
            pltpu.VMEM((length, 128), BF16),
            pltpu.VMEM((length // 2, 128), BF16),
            pltpu.VMEM((144, length), BF16),
            pltpu.VMEM((length, 256), BF16),
            pltpu.VMEM((length, HEAD_DIM), BF16),
            pltpu.VMEM((BLOCK_K, BLOCK_K), BF16),
            pltpu.VMEM((RING, RING, BLOCK_Q, HEAD_DIM), F32),
            pltpu.VMEM((RING, RING, BLOCK_Q, 128), F32),
            pltpu.VMEM((BLOCK_Q, HEAD_DIM), F32),
            pltpu.VMEM((BLOCK_Q, 128), F32),
            pltpu.VMEM((RING * RING, rows // 2, 2 * HEAD_DIM), BF16),
            dma((RING * RING,)), dma((RING * RING,)),
            pltpu.VMEM(bias.shape, F32), pltpu.VMEM(out_gain.shape, F32),
            pltpu.VMEM((2, RING, RING, 2, 96, depth // 2), BF16),
            pltpu.VMEM((width, 384), BF16),
            pltpu.VMEM((3, rows, width), BF16),
            pltpu.VMEM((RING, RING * rows, 128), BF16),
            pltpu.VMEM((RING * rows // 2, 128), BF16),
            dma((2, 4)), dma((2, 4)), dma((2, 4, 4)), dma((2, 4, 4)), dma((4,)), dma((4,)),
            dma((2, 2)), dma((2, 2)), dma((2, 2)), dma((2, 2)),
            dma((9, 4)), dma((9, 4)), dma((9, 4)), dma((9, 4)),
            dma((4,)), dma((4,)), dma((2, 2)), dma((2, 2)), dma((2, 4)), dma((2, 4)),
            dma((2, 4)), dma((2, 4)), dma((4,)), dma((4,)), dma((8,)),
            pltpu.VMEM(x.shape, BF16), pltpu.VMEM(gain.shape, F32), pltpu.VMEM(wq.shape, BF16),
            pltpu.VMEM(wk.shape, BF16), pltpu.VMEM(wv.shape, BF16), pltpu.VMEM(wo.shape, BF16),
        ],
        compiler_params=pltpu.CompilerParams(
            collective_id=0, has_side_effects=True, vmem_limit_bytes=44 << 20
        ),
    )(*operands)


def mix_kernel(ho_ref, wo_ref, o_ref, lhs):
    heads, half, _ = ho_ref.shape
    for n in range(0, heads, 2):
        a, b = ho_ref[n], ho_ref[n + 1]
        cols = pl.ds(n * HEAD_DIM, 2 * HEAD_DIM)
        lhs[0:half, cols] = jnp.concatenate([a[:, 0:64], b[:, 0:64]], axis=1)
        lhs[half : 2 * half, cols] = jnp.concatenate([a[:, 64:128], b[:, 64:128]], axis=1)
    width = o_ref.shape[1]
    for n in range(0, width, 512):
        o_ref[:, n : n + 512] = jnp.dot(
            lhs[...], wo_ref[:, n : n + 512], preferred_element_type=F32
        ).astype(BF16)


def mix(ho, wo):
    heads, half, _ = ho.shape
    vmem = pl.BlockSpec(memory_space=pltpu.VMEM)
    return pl.pallas_call(
        mix_kernel,
        name="mix",
        out_shape=jax.ShapeDtypeStruct((2 * half, wo.shape[1]), BF16),
        in_specs=[vmem] * 2,
        out_specs=vmem,
        scratch_shapes=[pltpu.VMEM((2 * half, heads * HEAD_DIM), BF16)],
        compiler_params=pltpu.CompilerParams(vmem_limit_bytes=16 << 20),
    )(ho, wo)


def body(inputs, in_gain, w_query, w_key, w_value, key_bias, out_gain, w_out):
    ho, wo = layer(
        inputs[0], in_gain[None], w_query.T, w_key.T, w_value.T, w_out, key_bias[0].T, out_gain[None]
    )
    return mix(ho, wo.reshape(-1, wo.shape[-1]))[None]


def solution(mesh):
    placed = (
        P("dp", "sp", None), P(), P("dp", "sp"), P("dp", "sp"), P("dp", "sp"),
        P("dp", None, "sp"), P(), P("sp", "dp"),
    )
    return jax.shard_map(body, mesh=mesh, in_specs=placed, out_specs=P("dp", "sp", None), check_vma=False)
```

```python
import functools

import jax
import jax.numpy as jnp
from jax import lax
from jax.experimental import pallas as pl
from jax.experimental.pallas import tpu as pltpu
from jax.sharding import PartitionSpec as P

HEAD_DIM = 64
RING = 4
EPS = 1e-06
LOG2E = 1.4426950408889634
F32 = jnp.float32
BF16 = jnp.bfloat16
MESH = pl.DeviceIdType.MESH


def rcopy(src, dst, send, recv, device):
    return pltpu.make_async_remote_copy(
        src_ref=src, dst_ref=dst, send_sem=send, recv_sem=recv, device_id=device, device_id_type=MESH
    )


def places():
    sp, dp = lax.axis_index("sp"), lax.axis_index("dp")
    z, y = lax.div(sp, RING), lax.rem(sp, RING)
    x, c = lax.div(dp, 2), lax.rem(dp, 2)

    def at(dz=0, dy=0, dx=0, dc=0):
        nz, ny = lax.rem(z + dz, RING), lax.rem(y + dy, RING)
        nx, nc = lax.rem(x + dx, RING), lax.rem(c + dc, 2)
        return {"sp": nz * RING + ny, "dp": nx * 2 + nc}

    return z, y, x, c, at


def layer_kernel(
    x_hbm, gain_hbm, wq_hbm, wk_hbm, wv_hbm, wo_hbm, b_hbm, g_hbm,
    ho_ref, wo_ref,
    qv_ref, kk_ref, keys_t, qa, vv, tri, part, rsum, acc, car, stage, h_s, h_r, b_ref, g_all,
    packs, w_all, xg, stage_qv, stage_k,
    wa_s, wa_r, wb_s, wb_r, wc_s, wc_r, xd_s, xd_r, xf_s, xf_r, a_s, a_r,
    oz_s, oz_r, oy_s, oy_r, ox_s, ox_r, of_s, of_r, oc_s, oc_r, local_sem,
    x_ref, gain_ref, wq_ref, wk_ref, wv_ref, wo_in,
):
    z, y, x, c, at = places()
    loads = [
        pltpu.make_async_copy(s, d, local_sem.at[i])
        for i, (s, d) in enumerate(
            (
                (wq_hbm, wq_ref), (wk_hbm, wk_ref), (wv_hbm, wv_ref), (wo_hbm, wo_in),
                (gain_hbm, gain_ref), (x_hbm, x_ref), (b_hbm, b_ref), (g_hbm, g_all),
            )
        )
    ]
    for load in loads:
        load.start()
    friends = [at(dz=i, dy=j) for i in range(RING) for j in range(RING) if i or j]
    friends += [at(dx=1), at(dx=2), at(dx=3), at(dc=1)]
    barrier = pltpu.get_barrier_semaphore()
    for f in friends:
        pl.semaphore_signal(barrier, inc=1, device_id=f, device_id_type=MESH)
    for load in loads:
        load.wait()
    rows = x_ref.shape[0]
    half = rows // 2
    depth = wq_ref.shape[1]
    qn, kn = wq_ref.shape[0], wk_ref.shape[0]
    split = depth // 2
    piece_rows = qn + 2 * kn
    own_piece = jnp.concatenate([wq_ref[...], wk_ref[...], wv_ref[...]], axis=0)
    packs[c, x, y, 0] = own_piece[:, 0:split]
    packs[c, x, y, 1] = own_piece[:, split:]

    def wo_cols(dx, cc):
        return pl.ds(pl.multiple_of((lax.rem(x + dx, RING) * 2 + cc) * depth, depth), depth)

    wo_ref[y, z, :, wo_cols(0, c)] = wo_in[...]
    pl.semaphore_wait(barrier, len(friends))

    def go(copy):
        copy.start()

    def settle(sem, count):
        ref = qv_ref.at[pl.ds(0, count)]
        pltpu.make_async_copy(ref, ref, sem).wait()

    def near(d, axis):
        return at(**{axis: 1 if d == 0 else 3})

    def back(d):
        return 3 if d == 0 else 1


    def oz(dz, n):
        return wo_ref.at[y, lax.rem(z + dz, RING), n, wo_cols(0, c)]

    every = slice(None)
    wo_rows = wo_in.shape[0] * wo_in.shape[1] // 128

    def oz_out(dz):
        return rcopy(wo_in, oz(0, every), oz_s, oz_r, at(dz=dz))

    third = rows // 3
    parts = (
        (pl.ds(0, 2 * third), pl.ds(2 * third, third)),
        (pl.ds(third, 2 * third), pl.ds(0, third)),
    )

    def x_out(d, i):
        p = parts[d][i]
        return rcopy(x_ref.at[p], xg.at[d, p], xd_s, xd_r.at[d, i], near(d, "dz"))

    def x_in(d, i):
        p = parts[d][i]
        return rcopy(xg.at[d, p], xg.at[d, p], xd_s, xd_r.at[d, i], near(d, "dz"))

    cuts = ((0, 64), (64, 32))

    def far_z(d, i):
        a, n = cuts[i]
        part = pl.ds(a + (0 if d == 0 else half), n)
        return rcopy(xg.at[d, part], xg.at[2, part], xf_s, xf_r.at[i], near(d, "dz"))

    def piece(o):
        return lax.rem(y + RING - o, RING)

    def w_first(side, o, arrived):
        py = piece(o) if arrived and side == 0 else y
        px = lax.rem(x + RING - o, RING) if arrived and side == 1 else x
        p = packs.at[c, px, py, side]
        return rcopy(p, p, wa_s, wa_r.at[side, o - 1], at(dy=o) if side == 0 else at(dx=o))

    def w_second(side, came, o):
        p = packs.at[c, lax.rem(x + RING - (came if side else 0), RING), piece(0 if side else came), side]
        return rcopy(p, p, wb_s, wb_r.at[came if side else o], at(dy=o) if side else at(dx=o))

    def w_c(dx):
        slab = packs.at[c, lax.rem(x + dx, RING)]
        return rcopy(slab, slab, wc_s, wc_r, at(dc=1))

    def oy(d, arrived):
        s = wo_ref.at[lax.rem(y + back(d), RING) if arrived else y, :, :, wo_cols(0, c)]
        return rcopy(s, s, oy_s, oy_r.at[d], near(d, "dy"))

    def oy_far(d, dy):
        s = wo_ref.at[lax.rem(y + dy, RING), pl.ds(0 if d == 0 else 2, 2), :, wo_cols(0, c)]
        return rcopy(s, s, oy_s, oy_r.at[2], near(d, "dy"))

    def ox(o, d):
        s = wo_ref.at[piece(o), :, :, wo_cols(0, c)]
        return rcopy(s, s, ox_s, ox_r.at[1 if o == 2 else 0], near(d, "dx"))

    def ox_far(o, d, dx):
        s = wo_ref.at[piece(o), pl.ds(0 if d == 0 else 2, 2), :, wo_cols(dx, c)]
        return rcopy(s, s, of_s, of_r, near(d, "dx"))

    def oc(dx):
        s = wo_ref.at[:, :, :, wo_cols(dx, c)]
        return rcopy(s, s, oc_s, oc_r, at(dc=1))

    with jax.named_scope("issue"):
        for o in (2, 1, 3):
            for side in (0, 1):
                go(w_first(side, o, False))
        for o in (2, 1, 3):
            for side in (0, 1):
                go(w_second(side, 0, o))
        for dz in (2, 1, 3):
            go(oz_out(dz))
        for i in (0, 1):
            for d in (0, 1):
                go(x_out(d, i))
    with jax.named_scope("wait_wfirst"):
        for came in (1, 3, 2):
            for side in (0, 1):
                w_first(side, came, True).wait_recv()
                for o in (2, 1, 3):
                    go(w_second(side, came, o))
    with jax.named_scope("wait_oz"):
        settle(oz_r, 3 * wo_rows)
        for d in (0, 1):
            go(oy(d, False))
    with jax.named_scope("wait_wsecond"):
        for d in (0, 1):
            go(ox(0, d))
        settle(wb_r.at[0], 3 * piece_rows)
        go(w_c(0))
        for px in (1, 3, 2):
            settle(wb_r.at[px], 7 * piece_rows)
            go(w_c(RING - px))
    def chunk(source, segments, stage_at):
        wide = source.astype(F32)
        normed = (
            wide * lax.rsqrt(jnp.mean(wide * wide, axis=-1, keepdims=True) + EPS) * gain_ref[...]
        ).astype(BF16)
        out = jnp.dot(normed, w_all[...], preferred_element_type=F32).astype(BF16)
        total = out.shape[0]
        v = out[:, 320:384]
        k = out[:, 256:320].reshape(total // 32, 2, 16, HEAD_DIM)
        for i in range(RING):
            stage_qv[i, pl.ds(stage_at, total)] = jnp.concatenate([out[:, i * 64 : i * 64 + 64], v], axis=1)
        stage_k[pl.ds(stage_at // 2, total // 2)] = jnp.concatenate([k[:, 0], k[:, 1]], axis=2).reshape(
            total // 2, 128
        )
        for dz, first, count in segments:
            here, here_k = pl.ds(stage_at, count), pl.ds(stage_at // 2, count // 2)
            nz = lax.rem(z + dz, RING)

            def spot(halved):
                start = (nz * RING + y) * rows + first
                if halved:
                    return pl.ds(pl.multiple_of(lax.div(start, 2), 16), count // 2)
                return pl.ds(pl.multiple_of(start, 32), count)

            for o in (2, 1, 3):
                ny = lax.rem(y + o, RING)
                go(rcopy(stage_qv.at[ny, here], qv_ref.at[spot(False)], a_s.at[dz], a_r.at[dz, o - 1], at(dy=o)))
                go(rcopy(stage_k.at[here_k], kk_ref.at[spot(True)], a_s.at[dz], a_r.at[dz, o - 1], at(dy=o)))
            qv_ref[spot(False)] = stage_qv[y, here]
            kk_ref[spot(True)] = stage_k[here_k]
            stage_at = stage_at + count

    ratio = BLOCK_Q // BLOCK_K
    me = z * RING + y

    def place(dz):
        return lax.rem(z + dz, RING)

    def block_rows(i, size):
        return pl.ds(pl.multiple_of(i * size, size), size)

    def prepare(dz):
        for o in range(RING - 1):
            settle(a_r.at[dz, o], rows + half)
        i = place(dz)
        at_rows = block_rows(i, BLOCK_Q)
        packed = kk_ref[block_rows(i, BLOCK_Q // 2), :].reshape(BLOCK_Q // 32, 16, 128)
        k = jnp.concatenate([packed[:, :, 0:64], packed[:, :, 64:128]], axis=1).reshape(BLOCK_Q, HEAD_DIM)
        kk = k.astype(F32) * (LOG2E / 8.0)
        hi_part = kk.astype(BF16)
        lo_part = (kk - hi_part.astype(F32)).astype(BF16)
        keys_t[0:128, at_rows] = jnp.concatenate([hi_part, lo_part], axis=1).T
        both = qv_ref[at_rows, :]
        qa[at_rows, 0:128] = jnp.concatenate([both[:, 0:64], both[:, 0:64]], axis=1)
        vv[at_rows, :] = both[:, 64:128]

    def block(q, j, carry, diagonal=False):
        count = q.shape[0]
        cols = block_rows(j, BLOCK_K)
        l2 = jnp.dot(q, keys_t[:, cols], preferred_element_type=F32)
        if diagonal:
            t = lax.broadcasted_iota(jnp.int32, (BLOCK_K, BLOCK_K), 0)
            u = lax.broadcasted_iota(jnp.int32, (BLOCK_K, BLOCK_K), 1)
            first = jnp.where(u < t, l2[0:BLOCK_K], -1e30)
            l2 = first if count == BLOCK_K else jnp.concatenate([first, l2[BLOCK_K:]], axis=0)
        soft = jnp.maximum(l2, jnp.log2(1.0 + jnp.exp2(jnp.minimum(l2, 100.0))))
        drop = soft.astype(BF16)
        after = jnp.dot(drop, tri[...], preferred_element_type=F32)
        e = (l2 - soft) - after
        if carry is not None:
            e = e - jnp.concatenate([carry] * (BLOCK_K // 128), axis=1)
        pv = jnp.dot(jnp.exp2(e).astype(BF16), vv[cols, :], preferred_element_type=F32)
        whole = jnp.broadcast_to(after[:, 0:1] + soft[:, 0:1], (count, 128))
        return pv, whole if carry is None else carry + whole

    def diagonal(dz):
        i = place(dz)
        q = qa[block_rows(i, BLOCK_Q), 0:144]
        carry, total = None, None
        for d in reversed(range(ratio)):
            if carry is not None:
                carry = jnp.concatenate([jnp.zeros((BLOCK_K, 128), F32), carry], axis=0)
            pv, carry = block(q[d * BLOCK_K :], i * ratio + d, carry, True)
            if total is None:
                total = pv
            else:
                total = jnp.concatenate([pv[:BLOCK_K], pv[BLOCK_K:] + total], axis=0)
        part[i, i] = total
        rsum[i, i] = carry

    def pair(da, db):
        a, b = place(da), place(db)
        i, j = jnp.maximum(a, b), jnp.minimum(a, b)
        q = qa[block_rows(i, BLOCK_Q), 0:144]
        carry, total = None, None
        for d in reversed(range(ratio)):
            pv, carry = block(q, j * ratio + d, carry)
            total = pv if total is None else total + pv
        part[i, j] = total
        rsum[i, j] = carry

    def finish(i):
        acc[...] = part[i, i]
        car[...] = rsum[i, i]

        def add(n, _):
            j = i - 1 - n
            acc[...] += jnp.exp2(-car[...])[:, 0:HEAD_DIM] * part[i, j]
            car[...] += rsum[i, j]
            return 0

        lax.fori_loop(0, i, add, 0)
        pair_gain = g_all[0:1, block_rows(lax.div(me, 2), 128)]
        own_gain = jnp.where(lax.rem(me, 2) == 0, pair_gain[:, 0:64], pair_gain[:, 64:128])
        a = acc[...]
        scaled = a * lax.rsqrt(jnp.mean(a * a, axis=-1, keepdims=True) + EPS)
        head = (scaled * own_gain).astype(BF16)
        for yy in range(RING):
            mine = head[yy * rows : (yy + 1) * rows]
            stage[i * RING + yy] = jnp.concatenate([mine[:half], mine[half:]], axis=1)
        for yy in range(RING):
            dest = i * RING + yy

            @pl.when(dest != me)
            def _():
                rcopy(
                    stage.at[dest], ho_ref.at[y * RING + z], h_s, h_r,
                    {"sp": dest, "dp": lax.axis_index("dp")},
                ).start()

            @pl.when(dest == me)
            def _():
                ho_ref[y * RING + z] = stage[dest]

    with jax.named_scope("constants"):
        r = lax.broadcasted_iota(jnp.int32, (BLOCK_K, BLOCK_K), 0)
        u = lax.broadcasted_iota(jnp.int32, (BLOCK_K, BLOCK_K), 1)
        tri[...] = jnp.where(r > u, 1.0, 0.0).astype(BF16)
        length = qv_ref.shape[0]
        lane = lax.broadcasted_iota(jnp.int32, (length, 128), 1)
        qa[:, 128:256] = jnp.where(lane < 3, 1.0, 0.0).astype(BF16)
        bb = b_ref[...] * LOG2E
        bh = bb.astype(BF16)
        r1 = bb - bh.astype(F32)
        bm = r1.astype(BF16)
        bl = (r1 - bm.astype(F32)).astype(BF16)
        keys_t[128:144, :] = jnp.concatenate([bh, bm, bl, jnp.zeros((13, length), BF16)], axis=0)
    with jax.named_scope("wait_wc"):
        settle(wc_r, RING * RING * 2 * piece_rows)
    with jax.named_scope("assemble"):
        for n in range(2 * RING):
            for side in (0, 1):
                p = [packs[n % 2, n // 2, i, side] for i in range(RING)]
                first = n * depth + side * split
                w_all[first : first + split, :] = jnp.concatenate(
                    [t[0:qn] for t in p] + [t[qn : qn + kn] for t in p] + [t[qn + kn :] for t in p], axis=0
                ).T
    with jax.named_scope("chunk0"):
        chunk(x_ref[...], ((0, 0, rows),), 0)
    with jax.named_scope("wait_oy"):
        for d in (0, 1):
            oy(d, True).wait_recv()
            go(oy_far(d, back(d)))
        for o in (1, 3):
            for d in (0, 1):
                go(ox(o, d))
    with jax.named_scope("wait_x0"):
        for d in (0, 1):
            x_in(d, 0).wait_recv()
            for i in (0, 1):
                go(far_z(d, i))
    with jax.named_scope("chunk12"):
        chunk(
            jnp.concatenate([xg[0, parts[0][0]], xg[1, parts[1][0]]], axis=0),
            ((3, 0, 2 * third), (1, third, 2 * third)),
            rows,
        )
    with jax.named_scope("prepare_own"):
        prepare(0)
    with jax.named_scope("diagonal_own"):
        diagonal(0)
    with jax.named_scope("wait_x1"):
        x_in(0, 1).wait_recv()
        x_in(1, 1).wait_recv()
    with jax.named_scope("chunk34"):
        chunk(
            jnp.concatenate([xg[0, parts[0][1]], xg[1, parts[1][1]]], axis=0),
            ((3, 2 * third, third), (1, 0, third)),
            rows + 4 * third,
        )
    with jax.named_scope("wait_oyfar"):
        settle(oy_r.at[2], RING * wo_rows)
        for d in (0, 1):
            go(ox(2, d))
        go(oc(0))
    def far_chunk(i):
        a, count = cuts[i]
        with jax.named_scope("wait_far%d" % i):
            settle(xf_r.at[i], 2 * count * x_ref.shape[1] // 128)
        with jax.named_scope("chunk_far%d" % i):
            chunk(
                jnp.concatenate([xg[2, pl.ds(a, count)], xg[2, pl.ds(a + half, count)]], axis=0),
                ((2, a, count), (2, a + half, count)),
                3 * rows + 2 * i * cuts[0][1],
            )

    with jax.named_scope("wait_ox"):
        settle(ox_r.at[0], 6 * RING * wo_rows)
        for o in (0, 1, 3):
            for d in (0, 1):
                go(ox_far(o, d, back(d)))

    with jax.named_scope("prepare_near"):
        prepare(3)
        prepare(1)
    far_chunk(0)
    far_chunk(1)
    with jax.named_scope("wait_ox2"):
        settle(ox_r.at[1], 2 * RING * wo_rows)
        for d in (0, 1):
            go(ox_far(2, d, back(d)))
        go(oc(3))
        go(oc(1))
    with jax.named_scope("blocks_near"):
        diagonal(3)
        diagonal(1)
        pair(0, 3)
        pair(0, 1)
        pair(3, 1)

    far = place(2)
    with jax.named_scope("wait_oxfar"):
        settle(of_r, RING * RING * wo_rows)
        go(oc(2))
    with jax.named_scope("finish_early"):

        @pl.loop(0, far)
        def _(i):
            finish(i)

    with jax.named_scope("prepare_far"):
        prepare(2)
    with jax.named_scope("diagonal_far"):
        diagonal(2)
    with jax.named_scope("blocks_far"):

        @pl.loop(0, RING)
        def _(i):
            @pl.when(i < far)
            def _():
                pair(2, i - z + RING)

            @pl.when(i > far)
            def _():
                pair(2, i - z + RING)
                finish(i)

            @pl.when(i == far)
            def _():
                finish(i)

    whole_w = wo_ref.at[:, :, :, pl.ds(0, RING * depth)]
    ho_rows = (RING * RING - 1) * half
    with jax.named_scope("wait_ho"):
        settle(h_r, ho_rows)
    with jax.named_scope("wait_oc"):
        pltpu.make_async_copy(whole_w, whole_w, oc_r).wait()
    with jax.named_scope("wait_send"):
        settle(h_s, ho_rows)
        pltpu.make_async_copy(whole_w, whole_w, oc_s).wait()
        both_x = xg.at[pl.ds(0, 2)]
        pltpu.make_async_copy(both_x, both_x, xd_s).wait()
        one_x = xg.at[0]
        pltpu.make_async_copy(one_x, one_x, xf_s).wait()
        settle(wa_s, 6 * piece_rows)
        settle(wb_s, 24 * piece_rows)
        settle(wc_s, RING * RING * 2 * piece_rows)
        settle(oz_s, 3 * wo_rows)
        settle(oy_s, 3 * RING * wo_rows)
        x_w = wo_ref.at[:, :, :, pl.ds(0, 2 * depth)]
        pltpu.make_async_copy(x_w, x_w, ox_s).wait()
        settle(of_s, RING * RING * wo_rows)
        for dz in range(RING):
            settle(a_s.at[dz], 3 * (rows + half))


BLOCK_Q = 768
BLOCK_K = 256


def layer(x, gain, wq, wk, wv, wo, bias, out_gain):
    rows, width = x.shape
    length = rows * RING * RING
    depth = wq.shape[1]
    dma = pltpu.SemaphoreType.DMA
    vmem = pl.BlockSpec(memory_space=pltpu.VMEM)
    operands = [
        pltpu.with_memory_space_constraint(t, pltpu.HBM) for t in (x, gain, wq, wk, wv, wo, bias, out_gain)
    ]
    return pl.pallas_call(
        layer_kernel,
        name="layer",
        out_shape=(
            jax.ShapeDtypeStruct((RING * RING, rows // 2, 2 * HEAD_DIM), BF16),
            jax.ShapeDtypeStruct((RING, RING, wo.shape[0], wo.shape[1] * 2 * RING), BF16),
        ),
        in_specs=[pl.BlockSpec(memory_space=pltpu.HBM)] * 8,
        out_specs=(vmem, vmem),
        scratch_shapes=[
            pltpu.VMEM((length, 128), BF16),
            pltpu.VMEM((length // 2, 128), BF16),
            pltpu.VMEM((144, length), BF16),
            pltpu.VMEM((length, 256), BF16),
            pltpu.VMEM((length, HEAD_DIM), BF16),
            pltpu.VMEM((BLOCK_K, BLOCK_K), BF16),
            pltpu.VMEM((RING, RING, BLOCK_Q, HEAD_DIM), F32),
            pltpu.VMEM((RING, RING, BLOCK_Q, 128), F32),
            pltpu.VMEM((BLOCK_Q, HEAD_DIM), F32),
            pltpu.VMEM((BLOCK_Q, 128), F32),
            pltpu.VMEM((RING * RING, rows // 2, 2 * HEAD_DIM), BF16),
            dma(()), dma(()),
            pltpu.VMEM(bias.shape, F32), pltpu.VMEM(out_gain.shape, F32),
            pltpu.VMEM((2, RING, RING, 2, 96, depth // 2), BF16),
            pltpu.VMEM((width, 384), BF16),
            pltpu.VMEM((3, rows, width), BF16),
            pltpu.VMEM((RING, RING * rows, 128), BF16),
            pltpu.VMEM((RING * rows // 2, 128), BF16),
            dma(()), dma((2, 3)), dma(()), dma((4,)), dma(()), dma(()),
            dma(()), dma((2, 2)), dma(()), dma((2,)),
            dma((4,)), dma((4, 3)),
            dma(()), dma(()), dma(()), dma((3,)), dma(()), dma((2,)),
            dma(()), dma(()), dma(()), dma(()), dma((8,)),
            pltpu.VMEM(x.shape, BF16), pltpu.VMEM(gain.shape, F32), pltpu.VMEM(wq.shape, BF16),
            pltpu.VMEM(wk.shape, BF16), pltpu.VMEM(wv.shape, BF16), pltpu.VMEM(wo.shape, BF16),
        ],
        compiler_params=pltpu.CompilerParams(
            collective_id=0, has_side_effects=True, vmem_limit_bytes=44 << 20
        ),
    )(*operands)


def mix_kernel(ho_ref, wo_ref, o_ref, lhs):
    heads, half, _ = ho_ref.shape
    for n in range(0, heads, 2):
        a, b = ho_ref[n], ho_ref[n + 1]
        cols = pl.ds(n * HEAD_DIM, 2 * HEAD_DIM)
        lhs[0:half, cols] = jnp.concatenate([a[:, 0:64], b[:, 0:64]], axis=1)
        lhs[half : 2 * half, cols] = jnp.concatenate([a[:, 64:128], b[:, 64:128]], axis=1)
    width = o_ref.shape[1]
    for n in range(0, width, 512):
        o_ref[:, n : n + 512] = jnp.dot(
            lhs[...], wo_ref[:, n : n + 512], preferred_element_type=F32
        ).astype(BF16)


def mix(ho, wo):
    heads, half, _ = ho.shape
    vmem = pl.BlockSpec(memory_space=pltpu.VMEM)
    return pl.pallas_call(
        mix_kernel,
        name="mix",
        out_shape=jax.ShapeDtypeStruct((2 * half, wo.shape[1]), BF16),
        in_specs=[vmem] * 2,
        out_specs=vmem,
        scratch_shapes=[pltpu.VMEM((2 * half, heads * HEAD_DIM), BF16)],
        compiler_params=pltpu.CompilerParams(vmem_limit_bytes=16 << 20),
    )(ho, wo)


def body(inputs, in_gain, w_query, w_key, w_value, key_bias, out_gain, w_out):
    ho, wo = layer(
        inputs[0], in_gain[None], w_query.T, w_key.T, w_value.T, w_out, key_bias[0].T, out_gain[None]
    )
    return mix(ho, wo.reshape(-1, wo.shape[-1]))[None]


def solution(mesh):
    placed = (
        P("dp", "sp", None), P(), P("dp", "sp"), P("dp", "sp"), P("dp", "sp"),
        P("dp", None, "sp"), P(), P("sp", "dp"),
    )
    return jax.shard_map(body, mesh=mesh, in_specs=placed, out_specs=P("dp", "sp", None), check_vma=False)
```

```python
import functools

import jax
import jax.numpy as jnp
from jax import lax
from jax.experimental import pallas as pl
from jax.experimental.pallas import tpu as pltpu
from jax.sharding import PartitionSpec as P

HEAD_DIM = 64
RING = 4
EPS = 1e-06
LOG2E = 1.4426950408889634
F32 = jnp.float32
BF16 = jnp.bfloat16
MESH = pl.DeviceIdType.MESH


def rcopy(src, dst, send, recv, device):
    return pltpu.make_async_remote_copy(
        src_ref=src, dst_ref=dst, send_sem=send, recv_sem=recv, device_id=device, device_id_type=MESH
    )


def places():
    sp, dp = lax.axis_index("sp"), lax.axis_index("dp")
    z, y = lax.div(sp, RING), lax.rem(sp, RING)
    x, c = lax.div(dp, 2), lax.rem(dp, 2)

    def at(dz=0, dy=0, dx=0, dc=0):
        nz, ny = lax.rem(z + dz, RING), lax.rem(y + dy, RING)
        nx, nc = lax.rem(x + dx, RING), lax.rem(c + dc, 2)
        return {"sp": nz * RING + ny, "dp": nx * 2 + nc}

    return z, y, x, c, at


def layer_kernel(
    x_hbm, gain_hbm, wq_hbm, wk_hbm, wv_hbm, wo_hbm, b_hbm, g_hbm,
    ho_ref, wo_ref,
    qv_ref, kk_ref, keys_t, qa, vv, tri, part, rsum, stage, h_s, h_r, b_ref, g_all,
    packs, w_all, xg, stage_qv, stage_k,
    wa_s, wa_r, wb_s, wb_r, wc_s, wc_r, xd_s, xd_r, xf_s, xf_r, a_s, a_r,
    oz_s, oz_r, oy_s, oy_r, ox_s, ox_r, of_s, of_r, oc_s, oc_r, local_sem,
    x_ref, gain_ref, wq_ref, wk_ref, wv_ref, wo_in,
):
    z, y, x, c, at = places()
    loads = [
        pltpu.make_async_copy(s, d, local_sem.at[i])
        for i, (s, d) in enumerate(
            (
                (wq_hbm, wq_ref), (wk_hbm, wk_ref), (wv_hbm, wv_ref), (wo_hbm, wo_in),
                (gain_hbm, gain_ref), (x_hbm, x_ref), (b_hbm, b_ref), (g_hbm, g_all),
            )
        )
    ]
    for load in loads:
        load.start()
    friends = [at(dz=i, dy=j) for i in range(RING) for j in range(RING) if i or j]
    friends += [at(dx=1), at(dx=2), at(dx=3), at(dc=1)]
    barrier = pltpu.get_barrier_semaphore()
    for f in friends:
        pl.semaphore_signal(barrier, inc=1, device_id=f, device_id_type=MESH)
    for load in loads:
        load.wait()
    rows = x_ref.shape[0]
    half = rows // 2
    depth = wq_ref.shape[1]
    qn, kn = wq_ref.shape[0], wk_ref.shape[0]
    split = depth // 2
    piece_rows = qn + 2 * kn
    own_piece = jnp.concatenate([wq_ref[...], wk_ref[...], wv_ref[...]], axis=0)
    packs[c, x, y, 0] = own_piece[:, 0:split]
    packs[c, x, y, 1] = own_piece[:, split:]

    def wo_cols(dx, cc):
        return pl.ds(pl.multiple_of((lax.rem(x + dx, RING) * 2 + cc) * depth, depth), depth)

    wo_ref[y, z, :, wo_cols(0, c)] = wo_in[...]
    pl.semaphore_wait(barrier, len(friends))

    def go(copy):
        copy.start()

    def settle(sem, count):
        ref = qv_ref.at[pl.ds(0, count)]
        pltpu.make_async_copy(ref, ref, sem).wait()

    def near(d, axis):
        return at(**{axis: 1 if d == 0 else 3})

    def back(d):
        return 3 if d == 0 else 1


    def oz(dz, n):
        return wo_ref.at[y, lax.rem(z + dz, RING), n, wo_cols(0, c)]

    every = slice(None)
    wo_rows = wo_in.shape[0] * wo_in.shape[1] // 128

    def oz_out(dz):
        return rcopy(wo_in, oz(0, every), oz_s, oz_r, at(dz=dz))

    sixth = rows // 6
    spans = (
        ((0, 3 * sixth), (3 * sixth, 2 * sixth), (5 * sixth, sixth)),
        ((3 * sixth, 3 * sixth), (sixth, 2 * sixth), (0, sixth)),
    )
    parts = tuple(tuple(pl.ds(*span) for span in side) for side in spans)

    def x_out(d, i):
        p = parts[d][i]
        return rcopy(x_ref.at[p], xg.at[d, p], xd_s, xd_r.at[d, i], near(d, "dz"))

    def x_in(d, i):
        p = parts[d][i]
        return rcopy(xg.at[d, p], xg.at[d, p], xd_s, xd_r.at[d, i], near(d, "dz"))

    cuts = ((0, 64), (64, 32))

    def far_z(d, i):
        a, n = cuts[i]
        part = pl.ds(a + (0 if d == 0 else half), n)
        return rcopy(xg.at[d, part], xg.at[2, part], xf_s, xf_r.at[i], near(d, "dz"))

    def piece(o):
        return lax.rem(y + RING - o, RING)

    def w_first(side, o, arrived):
        py = piece(o) if arrived and side == 0 else y
        px = lax.rem(x + RING - o, RING) if arrived and side == 1 else x
        p = packs.at[c, px, py, side]
        return rcopy(p, p, wa_s, wa_r.at[side, o - 1], at(dy=o) if side == 0 else at(dx=o))

    def w_second(side, came, o):
        p = packs.at[c, lax.rem(x + RING - (came if side else 0), RING), piece(0 if side else came), side]
        return rcopy(p, p, wb_s, wb_r.at[came if side else o], at(dy=o) if side else at(dx=o))

    def w_c(dx):
        slab = packs.at[c, lax.rem(x + dx, RING)]
        return rcopy(slab, slab, wc_s, wc_r, at(dc=1))

    def oy(d, arrived):
        s = wo_ref.at[lax.rem(y + back(d), RING) if arrived else y, :, :, wo_cols(0, c)]
        return rcopy(s, s, oy_s, oy_r.at[d], near(d, "dy"))

    def oy_far(d, dy):
        s = wo_ref.at[lax.rem(y + dy, RING), pl.ds(0 if d == 0 else 2, 2), :, wo_cols(0, c)]
        return rcopy(s, s, oy_s, oy_r.at[2], near(d, "dy"))

    def ox(o, d):
        s = wo_ref.at[piece(o), :, :, wo_cols(0, c)]
        return rcopy(s, s, ox_s, ox_r.at[1 if o == 2 else 0], near(d, "dx"))

    def ox_far(o, d, dx):
        s = wo_ref.at[piece(o), pl.ds(0 if d == 0 else 2, 2), :, wo_cols(dx, c)]
        return rcopy(s, s, of_s, of_r, near(d, "dx"))

    def oc(dx):
        s = wo_ref.at[:, :, :, wo_cols(dx, c)]
        return rcopy(s, s, oc_s, oc_r, at(dc=1))

    with jax.named_scope("issue"):
        for o in (2, 1, 3):
            for side in (0, 1):
                go(w_first(side, o, False))
        for o in (2, 1, 3):
            for side in (0, 1):
                go(w_second(side, 0, o))
        for dz in (2, 1, 3):
            go(oz_out(dz))
        for i in (0, 1, 2):
            for d in (0, 1):
                go(x_out(d, i))
    with jax.named_scope("wait_wfirst"):
        for came in (1, 3, 2):
            for side in (0, 1):
                w_first(side, came, True).wait_recv()
                for o in (2, 1, 3):
                    go(w_second(side, came, o))
    with jax.named_scope("wait_oz"):
        settle(oz_r, 3 * wo_rows)
        for d in (0, 1):
            go(oy(d, False))
    with jax.named_scope("wait_wsecond"):
        for d in (0, 1):
            go(ox(0, d))
        settle(wb_r.at[0], 3 * piece_rows)
        go(w_c(0))
        for px in (1, 3, 2):
            settle(wb_r.at[px], 7 * piece_rows)
            go(w_c(RING - px))
    def chunk(source, segments, stage_at):
        wide = source.astype(F32)
        normed = (
            wide * lax.rsqrt(jnp.mean(wide * wide, axis=-1, keepdims=True) + EPS) * gain_ref[...]
        ).astype(BF16)
        out = jnp.dot(normed, w_all[...], preferred_element_type=F32).astype(BF16)
        total = out.shape[0]
        v = out[:, 320:384]
        k = out[:, 256:320].reshape(total // 32, 2, 16, HEAD_DIM)
        for i in range(RING):
            stage_qv[i, pl.ds(stage_at, total)] = jnp.concatenate([out[:, i * 64 : i * 64 + 64], v], axis=1)
        stage_k[pl.ds(stage_at // 2, total // 2)] = jnp.concatenate([k[:, 0], k[:, 1]], axis=2).reshape(
            total // 2, 128
        )
        for dz, first, count in segments:
            here, here_k = pl.ds(stage_at, count), pl.ds(stage_at // 2, count // 2)
            nz = lax.rem(z + dz, RING)

            def spot(halved):
                start = (nz * RING + y) * rows + first
                if halved:
                    return pl.ds(pl.multiple_of(lax.div(start, 2), 16), count // 2)
                return pl.ds(pl.multiple_of(start, 32), count)

            for o in (2, 1, 3):
                ny = lax.rem(y + o, RING)
                go(rcopy(stage_qv.at[ny, here], qv_ref.at[spot(False)], a_s.at[dz], a_r.at[dz, o - 1], at(dy=o)))
                go(rcopy(stage_k.at[here_k], kk_ref.at[spot(True)], a_s.at[dz], a_r.at[dz, o - 1], at(dy=o)))
            qv_ref[spot(False)] = stage_qv[y, here]
            kk_ref[spot(True)] = stage_k[here_k]
            stage_at = stage_at + count

    ratio = BLOCK_Q // BLOCK_K
    me = z * RING + y

    def place(dz):
        return lax.rem(z + dz, RING)

    def block_rows(i, size):
        return pl.ds(pl.multiple_of(i * size, size), size)

    def prepare(dz):
        for o in range(RING - 1):
            settle(a_r.at[dz, o], rows + half)
        i = place(dz)
        at_rows = block_rows(i, BLOCK_Q)
        packed = kk_ref[block_rows(i, BLOCK_Q // 2), :].reshape(BLOCK_Q // 32, 16, 128)
        k = jnp.concatenate([packed[:, :, 0:64], packed[:, :, 64:128]], axis=1).reshape(BLOCK_Q, HEAD_DIM)
        kk = k.astype(F32) * (LOG2E / 8.0)
        hi_part = kk.astype(BF16)
        lo_part = (kk - hi_part.astype(F32)).astype(BF16)
        keys_t[0:128, at_rows] = jnp.concatenate([hi_part, lo_part], axis=1).T
        both = qv_ref[at_rows, :]
        qa[at_rows, 0:128] = jnp.concatenate([both[:, 0:64], both[:, 0:64]], axis=1)
        vv[at_rows, :] = both[:, 64:128]

    def block(q, j, carry, diagonal=False):
        count = q.shape[0]
        cols = block_rows(j, BLOCK_K)
        l2 = jnp.dot(q, keys_t[:, cols], preferred_element_type=F32)
        if diagonal:
            t = lax.broadcasted_iota(jnp.int32, (BLOCK_K, BLOCK_K), 0)
            u = lax.broadcasted_iota(jnp.int32, (BLOCK_K, BLOCK_K), 1)
            first = jnp.where(u < t, l2[0:BLOCK_K], -1e30)
            l2 = first if count == BLOCK_K else jnp.concatenate([first, l2[BLOCK_K:]], axis=0)
        soft = jnp.maximum(l2, jnp.log2(1.0 + jnp.exp2(jnp.minimum(l2, 100.0))))
        drop = soft.astype(BF16)
        after = jnp.dot(drop, tri[...], preferred_element_type=F32)
        e = (l2 - soft) - after
        if carry is not None:
            e = e - jnp.concatenate([carry] * (BLOCK_K // 128), axis=1)
        pv = jnp.dot(jnp.exp2(e).astype(BF16), vv[cols, :], preferred_element_type=F32)
        whole = jnp.broadcast_to(after[:, 0:1] + soft[:, 0:1], (count, 128))
        return pv, whole if carry is None else carry + whole

    def diagonal(dz):
        i = place(dz)
        q = qa[block_rows(i, BLOCK_Q), 0:144]
        carry, total = None, None
        for d in reversed(range(ratio)):
            if carry is not None:
                carry = jnp.concatenate([jnp.zeros((BLOCK_K, 128), F32), carry], axis=0)
            pv, carry = block(q[d * BLOCK_K :], i * ratio + d, carry, True)
            if total is None:
                total = pv
            else:
                total = jnp.concatenate([pv[:BLOCK_K], pv[BLOCK_K:] + total], axis=0)
        part[i, i] = total
        rsum[i, i] = carry

    def pair(da, db):
        a, b = place(da), place(db)
        i, j = jnp.maximum(a, b), jnp.minimum(a, b)
        q = qa[block_rows(i, BLOCK_Q), 0:144]
        carry, total = None, None
        for d in reversed(range(ratio)):
            pv, carry = block(q, j * ratio + d, carry)
            total = pv if total is None else total + pv
        part[i, j] = total
        rsum[i, j] = carry

    def finish(i):
        a, later = part[i, i], rsum[i, i]
        for n in range(1, RING):
            j = jnp.maximum(i - n, 0)
            there = jnp.where(i >= n, 1.0, 0.0).astype(F32)
            a = a + (jnp.exp2(-later) * there)[:, 0:HEAD_DIM] * part[i, j]
            later = later + rsum[i, j]
        pair_gain = g_all[0:1, block_rows(lax.div(me, 2), 128)]
        own_gain = jnp.where(lax.rem(me, 2) == 0, pair_gain[:, 0:64], pair_gain[:, 64:128])
        scaled = a * lax.rsqrt(jnp.mean(a * a, axis=-1, keepdims=True) + EPS)
        head = (scaled * own_gain).astype(BF16)
        for yy in range(RING):
            mine = head[yy * rows : (yy + 1) * rows]
            stage[i * RING + yy] = jnp.concatenate([mine[:half], mine[half:]], axis=1)
        for yy in range(RING):
            dest = i * RING + yy

            @pl.when(dest != me)
            def _():
                rcopy(
                    stage.at[dest], ho_ref.at[y * RING + z], h_s, h_r,
                    {"sp": dest, "dp": lax.axis_index("dp")},
                ).start()

            @pl.when(dest == me)
            def _():
                ho_ref[y * RING + z] = stage[dest]

    with jax.named_scope("constants"):
        r = lax.broadcasted_iota(jnp.int32, (BLOCK_K, BLOCK_K), 0)
        u = lax.broadcasted_iota(jnp.int32, (BLOCK_K, BLOCK_K), 1)
        tri[...] = jnp.where(r > u, 1.0, 0.0).astype(BF16)
        length = qv_ref.shape[0]
        lane = lax.broadcasted_iota(jnp.int32, (length, 128), 1)
        qa[:, 128:256] = jnp.where(lane < 3, 1.0, 0.0).astype(BF16)
        bb = b_ref[...] * LOG2E
        bh = bb.astype(BF16)
        r1 = bb - bh.astype(F32)
        bm = r1.astype(BF16)
        bl = (r1 - bm.astype(F32)).astype(BF16)
        keys_t[128:144, :] = jnp.concatenate([bh, bm, bl, jnp.zeros((13, length), BF16)], axis=0)
    with jax.named_scope("wait_wc"):
        settle(wc_r, RING * RING * 2 * piece_rows)
    with jax.named_scope("assemble"):
        for n in range(2 * RING):
            for side in (0, 1):
                p = [packs[n % 2, n // 2, i, side] for i in range(RING)]
                first = n * depth + side * split
                w_all[first : first + split, :] = jnp.concatenate(
                    [t[0:qn] for t in p] + [t[qn : qn + kn] for t in p] + [t[qn + kn :] for t in p], axis=0
                ).T
    with jax.named_scope("chunk0"):
        chunk(x_ref[...], ((0, 0, rows),), 0)
    with jax.named_scope("wait_oy"):
        for d in (0, 1):
            oy(d, True).wait_recv()
            go(oy_far(d, back(d)))
        for o in (1, 3):
            for d in (0, 1):
                go(ox(o, d))
    with jax.named_scope("wait_x0"):
        for d in (0, 1):
            x_in(d, 0).wait_recv()
            for i in (0, 1):
                go(far_z(d, i))
    def near_chunk(i, place):
        with jax.named_scope("chunk_near%d" % i):
            chunk(
                jnp.concatenate([xg[0, parts[0][i]], xg[1, parts[1][i]]], axis=0),
                ((3, *spans[0][i]), (1, *spans[1][i])),
                place,
            )

    near_chunk(0, rows)
    with jax.named_scope("wait_x1"):
        x_in(0, 1).wait_recv()
        x_in(1, 1).wait_recv()
    near_chunk(1, rows + 6 * sixth)
    with jax.named_scope("prepare_own"):
        prepare(0)
    with jax.named_scope("diagonal_own"):
        diagonal(0)
    with jax.named_scope("wait_x2"):
        x_in(0, 2).wait_recv()
        x_in(1, 2).wait_recv()
    near_chunk(2, rows + 10 * sixth)
    with jax.named_scope("wait_oyfar"):
        settle(oy_r.at[2], RING * wo_rows)
        for d in (0, 1):
            go(ox(2, d))
        go(oc(0))
    def far_chunk(i):
        a, count = cuts[i]
        with jax.named_scope("wait_far%d" % i):
            settle(xf_r.at[i], 2 * count * x_ref.shape[1] // 128)
        with jax.named_scope("chunk_far%d" % i):
            chunk(
                jnp.concatenate([xg[2, pl.ds(a, count)], xg[2, pl.ds(a + half, count)]], axis=0),
                ((2, a, count), (2, a + half, count)),
                3 * rows + 2 * i * cuts[0][1],
            )

    with jax.named_scope("wait_ox"):
        settle(ox_r.at[0], 6 * RING * wo_rows)
        for o in (0, 1, 3):
            for d in (0, 1):
                go(ox_far(o, d, back(d)))

    with jax.named_scope("prepare_near"):
        prepare(3)
        prepare(1)
    far_chunk(0)
    far_chunk(1)
    with jax.named_scope("wait_ox2"):
        settle(ox_r.at[1], 2 * RING * wo_rows)
        for d in (0, 1):
            go(ox_far(2, d, back(d)))
        go(oc(3))
        go(oc(1))
    with jax.named_scope("blocks_near"):
        diagonal(3)
        diagonal(1)
        pair(0, 3)
        pair(0, 1)
        pair(3, 1)

    far = place(2)
    with jax.named_scope("wait_oxfar"):
        settle(of_r, RING * RING * wo_rows)
        go(oc(2))
    with jax.named_scope("finish_early"):

        @pl.loop(0, jnp.where(far < RING - 1, far, 1))
        def _(i):
            finish(i)

    with jax.named_scope("prepare_far"):
        prepare(2)
    with jax.named_scope("diagonal_far"):
        diagonal(2)
    with jax.named_scope("blocks_far"):

        @pl.loop(0, far)
        def _(i):
            pair(2, i - z + RING)

        finish(far)

        @pl.loop(0, RING - 1)
        def _(n):
            dz = jnp.where(n == 0, 1, jnp.where(n == 1, 0, 3))
            i = place(dz)

            @pl.when(i > far)
            def _():
                pair(2, dz)
                finish(i)

        @pl.loop(1, jnp.where(far < RING - 1, 1, far))
        def _(i):
            finish(i)

    whole_w = wo_ref.at[:, :, :, pl.ds(0, RING * depth)]
    ho_rows = (RING * RING - 1) * half
    with jax.named_scope("wait_ho"):
        settle(h_r, ho_rows)
    with jax.named_scope("wait_oc"):
        pltpu.make_async_copy(whole_w, whole_w, oc_r).wait()
    with jax.named_scope("wait_send"):
        settle(h_s, ho_rows)
        pltpu.make_async_copy(whole_w, whole_w, oc_s).wait()
        both_x = xg.at[pl.ds(0, 2)]
        pltpu.make_async_copy(both_x, both_x, xd_s).wait()
        one_x = xg.at[0]
        pltpu.make_async_copy(one_x, one_x, xf_s).wait()
        settle(wa_s, 6 * piece_rows)
        settle(wb_s, 24 * piece_rows)
        settle(wc_s, RING * RING * 2 * piece_rows)
        settle(oz_s, 3 * wo_rows)
        settle(oy_s, 3 * RING * wo_rows)
        x_w = wo_ref.at[:, :, :, pl.ds(0, 2 * depth)]
        pltpu.make_async_copy(x_w, x_w, ox_s).wait()
        settle(of_s, RING * RING * wo_rows)
        for dz in range(RING):
            settle(a_s.at[dz], 3 * (rows + half))


BLOCK_Q = 768
BLOCK_K = 256


def layer(x, gain, wq, wk, wv, wo, bias, out_gain):
    rows, width = x.shape
    length = rows * RING * RING
    depth = wq.shape[1]
    dma = pltpu.SemaphoreType.DMA
    vmem = pl.BlockSpec(memory_space=pltpu.VMEM)
    operands = [
        pltpu.with_memory_space_constraint(t, pltpu.HBM) for t in (x, gain, wq, wk, wv, wo, bias, out_gain)
    ]
    return pl.pallas_call(
        layer_kernel,
        name="layer",
        out_shape=(
            jax.ShapeDtypeStruct((RING * RING, rows // 2, 2 * HEAD_DIM), BF16),
            jax.ShapeDtypeStruct((RING, RING, wo.shape[0], wo.shape[1] * 2 * RING), BF16),
        ),
        in_specs=[pl.BlockSpec(memory_space=pltpu.HBM)] * 8,
        out_specs=(vmem, vmem),
        scratch_shapes=[
            pltpu.VMEM((length, 128), BF16),
            pltpu.VMEM((length // 2, 128), BF16),
            pltpu.VMEM((144, length), BF16),
            pltpu.VMEM((length, 256), BF16),
            pltpu.VMEM((length, HEAD_DIM), BF16),
            pltpu.VMEM((BLOCK_K, BLOCK_K), BF16),
            pltpu.VMEM((RING, RING, BLOCK_Q, HEAD_DIM), F32),
            pltpu.VMEM((RING, RING, BLOCK_Q, 128), F32),
            pltpu.VMEM((RING * RING, rows // 2, 2 * HEAD_DIM), BF16),
            dma(()), dma(()),
            pltpu.VMEM(bias.shape, F32), pltpu.VMEM(out_gain.shape, F32),
            pltpu.VMEM((2, RING, RING, 2, 96, depth // 2), BF16),
            pltpu.VMEM((width, 384), BF16),
            pltpu.VMEM((3, rows, width), BF16),
            pltpu.VMEM((RING, RING * rows, 128), BF16),
            pltpu.VMEM((RING * rows // 2, 128), BF16),
            dma(()), dma((2, 3)), dma(()), dma((4,)), dma(()), dma(()),
            dma(()), dma((2, 3)), dma(()), dma((2,)),
            dma((4,)), dma((4, 3)),
            dma(()), dma(()), dma(()), dma((3,)), dma(()), dma((2,)),
            dma(()), dma(()), dma(()), dma(()), dma((8,)),
            pltpu.VMEM(x.shape, BF16), pltpu.VMEM(gain.shape, F32), pltpu.VMEM(wq.shape, BF16),
            pltpu.VMEM(wk.shape, BF16), pltpu.VMEM(wv.shape, BF16), pltpu.VMEM(wo.shape, BF16),
        ],
        compiler_params=pltpu.CompilerParams(
            collective_id=0, has_side_effects=True, vmem_limit_bytes=44 << 20
        ),
    )(*operands)


def mix_kernel(ho_ref, wo_ref, o_hbm, lhs, o_ref, sems):
    heads, half, _ = ho_ref.shape
    for n in range(0, heads, 2):
        a, b = ho_ref[n], ho_ref[n + 1]
        cols = pl.ds(n * HEAD_DIM, 2 * HEAD_DIM)
        lhs[0:half, cols] = jnp.concatenate([a[:, 0:64], b[:, 0:64]], axis=1)
        lhs[half : 2 * half, cols] = jnp.concatenate([a[:, 64:128], b[:, 64:128]], axis=1)
    width = o_ref.shape[1]
    out = []
    for n in range(width // MIX):
        cols = slice(n * MIX, (n + 1) * MIX)
        o_ref[:, cols] = jnp.dot(lhs[...], wo_ref[:, cols], preferred_element_type=F32).astype(BF16)
        copy = pltpu.make_async_copy(o_ref.at[:, cols], o_hbm.at[:, cols], sems.at[n])
        copy.start()
        out.append(copy)
    for copy in out:
        copy.wait()


MIX = 512


def mix(ho, wo):
    heads, half, _ = ho.shape
    vmem = pl.BlockSpec(memory_space=pltpu.VMEM)
    return pl.pallas_call(
        mix_kernel,
        name="mix",
        out_shape=jax.ShapeDtypeStruct((2 * half, wo.shape[1]), BF16),
        in_specs=[vmem] * 2,
        out_specs=pl.BlockSpec(memory_space=pl.ANY),
        scratch_shapes=[
            pltpu.VMEM((2 * half, heads * HEAD_DIM), BF16),
            pltpu.VMEM((2 * half, wo.shape[1]), BF16),
            pltpu.SemaphoreType.DMA((wo.shape[1] // MIX,)),
        ],
        compiler_params=pltpu.CompilerParams(vmem_limit_bytes=16 << 20),
    )(ho, wo)


def body(inputs, in_gain, w_query, w_key, w_value, key_bias, out_gain, w_out):
    ho, wo = layer(
        inputs[0], in_gain[None], w_query.T, w_key.T, w_value.T, w_out, key_bias[0].T, out_gain[None]
    )
    return mix(ho, wo.reshape(-1, wo.shape[-1]))[None]


def solution(mesh):
    placed = (
        P("dp", "sp", None), P(), P("dp", "sp"), P("dp", "sp"), P("dp", "sp"),
        P("dp", None, "sp"), P(), P("sp", "dp"),
    )
    return jax.shard_map(body, mesh=mesh, in_specs=placed, out_specs=P("dp", "sp", None), check_vma=False)
```

```python
import functools

import jax
import jax.numpy as jnp
from jax import lax
from jax.experimental import pallas as pl
from jax.experimental.pallas import tpu as pltpu
from jax.sharding import PartitionSpec as P

HEAD_DIM = 64
RING = 4
EPS = 1e-06
LOG2E = 1.4426950408889634
F32 = jnp.float32
BF16 = jnp.bfloat16
MESH = pl.DeviceIdType.MESH


def rcopy(src, dst, send, recv, device):
    return pltpu.make_async_remote_copy(
        src_ref=src, dst_ref=dst, send_sem=send, recv_sem=recv, device_id=device, device_id_type=MESH
    )


def places():
    sp, dp = lax.axis_index("sp"), lax.axis_index("dp")
    z, y = lax.div(sp, RING), lax.rem(sp, RING)
    x, c = lax.div(dp, 2), lax.rem(dp, 2)

    def at(dz=0, dy=0, dx=0, dc=0):
        nz, ny = lax.rem(z + dz, RING), lax.rem(y + dy, RING)
        nx, nc = lax.rem(x + dx, RING), lax.rem(c + dc, 2)
        return {"sp": nz * RING + ny, "dp": nx * 2 + nc}

    return z, y, x, c, at


def layer_kernel(
    x_hbm, gain_hbm, wq_hbm, wk_hbm, wv_hbm, wo_hbm, b_hbm, g_hbm,
    ho_ref, wo_ref,
    qv_ref, kk_ref, keys_t, qa, vv, tri, part, rsum, stage, h_s, h_r, b_ref, g_all,
    packs, w_all, xg, stage_qv, stage_k,
    wa_s, wa_r, wb_s, wb_r, wc_s, wc_r, xd_s, xd_r, xf_s, xf_r, a_s, a_r,
    oz_s, oz_r, oy_s, oy_r, ox_s, ox_r, of_s, of_r, oc_s, oc_r, local_sem,
    x_ref, gain_ref, wq_ref, wk_ref, wv_ref, wo_in,
):
    z, y, x, c, at = places()
    loads = [
        pltpu.make_async_copy(s, d, local_sem.at[i])
        for i, (s, d) in enumerate(
            (
                (wq_hbm, wq_ref), (wk_hbm, wk_ref), (wv_hbm, wv_ref), (wo_hbm, wo_in),
                (gain_hbm, gain_ref), (x_hbm, x_ref), (b_hbm, b_ref), (g_hbm, g_all),
            )
        )
    ]
    for load in loads:
        load.start()
    friends = [at(dz=i, dy=j) for i in range(RING) for j in range(RING) if i or j]
    friends += [at(dx=1), at(dx=2), at(dx=3), at(dc=1)]
    barrier = pltpu.get_barrier_semaphore()
    for f in friends:
        pl.semaphore_signal(barrier, inc=1, device_id=f, device_id_type=MESH)
    for load in loads:
        load.wait()
    rows = x_ref.shape[0]
    half = rows // 2
    depth = wq_ref.shape[1]
    qn, kn = wq_ref.shape[0], wk_ref.shape[0]
    split = depth // 2
    piece_rows = qn + 2 * kn
    own_piece = jnp.concatenate([wq_ref[...], wk_ref[...], wv_ref[...]], axis=0)
    packs[c, x, y, 0] = own_piece[:, 0:split]
    packs[c, x, y, 1] = own_piece[:, split:]

    def wo_cols(dx, cc):
        return pl.ds(pl.multiple_of((lax.rem(x + dx, RING) * 2 + cc) * depth, depth), depth)

    wo_ref[y, z, :, wo_cols(0, c)] = wo_in[...]
    pl.semaphore_wait(barrier, len(friends))

    def go(copy):
        copy.start()

    def settle(sem, count):
        ref = qv_ref.at[pl.ds(0, count)]
        pltpu.make_async_copy(ref, ref, sem).wait()

    def near(d, axis):
        return at(**{axis: 1 if d == 0 else 3})

    def back(d):
        return 3 if d == 0 else 1


    def oz(dz, n):
        return wo_ref.at[y, lax.rem(z + dz, RING), n, wo_cols(0, c)]

    every = slice(None)
    wo_rows = wo_in.shape[0] * wo_in.shape[1] // 128

    def oz_out(dz):
        return rcopy(wo_in, oz(0, every), oz_s, oz_r, at(dz=dz))

    sixth = rows // 6
    spans = (
        ((0, 3 * sixth), (3 * sixth, 2 * sixth), (5 * sixth, sixth)),
        ((3 * sixth, 3 * sixth), (sixth, 2 * sixth), (0, sixth)),
    )
    parts = tuple(tuple(pl.ds(*span) for span in side) for side in spans)

    def x_out(d, i):
        p = parts[d][i]
        return rcopy(x_ref.at[p], xg.at[d, p], xd_s, xd_r.at[d, i], near(d, "dz"))

    def x_in(d, i):
        p = parts[d][i]
        return rcopy(xg.at[d, p], xg.at[d, p], xd_s, xd_r.at[d, i], near(d, "dz"))

    cuts = ((0, 64), (64, 32))

    def far_z(d, i):
        a, n = cuts[i]
        part = pl.ds(a + (0 if d == 0 else half), n)
        return rcopy(xg.at[d, part], xg.at[2, part], xf_s, xf_r.at[i], near(d, "dz"))

    def piece(o):
        return lax.rem(y + RING - o, RING)

    def w_first(side, o, arrived):
        py = piece(o) if arrived and side == 0 else y
        px = lax.rem(x + RING - o, RING) if arrived and side == 1 else x
        p = packs.at[c, px, py, side]
        return rcopy(p, p, wa_s, wa_r.at[side, o - 1], at(dy=o) if side == 0 else at(dx=o))

    def w_second(side, came, o):
        p = packs.at[c, lax.rem(x + RING - (came if side else 0), RING), piece(0 if side else came), side]
        return rcopy(p, p, wb_s, wb_r.at[came if side else o], at(dy=o) if side else at(dx=o))

    def w_c(dx):
        slab = packs.at[c, lax.rem(x + dx, RING)]
        return rcopy(slab, slab, wc_s, wc_r, at(dc=1))

    def oy(d, arrived):
        s = wo_ref.at[lax.rem(y + back(d), RING) if arrived else y, :, :, wo_cols(0, c)]
        return rcopy(s, s, oy_s, oy_r.at[d], near(d, "dy"))

    def oy_far(d, dy):
        s = wo_ref.at[lax.rem(y + dy, RING), pl.ds(0 if d == 0 else 2, 2), :, wo_cols(0, c)]
        return rcopy(s, s, oy_s, oy_r.at[2], near(d, "dy"))

    def ox(o, d):
        s = wo_ref.at[piece(o), :, :, wo_cols(0, c)]
        return rcopy(s, s, ox_s, ox_r.at[1 if o == 2 else 0], near(d, "dx"))

    def ox_far(o, d, dx):
        s = wo_ref.at[piece(o), pl.ds(0 if d == 0 else 2, 2), :, wo_cols(dx, c)]
        return rcopy(s, s, of_s, of_r, near(d, "dx"))

    def oc(dx):
        s = wo_ref.at[:, :, :, wo_cols(dx, c)]
        return rcopy(s, s, oc_s, oc_r, at(dc=1))

    with jax.named_scope("issue"):
        for o in (2, 1, 3):
            for side in (0, 1):
                go(w_first(side, o, False))
        for o in (2, 1, 3):
            for side in (0, 1):
                go(w_second(side, 0, o))
        for dz in (2, 1, 3):
            go(oz_out(dz))
        for i in (0, 1, 2):
            for d in (0, 1):
                go(x_out(d, i))
    with jax.named_scope("wait_wfirst"):
        for came in (1, 3, 2):
            for side in (0, 1):
                w_first(side, came, True).wait_recv()
                for o in (2, 1, 3):
                    go(w_second(side, came, o))
    with jax.named_scope("wait_oz"):
        settle(oz_r, 3 * wo_rows)
        for d in (0, 1):
            go(oy(d, False))
    with jax.named_scope("wait_wsecond"):
        for d in (0, 1):
            go(ox(0, d))
        settle(wb_r.at[0], 3 * piece_rows)
        go(w_c(0))
        for px in (1, 3, 2):
            settle(wb_r.at[px], 7 * piece_rows)
            go(w_c(RING - px))
    def chunk(source, segments, stage_at):
        wide = source.astype(F32)
        normed = (
            wide * lax.rsqrt(jnp.mean(wide * wide, axis=-1, keepdims=True) + EPS) * gain_ref[...]
        ).astype(BF16)
        out = jnp.dot(normed, w_all[...], preferred_element_type=F32).astype(BF16)
        total = out.shape[0]
        v = out[:, 320:384]
        k = out[:, 256:320].reshape(total // 32, 2, 16, HEAD_DIM)
        for i in range(RING):
            stage_qv[i, pl.ds(stage_at, total)] = jnp.concatenate([out[:, i * 64 : i * 64 + 64], v], axis=1)
        stage_k[pl.ds(stage_at // 2, total // 2)] = jnp.concatenate([k[:, 0], k[:, 1]], axis=2).reshape(
            total // 2, 128
        )
        for dz, first, count in segments:
            here, here_k = pl.ds(stage_at, count), pl.ds(stage_at // 2, count // 2)
            nz = lax.rem(z + dz, RING)

            def spot(halved):
                start = (nz * RING + y) * rows + first
                if halved:
                    return pl.ds(pl.multiple_of(lax.div(start, 2), 16), count // 2)
                return pl.ds(pl.multiple_of(start, 32), count)

            for o in (2, 1, 3):
                ny = lax.rem(y + o, RING)
                go(rcopy(stage_qv.at[ny, here], qv_ref.at[spot(False)], a_s.at[dz], a_r.at[dz, o - 1], at(dy=o)))
                go(rcopy(stage_k.at[here_k], kk_ref.at[spot(True)], a_s.at[dz], a_r.at[dz, o - 1], at(dy=o)))
            qv_ref[spot(False)] = stage_qv[y, here]
            kk_ref[spot(True)] = stage_k[here_k]
            stage_at = stage_at + count

    ratio = BLOCK_Q // BLOCK_K
    me = z * RING + y

    def place(dz):
        return lax.rem(z + dz, RING)

    def block_rows(i, size):
        return pl.ds(pl.multiple_of(i * size, size), size)

    def prepare(dz):
        for o in range(RING - 1):
            settle(a_r.at[dz, o], rows + half)
        i = place(dz)
        at_rows = block_rows(i, BLOCK_Q)
        packed = kk_ref[block_rows(i, BLOCK_Q // 2), :].reshape(BLOCK_Q // 32, 16, 128)
        k = jnp.concatenate([packed[:, :, 0:64], packed[:, :, 64:128]], axis=1).reshape(BLOCK_Q, HEAD_DIM)
        kk = k.astype(F32) * (LOG2E / 8.0)
        hi_part = kk.astype(BF16)
        lo_part = (kk - hi_part.astype(F32)).astype(BF16)
        keys_t[0:128, at_rows] = jnp.concatenate([hi_part, lo_part], axis=1).T
        both = qv_ref[at_rows, :]
        qa[at_rows, 0:128] = jnp.concatenate([both[:, 0:64], both[:, 0:64]], axis=1)
        vv[at_rows, :] = both[:, 64:128]

    def block(q, j, carry, diagonal=False):
        count = q.shape[0]
        cols = block_rows(j, BLOCK_K)
        l2 = jnp.dot(q, keys_t[:, cols], preferred_element_type=F32)
        if diagonal:
            t = lax.broadcasted_iota(jnp.int32, (BLOCK_K, BLOCK_K), 0)
            u = lax.broadcasted_iota(jnp.int32, (BLOCK_K, BLOCK_K), 1)
            first = jnp.where(u < t, l2[0:BLOCK_K], -1e30)
            l2 = first if count == BLOCK_K else jnp.concatenate([first, l2[BLOCK_K:]], axis=0)
        soft = jnp.maximum(l2, jnp.log2(1.0 + jnp.exp2(jnp.minimum(l2, 100.0))))
        drop = soft.astype(BF16)
        after = jnp.dot(drop, tri[...], preferred_element_type=F32)
        e = (l2 - soft) - after
        if carry is not None:
            e = e - jnp.concatenate([carry] * (BLOCK_K // 128), axis=1)
        pv = jnp.dot(jnp.exp2(e).astype(BF16), vv[cols, :], preferred_element_type=F32)
        whole = jnp.broadcast_to(after[:, 0:1] + soft[:, 0:1], (count, 128))
        return pv, whole if carry is None else carry + whole

    def diagonal(dz):
        i = place(dz)
        q = qa[block_rows(i, BLOCK_Q), 0:144]
        carry, total = None, None
        for d in reversed(range(ratio)):
            if carry is not None:
                carry = jnp.concatenate([jnp.zeros((BLOCK_K, 128), F32), carry], axis=0)
            pv, carry = block(q[d * BLOCK_K :], i * ratio + d, carry, True)
            if total is None:
                total = pv
            else:
                total = jnp.concatenate([pv[:BLOCK_K], pv[BLOCK_K:] + total], axis=0)
        part[i, i] = total
        rsum[i, i] = carry

    def pair(da, db):
        a, b = place(da), place(db)
        i, j = jnp.maximum(a, b), jnp.minimum(a, b)
        q = qa[block_rows(i, BLOCK_Q), 0:144]
        carry, total = None, None
        for d in reversed(range(ratio)):
            pv, carry = block(q, j * ratio + d, carry)
            total = pv if total is None else total + pv
        part[i, j] = total
        rsum[i, j] = carry

    def finish(i):
        a, later = part[i, i], rsum[i, i]
        for n in range(1, RING):
            j = jnp.maximum(i - n, 0)
            there = jnp.where(i >= n, 1.0, 0.0).astype(F32)
            a = a + (jnp.exp2(-later) * there)[:, 0:HEAD_DIM] * part[i, j]
            later = later + rsum[i, j]
        pair_gain = g_all[0:1, block_rows(lax.div(me, 2), 128)]
        own_gain = jnp.where(lax.rem(me, 2) == 0, pair_gain[:, 0:64], pair_gain[:, 64:128])
        scaled = a * lax.rsqrt(jnp.mean(a * a, axis=-1, keepdims=True) + EPS)
        head = (scaled * own_gain).astype(BF16)
        for yy in range(RING):
            mine = head[yy * rows : (yy + 1) * rows]
            stage[i * RING + yy] = jnp.concatenate([mine[:half], mine[half:]], axis=1)
        for yy in range(RING):
            dest = i * RING + yy

            @pl.when(dest != me)
            def _():
                rcopy(
                    stage.at[dest], ho_ref.at[y * RING + z], h_s, h_r,
                    {"sp": dest, "dp": lax.axis_index("dp")},
                ).start()

            @pl.when(dest == me)
            def _():
                ho_ref[y * RING + z] = stage[dest]

    with jax.named_scope("constants"):
        r = lax.broadcasted_iota(jnp.int32, (BLOCK_K, BLOCK_K), 0)
        u = lax.broadcasted_iota(jnp.int32, (BLOCK_K, BLOCK_K), 1)
        tri[...] = jnp.where(r > u, 1.0, 0.0).astype(BF16)
        length = qv_ref.shape[0]
        lane = lax.broadcasted_iota(jnp.int32, (length, 128), 1)
        qa[:, 128:256] = jnp.where(lane < 3, 1.0, 0.0).astype(BF16)
        bb = b_ref[...] * LOG2E
        bh = bb.astype(BF16)
        r1 = bb - bh.astype(F32)
        bm = r1.astype(BF16)
        bl = (r1 - bm.astype(F32)).astype(BF16)
        keys_t[128:144, :] = jnp.concatenate([bh, bm, bl, jnp.zeros((13, length), BF16)], axis=0)
    with jax.named_scope("wait_wc"):
        settle(wc_r, RING * RING * 2 * piece_rows)
    with jax.named_scope("assemble"):
        for n in range(2 * RING):
            for side in (0, 1):
                p = [packs[n % 2, n // 2, i, side] for i in range(RING)]
                first = n * depth + side * split
                w_all[first : first + split, :] = jnp.concatenate(
                    [t[0:qn] for t in p] + [t[qn : qn + kn] for t in p] + [t[qn + kn :] for t in p], axis=0
                ).T
    with jax.named_scope("chunk0"):
        chunk(x_ref[...], ((0, 0, rows),), 0)
    with jax.named_scope("wait_oy"):
        for d in (0, 1):
            oy(d, True).wait_recv()
            go(oy_far(d, back(d)))
        for o in (1, 3):
            for d in (0, 1):
                go(ox(o, d))
    with jax.named_scope("wait_x0"):
        for d in (0, 1):
            x_in(d, 0).wait_recv()
            for i in (0, 1):
                go(far_z(d, i))
    def near_chunk(i, place):
        with jax.named_scope("chunk_near%d" % i):
            chunk(
                jnp.concatenate([xg[0, parts[0][i]], xg[1, parts[1][i]]], axis=0),
                ((3, *spans[0][i]), (1, *spans[1][i])),
                place,
            )

    near_chunk(0, rows)
    with jax.named_scope("wait_x1"):
        x_in(0, 1).wait_recv()
        x_in(1, 1).wait_recv()
    near_chunk(1, rows + 6 * sixth)
    with jax.named_scope("prepare_own"):
        prepare(0)
    with jax.named_scope("diagonal_own"):
        diagonal(0)
    with jax.named_scope("wait_x2"):
        x_in(0, 2).wait_recv()
        x_in(1, 2).wait_recv()
    near_chunk(2, rows + 10 * sixth)
    with jax.named_scope("wait_oyfar"):
        settle(oy_r.at[2], RING * wo_rows)
        for d in (0, 1):
            go(ox(2, d))
        go(oc(0))
    def far_chunk(i):
        a, count = cuts[i]
        with jax.named_scope("wait_far%d" % i):
            settle(xf_r.at[i], 2 * count * x_ref.shape[1] // 128)
        with jax.named_scope("chunk_far%d" % i):
            chunk(
                jnp.concatenate([xg[2, pl.ds(a, count)], xg[2, pl.ds(a + half, count)]], axis=0),
                ((2, a, count), (2, a + half, count)),
                3 * rows + 2 * i * cuts[0][1],
            )

    with jax.named_scope("wait_ox"):
        settle(ox_r.at[0], 6 * RING * wo_rows)
        for o in (0, 1, 3):
            for d in (0, 1):
                go(ox_far(o, d, back(d)))

    with jax.named_scope("prepare_near"):
        prepare(3)
        prepare(1)
    far_chunk(0)
    with jax.named_scope("diagonal_near"):
        diagonal(3)
        diagonal(1)
    far_chunk(1)
    with jax.named_scope("wait_ox2"):
        settle(ox_r.at[1], 2 * RING * wo_rows)
        for d in (0, 1):
            go(ox_far(2, d, back(d)))
        go(oc(3))
        go(oc(1))
    with jax.named_scope("blocks_near"):
        pair(0, 3)
        pair(0, 1)
        pair(3, 1)

    far = place(2)
    with jax.named_scope("finish_early"):

        @pl.loop(0, jnp.where(far < RING - 1, far, 1))
        def _(i):
            finish(i)

    with jax.named_scope("prepare_far"):
        prepare(2)
    with jax.named_scope("diagonal_far"):
        diagonal(2)
    with jax.named_scope("wait_oxfar"):
        settle(of_r, RING * RING * wo_rows)
        go(oc(2))
    with jax.named_scope("blocks_far"):

        @pl.loop(0, far)
        def _(i):
            pair(2, i - z + RING)

        finish(far)

        @pl.loop(0, RING - 1)
        def _(n):
            dz = jnp.where(n == 0, 1, jnp.where(n == 1, 0, 3))
            i = place(dz)

            @pl.when(i > far)
            def _():
                pair(2, dz)
                finish(i)

        @pl.loop(1, jnp.where(far < RING - 1, 1, far))
        def _(i):
            finish(i)

    whole_w = wo_ref.at[:, :, :, pl.ds(0, RING * depth)]
    ho_rows = (RING * RING - 1) * half
    with jax.named_scope("wait_ho"):
        settle(h_r, ho_rows)
    with jax.named_scope("wait_oc"):
        pltpu.make_async_copy(whole_w, whole_w, oc_r).wait()
    with jax.named_scope("wait_send"):
        settle(h_s, ho_rows)
        pltpu.make_async_copy(whole_w, whole_w, oc_s).wait()
        both_x = xg.at[pl.ds(0, 2)]
        pltpu.make_async_copy(both_x, both_x, xd_s).wait()
        one_x = xg.at[0]
        pltpu.make_async_copy(one_x, one_x, xf_s).wait()
        settle(wa_s, 6 * piece_rows)
        settle(wb_s, 24 * piece_rows)
        settle(wc_s, RING * RING * 2 * piece_rows)
        settle(oz_s, 3 * wo_rows)
        settle(oy_s, 3 * RING * wo_rows)
        x_w = wo_ref.at[:, :, :, pl.ds(0, 2 * depth)]
        pltpu.make_async_copy(x_w, x_w, ox_s).wait()
        settle(of_s, RING * RING * wo_rows)
        for dz in range(RING):
            settle(a_s.at[dz], 3 * (rows + half))


BLOCK_Q = 768
BLOCK_K = 256


def layer(x, gain, wq, wk, wv, wo, bias, out_gain):
    rows, width = x.shape
    length = rows * RING * RING
    depth = wq.shape[1]
    dma = pltpu.SemaphoreType.DMA
    vmem = pl.BlockSpec(memory_space=pltpu.VMEM)
    operands = [
        pltpu.with_memory_space_constraint(t, pltpu.HBM) for t in (x, gain, wq, wk, wv, wo, bias, out_gain)
    ]
    return pl.pallas_call(
        layer_kernel,
        name="layer",
        out_shape=(
            jax.ShapeDtypeStruct((RING * RING, rows // 2, 2 * HEAD_DIM), BF16),
            jax.ShapeDtypeStruct((RING, RING, wo.shape[0], wo.shape[1] * 2 * RING), BF16),
        ),
        in_specs=[pl.BlockSpec(memory_space=pltpu.HBM)] * 8,
        out_specs=(vmem, vmem),
        scratch_shapes=[
            pltpu.VMEM((length, 128), BF16),
            pltpu.VMEM((length // 2, 128), BF16),
            pltpu.VMEM((144, length), BF16),
            pltpu.VMEM((length, 256), BF16),
            pltpu.VMEM((length, HEAD_DIM), BF16),
            pltpu.VMEM((BLOCK_K, BLOCK_K), BF16),
            pltpu.VMEM((RING, RING, BLOCK_Q, HEAD_DIM), F32),
            pltpu.VMEM((RING, RING, BLOCK_Q, 128), F32),
            pltpu.VMEM((RING * RING, rows // 2, 2 * HEAD_DIM), BF16),
            dma(()), dma(()),
            pltpu.VMEM(bias.shape, F32), pltpu.VMEM(out_gain.shape, F32),
            pltpu.VMEM((2, RING, RING, 2, 96, depth // 2), BF16),
            pltpu.VMEM((width, 384), BF16),
            pltpu.VMEM((3, rows, width), BF16),
            pltpu.VMEM((RING, RING * rows, 128), BF16),
            pltpu.VMEM((RING * rows // 2, 128), BF16),
            dma(()), dma((2, 3)), dma(()), dma((4,)), dma(()), dma(()),
            dma(()), dma((2, 3)), dma(()), dma((2,)),
            dma((4,)), dma((4, 3)),
            dma(()), dma(()), dma(()), dma((3,)), dma(()), dma((2,)),
            dma(()), dma(()), dma(()), dma(()), dma((8,)),
            pltpu.VMEM(x.shape, BF16), pltpu.VMEM(gain.shape, F32), pltpu.VMEM(wq.shape, BF16),
            pltpu.VMEM(wk.shape, BF16), pltpu.VMEM(wv.shape, BF16), pltpu.VMEM(wo.shape, BF16),
        ],
        compiler_params=pltpu.CompilerParams(
            collective_id=0, has_side_effects=True, vmem_limit_bytes=44 << 20
        ),
    )(*operands)


def mix_kernel(ho_ref, wo_ref, o_hbm, lhs, o_ref, sems):
    heads, half, _ = ho_ref.shape
    for n in range(0, heads, 2):
        a, b = ho_ref[n], ho_ref[n + 1]
        cols = pl.ds(n * HEAD_DIM, 2 * HEAD_DIM)
        lhs[0:half, cols] = jnp.concatenate([a[:, 0:64], b[:, 0:64]], axis=1)
        lhs[half : 2 * half, cols] = jnp.concatenate([a[:, 64:128], b[:, 64:128]], axis=1)
    width = o_ref.shape[1]
    out = []
    for n in range(width // MIX):
        cols = slice(n * MIX, (n + 1) * MIX)
        o_ref[:, cols] = jnp.dot(lhs[...], wo_ref[:, cols], preferred_element_type=F32).astype(BF16)
        copy = pltpu.make_async_copy(o_ref.at[:, cols], o_hbm.at[:, cols], sems.at[n])
        copy.start()
        out.append(copy)
    for copy in out:
        copy.wait()


MIX = 512


def mix(ho, wo):
    heads, half, _ = ho.shape
    vmem = pl.BlockSpec(memory_space=pltpu.VMEM)
    return pl.pallas_call(
        mix_kernel,
        name="mix",
        out_shape=jax.ShapeDtypeStruct((2 * half, wo.shape[1]), BF16),
        in_specs=[vmem] * 2,
        out_specs=pl.BlockSpec(memory_space=pl.ANY),
        scratch_shapes=[
            pltpu.VMEM((2 * half, heads * HEAD_DIM), BF16),
            pltpu.VMEM((2 * half, wo.shape[1]), BF16),
            pltpu.SemaphoreType.DMA((wo.shape[1] // MIX,)),
        ],
        compiler_params=pltpu.CompilerParams(vmem_limit_bytes=16 << 20),
    )(ho, wo)


def body(inputs, in_gain, w_query, w_key, w_value, key_bias, out_gain, w_out):
    ho, wo = layer(
        inputs[0], in_gain[None], w_query.T, w_key.T, w_value.T, w_out, key_bias[0].T, out_gain[None]
    )
    return mix(ho, wo.reshape(-1, wo.shape[-1]))[None]


def solution(mesh):
    placed = (
        P("dp", "sp", None), P(), P("dp", "sp"), P("dp", "sp"), P("dp", "sp"),
        P("dp", None, "sp"), P(), P("sp", "dp"),
    )
    return jax.shard_map(body, mesh=mesh, in_specs=placed, out_specs=P("dp", "sp", None), check_vma=False)
```
